512 devices in a mesh: grp: 2 (over y), ra: 16 (over z), cb: 16 (over x, core).
Axes of the slice: x: 8, y: 2, z: 16, core: 2. Of those that a mesh axis runs over, the one named last changes fastest.
The devices are a block of a 8x16x16 slice.
Arguments:
- tokens: bfloat16 [256, 4096], P('grp', 'ra'), parts along dimension 0, may hold values from -20 to 20
- norm_gain: float32 [4096], P('ra'), may hold values from 0.1 to 1.9
- gate_weight: float32 [4096, 11264], P('ra', 'cb'), may hold values from -0.09375 to 0.09375
- gate_scale: float32 [11264], P('cb'), may hold values from 0.5 to 2
- up_weight: float32 [4096, 11264], P('ra', 'cb'), may hold values from -0.09375 to 0.09375
- up_scale: float32 [11264], P('cb'), may hold values from 0.5 to 2
- down_weight: float32 [11264, 4096], P('cb', 'ra'), may hold values from -1 to 1
- down_scale: float32 [4096], P('ra'), may hold values from 0.5 to 2
- out_gain: float32 [4096], P('ra'), may hold values from 0.1 to 1.9
Outputs:
- normed: bfloat16 [256, 4096], P('grp', 'ra'), parts along dimension 0
The draws below stay inside these ranges and needn't reach their ends.
There are 2 independent parts, one for each index of `grp`. The reference program is written for one: setup_inputs(seed, part) draws one part's arguments, and reference() takes and returns one part's arrays. A program takes and returns all parts, laid end to end along the dimension named above; an argument that names none is the same for every part. Nothing has to cross between parts.
All inputs are finite; a program needn't handle non-finite values.
Results may differ from the reference program's by a relative error of at most 0.012.
Values may be sent and summed in bfloat16 or wider, within the bound.
A program may use at most 64 MiB of HBM per device.

```python
import math
import jax
import jax.numpy as jnp
from jax import lax

D = 4096
FF = 11264
TOK = 128


def draw_tokens(key, part):
    first, second, third = jax.random.split(key, 3)
    base = jnp.clip(jax.random.normal(first, (TOK, D), jnp.float32), -5.0, 5.0)
    place = jnp.arange(D, dtype=jnp.float32) / D
    rows = jnp.exp(jax.random.uniform(second, (TOK, 1), jnp.float32, jnp.log(0.3), jnp.log(3.0)))
    cols = 10.0 ** (place - 1.0) * jax.random.uniform(third, (D,), jnp.float32, 0.7, 1.3)
    values = base * rows * cols
    return values.astype(jnp.bfloat16)


def draw_down_weight(key, part):
    row_key = jax.random.fold_in(key, 101)
    left_key = jax.random.fold_in(key, 102)
    right_key = jax.random.fold_in(key, 103)
    noise_key = jax.random.fold_in(key, 104)
    row_scale = jnp.exp(jax.random.uniform(row_key, (FF, 1), jnp.float32, -1.0, 1.0))
    left = jnp.clip(jax.random.normal(left_key, (FF, 1), jnp.float32), -3.0, 3.0)
    right = jnp.clip(jax.random.normal(right_key, (1, D), jnp.float32), -3.0, 3.0)
    noise = jnp.clip(jax.random.normal(noise_key, (FF, D), jnp.float32), -4.0, 4.0)
    values = row_scale * (0.7 * noise + 0.7 * left * right) * FF ** (-0.5) / 1.35
    return values.astype(jnp.float32)


def block_levels(key, dims, shards, least, largest):
    gain = 1.0
    for axis_at, blocks in shards:
        steps = jax.random.uniform(jax.random.fold_in(jax.random.fold_in(key, 6), axis_at), (blocks,), jnp.float32, least / len(shards), largest / len(shards))
        gain = gain * jnp.repeat(jnp.exp(steps), dims[axis_at] // blocks).reshape((-1,) + (1,) * (len(dims) - 1 - axis_at))
    return gain


def normal_values(key, dims, scale, most, pieces=(), held_as=jnp.bfloat16):
    entries = jax.random.normal(key, dims, jnp.float32) * scale
    if len(pieces) > 0:
        entries = block_levels(key, dims, pieces, -0.22, 0.18) * entries
    return jnp.clip(entries, min=-most, max=most).astype(held_as)


def setup_inputs(seed: int = 0, part: int = 0) -> dict:
    arg_keys = jax.random.split(jax.random.key(seed), 10)
    own_keys = jax.random.split(jax.random.fold_in(arg_keys[9], part), 10)
    return {
        "tokens": draw_tokens(jax.random.fold_in(jax.random.fold_in(arg_keys[9], part), 71), part),
        "norm_gain": jnp.clip(1.0 + 0.18 * jax.random.normal(arg_keys[1], (D,), jnp.float32), 0.1, 1.9),
        "gate_weight": normal_values(arg_keys[2], (D, FF), D ** -0.5, 0.09375, ((0, 16), (1, 16)), jnp.float32),
        "gate_scale": jnp.clip(jnp.exp(math.log(2.0) - 1.3862944 * jax.random.uniform(arg_keys[3], (FF,), jnp.float32) ** block_levels(arg_keys[3], (FF,), ((0, 16),), -0.2, 0.2)), 0.5, 2.0),
        "up_weight": normal_values(arg_keys[4], (D, FF), D ** -0.5, 0.09375, ((0, 16), (1, 16)), jnp.float32),
        "up_scale": jnp.clip(jnp.exp(math.log(2.0) - 1.3862944 * jax.random.uniform(arg_keys[5], (FF,), jnp.float32) ** block_levels(arg_keys[5], (FF,), ((0, 16),), -0.2, 0.2)), 0.5, 2.0),
        "down_weight": draw_down_weight(jax.random.fold_in(arg_keys[9], 71), part),
        "down_scale": jnp.clip(jnp.exp(math.log(2.0) - 1.3862944 * jax.random.uniform(arg_keys[7], (D,), jnp.float32) ** block_levels(arg_keys[7], (D,), ((0, 16),), -0.2, 0.2)), 0.5, 2.0),
        "out_gain": jnp.clip(1.0 + 0.18 * jax.random.normal(arg_keys[8], (D,), jnp.float32), 0.1, 1.9),
    }


def reference(tokens, norm_gain, gate_weight, gate_scale, up_weight, up_scale, down_weight, down_scale, out_gain):
    values = tokens.astype(jnp.float32)
    inv_first = lax.rsqrt(lax.optimization_barrier(jnp.mean(values * values, axis=1, keepdims=True)) + 1e-06)
    normed_in = (values * inv_first * norm_gain).astype(jnp.bfloat16)
    gate = jnp.dot(normed_in, gate_weight.astype(jnp.bfloat16), preferred_element_type=jnp.float32) * gate_scale
    up = jnp.dot(normed_in, up_weight.astype(jnp.bfloat16), preferred_element_type=jnp.float32) * up_scale
    hidden = (jax.nn.silu(gate) * up).astype(jnp.bfloat16)
    branch = jnp.dot(hidden, down_weight.astype(jnp.bfloat16), preferred_element_type=jnp.float32) * down_scale
    mixed = 0.5 * values + branch
    inv_second = lax.rsqrt(lax.optimization_barrier(jnp.mean(mixed * mixed, axis=1, keepdims=True)) + 1e-06)
    return (mixed * inv_second * out_gain).astype(jnp.bfloat16)
```

```python
import functools

import jax
import jax.numpy as jnp
from jax import lax
from jax.experimental import pallas as pl
from jax.experimental.pallas import tpu as pltpu
from jax.sharding import PartitionSpec as P

MESH = pl.DeviceIdType.MESH
LANES = 128
F32 = jnp.float32
BF16 = jnp.bfloat16


def far_first(n):
    return sorted(range(1, n), key=lambda d: -min(d, n - d))


def kernel(
    nz,
    nc,
    tok_ref,
    gain_ref,
    gw_ref,
    gs_ref,
    uw_ref,
    us_ref,
    dw_ref,
    ds_ref,
    og_ref,
    out_ref,
    gw_v,
    uw_v,
    dw_v,
    part,
    got,
    hid,
    pair,
    pair_got,
    chips,
    squares,
    load_sem,
    rs_send,
    rs_recv,
    ag_send,
    ag_recv,
    pr_send,
    pr_recv,
    x_send,
    x_recv,
    sq_send,
    sq_recv,
    o_send,
    o_recv,
):
    z = lax.axis_index("ra")
    cb = lax.axis_index("cb")
    chip = cb // 2
    core = cb % 2
    nx = nc // 2
    tokens, feats = tok_ref.shape
    units = gw_ref.shape[1]
    main = units // LANES * LANES
    rest = units - main
    tile = tokens // nz
    half = tokens // 2
    width = feats * nz

    loads = [
        pltpu.make_async_copy(src, dst, load_sem.at[k])
        for k, (src, dst) in enumerate([(gw_ref, gw_v), (uw_ref, uw_v), (dw_ref, dw_v.at[:units])])
    ]
    for copy in loads:
        copy.start()

    def to_z(d):
        return {"ra": lax.rem(z + d, nz)}

    def to_chip(d):
        return {"cb": lax.rem(chip + d, nx) * 2 + core}

    mate = {"cb": chip * 2 + 1 - core}

    barrier = pltpu.get_barrier_semaphore()
    peers = [to_z(d) for d in range(1, nz)] + [to_chip(d) for d in range(1, nx)] + [mate]
    for peer in peers:
        pl.semaphore_signal(barrier, inc=1, device_id=peer, device_id_type=MESH)

    values = tok_ref[...].astype(F32)
    scaled = (values * gain_ref[...]).astype(BF16)
    own_squares = jnp.sum(values * values, axis=1, keepdims=True)
    lane = lax.broadcasted_iota(jnp.int32, (tokens, LANES), 1)
    high = own_squares.astype(BF16).astype(F32)
    low = own_squares - high
    tail = jnp.where(lane == 0, high, jnp.where(lane == 1, low, 0.0))

    def put(columns, value):
        part[:, :, columns] = value.reshape(nz, tile, value.shape[1]).astype(BF16)

    put(slice(2 * main + 2 * rest, 2 * main + 2 * rest + LANES), tail)
    loads[0].wait()
    gate = jnp.dot(scaled, gw_v[...].astype(BF16), preferred_element_type=F32)
    put(slice(0, main), gate[:, :main])
    loads[1].wait()
    up = jnp.dot(scaled, uw_v[...].astype(BF16), preferred_element_type=F32)
    put(slice(main, 2 * main), up[:, :main])
    put(
        slice(2 * main, 2 * main + 2 * rest),
        jnp.concatenate([gate[:, main:], up[:, main:]], axis=1),
    )

    pl.semaphore_wait(barrier, len(peers))

    sends = []
    for d in far_first(nz):
        copy = pltpu.make_async_remote_copy(
            src_ref=part.at[lax.rem(z + d, nz)],
            dst_ref=got.at[d - 1],
            send_sem=rs_send.at[d - 1],
            recv_sem=rs_recv.at[d - 1],
            device_id=to_z(d),
            device_id_type=MESH,
        )
        copy.start()
        sends.append((d, copy))

    loads[2].wait()
    down = dw_v[...]
    pad = dw_v.shape[0] - units
    down = jnp.where(lax.broadcasted_iota(jnp.int32, down.shape, 0) < units, down, 0.0).astype(BF16)

    total = part[z].astype(F32)
    for d, copy in reversed(sends):
        copy.wait_recv()
        total += got[d - 1].astype(F32)
    square = jnp.sum(total[:, 2 * main + 2 * rest :], axis=1, keepdims=True)
    inv = lax.rsqrt(square / width + 1e-06)
    gate_scale = gs_ref[...]
    up_scale = us_ref[...]
    g = total[:, :main] * inv * gate_scale[:, :main]
    u = total[:, main : 2 * main] * inv * up_scale[:, :main]
    mixed_scale = jnp.concatenate([gate_scale[:, main:], up_scale[:, main:]], axis=1)
    both = total[:, 2 * main : 2 * main + 2 * rest] * inv * mixed_scale
    swapped = pltpu.roll(both, rest, 1)
    hid[z, :, :main] = (g * jax.nn.sigmoid(g) * u).astype(BF16)
    last = both * jax.nn.sigmoid(both) * swapped
    last_lane = lax.broadcasted_iota(jnp.int32, last.shape, 1)
    hid[z, :, main:] = jnp.where(last_lane < rest, last, 0.0).astype(BF16)

    hid_sends = []
    for d in far_first(nz):
        copy = pltpu.make_async_remote_copy(
            src_ref=hid.at[z],
            dst_ref=hid.at[z],
            send_sem=ag_send.at[d - 1],
            recv_sem=ag_recv.at[d - 1],
            device_id=to_z(d),
            device_id_type=MESH,
        )
        copy.start()
        hid_sends.append(copy)
    for d in far_first(nz):
        pltpu.make_async_remote_copy(
            src_ref=hid.at[z],
            dst_ref=hid.at[lax.rem(z + nz - d, nz)],
            send_sem=ag_send.at[d - 1],
            recv_sem=ag_recv.at[d - 1],
            device_id=to_z(d),
            device_id_type=MESH,
        ).wait_recv()

    partial = jnp.dot(
        hid[...].reshape(tokens, hid.shape[2]), down, preferred_element_type=F32
    )
    pair[0] = partial[:half].astype(BF16)
    pair[1] = partial[half:].astype(BF16)
    pair_copy = pltpu.make_async_remote_copy(
        src_ref=pair.at[1 - core],
        dst_ref=pair_got,
        send_sem=pr_send,
        recv_sem=pr_recv,
        device_id=mate,
        device_id_type=MESH,
    )
    pair_copy.start()
    pair_copy.wait_recv()
    chips[chip] = (pair[core].astype(F32) + pair_got[...].astype(F32)).astype(BF16)

    x_sends = []
    for d in far_first(nx):
        copy = pltpu.make_async_remote_copy(
            src_ref=chips.at[chip],
            dst_ref=chips.at[chip],
            send_sem=x_send.at[d - 1],
            recv_sem=x_recv.at[d - 1],
            device_id=to_chip(d),
            device_id_type=MESH,
        )
        copy.start()
        x_sends.append(copy)
    for d in far_first(nx):
        pltpu.make_async_remote_copy(
            src_ref=chips.at[chip],
            dst_ref=chips.at[lax.rem(chip + nx - d, nx)],
            send_sem=x_send.at[d - 1],
            recv_sem=x_recv.at[d - 1],
            device_id=to_chip(d),
            device_id_type=MESH,
        ).wait_recv()

    branch = chips[0].astype(F32)
    for k in range(1, nx):
        branch += chips[k].astype(F32)
    rows = pl.ds(pl.multiple_of(core * half, half), half)
    mixed = 0.5 * tok_ref[rows, :].astype(F32) + branch * ds_ref[...]
    column = jnp.sum(mixed * mixed, axis=1, keepdims=True)
    diagonal = lax.broadcasted_iota(jnp.int32, (half, LANES), 0) == lax.broadcasted_iota(
        jnp.int32, (half, LANES), 1
    )
    squares[z] = jnp.sum(jnp.where(diagonal, column, 0.0), axis=0, keepdims=True)

    sq_sends = []
    for d in far_first(nz):
        copy = pltpu.make_async_remote_copy(
            src_ref=squares.at[z],
            dst_ref=squares.at[z],
            send_sem=sq_send.at[d - 1],
            recv_sem=sq_recv.at[d - 1],
            device_id=to_z(d),
            device_id_type=MESH,
        )
        copy.start()
        sq_sends.append(copy)
    for d in far_first(nz):
        pltpu.make_async_remote_copy(
            src_ref=squares.at[z],
            dst_ref=squares.at[lax.rem(z + nz - d, nz)],
            send_sem=sq_send.at[d - 1],
            recv_sem=sq_recv.at[d - 1],
            device_id=to_z(d),
            device_id_type=MESH,
        ).wait_recv()
    everything = squares[0]
    for k in range(1, nz):
        everything += squares[k]
    inv_row = lax.rsqrt(everything / width + 1e-06)
    inv_second = jnp.sum(jnp.where(diagonal, inv_row, 0.0), axis=1, keepdims=True)
    out_ref[rows, :] = (mixed * inv_second * og_ref[...]).astype(BF16)
    out_copy = pltpu.make_async_remote_copy(
        src_ref=out_ref.at[rows],
        dst_ref=out_ref.at[rows],
        send_sem=o_send,
        recv_sem=o_recv,
        device_id=mate,
        device_id_type=MESH,
    )
    out_copy.start()
    for _, copy in sends:
        copy.wait_send()
    for copy in hid_sends + [pair_copy] + x_sends + sq_sends:
        copy.wait_send()
    out_copy.wait_send()
    other = pl.ds(pl.multiple_of((1 - core) * half, half), half)
    pltpu.make_async_remote_copy(
        src_ref=out_ref.at[other],
        dst_ref=out_ref.at[other],
        send_sem=o_send,
        recv_sem=o_recv,
        device_id=mate,
        device_id_type=MESH,
    ).wait_recv()


def solution(mesh):
    nz, nc = mesh.shape["ra"], mesh.shape["cb"]

    def on_device(tokens, norm_gain, gw, gs, uw, us, dw, ds, og):
        count, feats = tokens.shape
        units = gw.shape[1]
        padded = -(-units // LANES) * LANES
        tile = count // nz
        half = count // 2
        vmem = pl.BlockSpec(memory_space=pltpu.VMEM)
        hbm = pl.BlockSpec(memory_space=pl.ANY)
        dma = pltpu.SemaphoreType.DMA
        row = lambda v: v.reshape(1, -1)
        return pl.pallas_call(
            functools.partial(kernel, nz, nc),
            out_shape=jax.ShapeDtypeStruct((count, feats), BF16),
            in_specs=[vmem, vmem, hbm, vmem, hbm, vmem, hbm, vmem, vmem],
            out_specs=vmem,
            scratch_shapes=[
                pltpu.VMEM((feats, units), F32),
                pltpu.VMEM((feats, units), F32),
                pltpu.VMEM((padded, feats), F32),
                pltpu.VMEM((nz, tile, 2 * units + LANES), BF16),
                pltpu.VMEM((nz - 1, tile, 2 * units + LANES), BF16),
                pltpu.VMEM((nz, tile, padded), BF16),
                pltpu.VMEM((2, half, feats), BF16),
                pltpu.VMEM((half, feats), BF16),
                pltpu.VMEM((nc // 2, half, feats), BF16),
                pltpu.VMEM((nz, 1, LANES), F32),
                dma((3,)),
                dma((nz - 1,)),
                dma((nz - 1,)),
                dma((nz - 1,)),
                dma((nz - 1,)),
                dma,
                dma,
                dma((nc // 2 - 1,)),
                dma((nc // 2 - 1,)),
                dma((nz - 1,)),
                dma((nz - 1,)),
                dma,
                dma,
            ],
            compiler_params=pltpu.CompilerParams(collective_id=0, has_side_effects=True),
        )(tokens, row(norm_gain), gw, row(gs), uw, row(us), dw, row(ds), row(og))

    return jax.shard_map(
        on_device,
        mesh=mesh,
        in_specs=(
            P("grp", "ra"),
            P("ra"),
            P("ra", "cb"),
            P("cb"),
            P("ra", "cb"),
            P("cb"),
            P("cb", "ra"),
            P("ra"),
            P("ra"),
        ),
        out_specs=P("grp", "ra"),
        check_vma=False,
    )
```

```python
import functools

import jax
import jax.numpy as jnp
from jax import lax
from jax.experimental import pallas as pl
from jax.experimental.pallas import tpu as pltpu
from jax.sharding import PartitionSpec as P

MESH = pl.DeviceIdType.MESH
LANES = 128
F32 = jnp.float32
BF16 = jnp.bfloat16
HOP = 4


def remote(src, dst, send_sem, recv_sem, peer):
    return pltpu.make_async_remote_copy(
        src_ref=src,
        dst_ref=dst,
        send_sem=send_sem,
        recv_sem=recv_sem,
        device_id=peer,
        device_id_type=MESH,
    )


def split_tail(column, lane):
    high = column.astype(BF16).astype(F32)
    return jnp.where(lane == 0, high, jnp.where(lane == 1, column - high, 0.0))


def kernel(
    nz,
    nc,
    tok_ref,
    gain_ref,
    gw_ref,
    gs_ref,
    uw_ref,
    us_ref,
    dw_ref,
    ds_ref,
    og_ref,
    out_ref,
    gu_v,
    dw_v,
    part,
    far_in,
    far_in_half,
    near_in,
    relay_out,
    relay_in,
    hid,
    pair,
    pair_in,
    chips,
    mix,
    squares,
    load_sem,
    far_sems,
    near_sems,
    relay_sems,
    hid_sems,
    pair_sems,
    chip_sems,
    mix_sems,
    sq_sems,
):
    z = lax.axis_index("ra")
    cb = lax.axis_index("cb")
    chip = cb // 2
    core = cb % 2
    nx = nc // 2
    tile, feats = tok_ref.shape[1:]
    tokens = nz * tile
    units = gw_ref.shape[0]
    main = units // LANES * LANES
    rest = units - main
    width = feats * nz
    cols = part.shape[2]
    halves = (slice(0, cols // 2), slice(cols // 2, cols))

    def to_z(d):
        return {"ra": lax.rem(z + d + nz, nz)}

    def to_chip(d):
        return {"cb": lax.rem(chip + d, nx) * 2 + core}

    mate = {"cb": chip * 2 + 1 - core}

    def block(d):
        return lax.rem(z + d + 2 * nz, nz)

    barrier = pltpu.get_barrier_semaphore()
    peers = [to_z(s * d) for d in range(1, HOP + 1) for s in (1, -1)]
    peers += [to_chip(d) for d in range(1, nx)] + [mate]
    for peer in peers:
        pl.semaphore_signal(barrier, inc=1, device_id=peer, device_id_type=MESH)

    loads = [
        pltpu.make_async_copy(src, dst, load_sem.at[k])
        for k, (src, dst) in enumerate(
            [
                (gw_ref.at[:main], gu_v.at[:main]),
                (uw_ref.at[:main], gu_v.at[main : 2 * main]),
                (gw_ref.at[main:], gu_v.at[2 * main : 2 * main + rest]),
                (uw_ref.at[main:], gu_v.at[2 * main + rest :]),
                (dw_ref, dw_v.at[:units]),
            ]
        )
    ]
    for copy in loads:
        copy.start()

    values = tok_ref[...].astype(F32).reshape(tokens, feats)
    scaled = (values * gain_ref[...]).astype(BF16)
    lane = lax.broadcasted_iota(jnp.int32, (tokens, LANES), 1)
    tail = split_tail(jnp.sum(values * values, axis=1, keepdims=True), lane)
    part[:, :, 2 * units :] = tail.reshape(nz, tile, LANES).astype(BF16)
    for copy in loads[:-1]:
        copy.wait()
    both = lax.dot_general(
        scaled, gu_v[...].astype(BF16), (((1,), (1,)), ((), ())), preferred_element_type=F32
    )
    part[:, :, : 2 * units] = both.reshape(nz, tile, 2 * units).astype(BF16)

    pl.semaphore_wait(barrier, len(peers))

    waiting = []
    far = {}
    for k in range(HOP, 0, -1):
        for i, s in enumerate((1, -1)):
            src = part.at[block(s * (k + HOP))]
            dst = far_in.at[i, k - 1] if k < HOP else far_in_half.at[i]
            if k == HOP:
                src = part.at[block(s * (k + HOP)), :, halves[i]]
            far[i, k] = remote(src, dst, far_sems.at[0, i, k - 1], far_sems.at[1, i, k - 1], to_z(s * k))
            far[i, k].start()
    near = {}
    for k in range(HOP - 1, 0, -1):
        for i, s in enumerate((1, -1)):
            near[i, k] = remote(
                part.at[block(s * k)],
                near_in.at[i, k - 1],
                near_sems.at[0, i, k - 1],
                near_sems.at[1, i, k - 1],
                to_z(s * k),
            )
            near[i, k].start()

    loads[-1].wait()
    row = lax.broadcasted_iota(jnp.int32, dw_v.shape, 0)
    down = jnp.where(row < units, dw_v[...], 0.0).astype(BF16)

    tile_lane = lax.broadcasted_iota(jnp.int32, (tile, LANES), 1)
    relay = []
    for i, s in enumerate((1, -1)):
        for k in range(1, HOP + 1):
            far[i, k].wait_recv()
        total = part[block(s * HOP)].astype(F32)
        for k in range(1, HOP):
            total += far_in[i, k - 1].astype(F32)
        half = far_in_half[i].astype(F32)
        pieces = [total[:, halves[0]], total[:, halves[1]]]
        pieces[i] += half
        last = pieces[1][:, -LANES:]
        relay_out[i, :, halves[0]] = pieces[0].astype(BF16)
        relay_out[i, :, cols // 2 : cols - LANES] = pieces[1][:, :-LANES].astype(BF16)
        relay_out[i, :, cols - LANES :] = split_tail(
            jnp.sum(last, axis=1, keepdims=True), tile_lane
        ).astype(BF16)
        copy = remote(
            relay_out.at[i], relay_in.at[i], relay_sems.at[0, i], relay_sems.at[1, i], to_z(s * HOP)
        )
        copy.start()
        relay.append(copy)

    total = part[z].astype(F32)
    for k in range(1, HOP):
        for i in range(2):
            near[i, k].wait_recv()
            total += near_in[i, k - 1].astype(F32)
    gate_scale = gs_ref[...].reshape(1, units)
    up_scale = us_ref[...].reshape(1, units)
    mixed_scale = jnp.concatenate([gate_scale[:, main:], up_scale[:, main:]], axis=1)
    for i in range(2):
        relay[i].wait_recv()
        total += relay_in[i].astype(F32)
    square = jnp.sum(total[:, 2 * units :], axis=1, keepdims=True)
    inv = lax.rsqrt(square / width + 1e-06)
    g = total[:, :main] * inv * gate_scale[:, :main]
    u = total[:, main : 2 * main] * inv * up_scale[:, :main]
    both = total[:, 2 * main : 2 * units] * inv * mixed_scale
    swapped = pltpu.roll(both, rest, 1)
    hid[HOP, :, :main] = (g * jax.nn.sigmoid(g) * u).astype(BF16)
    last = both * jax.nn.sigmoid(both) * swapped
    hid[HOP, :, main:] = jnp.where(tile_lane < rest, last, 0.0).astype(BF16)

    spread = {}
    order = [s * k for k in range(HOP, 0, -1) for s in (1, -1)]
    order += [nz // 2] + [s * k for k in range(nz // 2 - 1, HOP, -1) for s in (1, -1)]
    for d in order:
        e = d % nz
        spread[e] = remote(
            hid.at[HOP],
            hid.at[(HOP - d) % nz],
            hid_sems.at[0, e - 1],
            hid_sems.at[1, e - 1],
            to_z(d),
        )
        spread[e].start()

    groups = 2
    size = nz // groups
    share = size // 2

    def multiply(k):
        for r in range(k * size, (k + 1) * size):
            if r != HOP:
                spread[(HOP - r) % nz].wait_recv()
        rows = hid[k * size : (k + 1) * size].reshape(size * tile, hid.shape[2])
        partial = jnp.dot(rows, down, preferred_element_type=F32)
        pair[k] = partial.reshape(size, tile, feats).astype(BF16)
        copy = remote(
            pair.at[k, pl.ds((1 - core) * share, share)],
            pair_in.at[k],
            pair_sems.at[0, k],
            pair_sems.at[1, k],
            mate,
        )
        copy.start()
        return copy

    def broadcast(k, copy):
        copy.wait_recv()
        own = pair[k, pl.ds(core * share, share)].astype(F32) + pair_in[k].astype(F32)
        chips[k, chip] = own.astype(BF16)
        copies = []
        for d in sorted(range(1, nx), key=lambda d: -min(d, nx - d)):
            to = remote(
                chips.at[k, chip],
                chips.at[k, chip],
                chip_sems.at[0, k, d - 1],
                chip_sems.at[1, k, d - 1],
                to_chip(d),
            )
            to.start()
            copies.append(to)
        return copies

    def finish(k):
        for d in range(1, nx):
            came = chips.at[k, lax.rem(chip + nx - d, nx)]
            remote(came, came, chip_sems.at[0, k, d - 1], chip_sems.at[1, k, d - 1], to_chip(d)).wait_recv()
        branch = chips[k, 0].astype(F32)
        for j in range(1, nx):
            branch += chips[k, j].astype(F32)
        first = k * size + core * share
        for j in range(share):
            own = tok_ref[block(first + j - HOP)].astype(F32)
            mix[first + j] = 0.5 * own + branch[j] * ds_ref[...]
        rows = pl.ds(first, share)
        copy = remote(mix.at[rows], mix.at[rows], mix_sems.at[0, k], mix_sems.at[1, k], mate)
        copy.start()
        other = pl.ds(k * size + (1 - core) * share, share)
        return copy, remote(mix.at[other], mix.at[other], mix_sems.at[0, k], mix_sems.at[1, k], mate)

    swaps = [multiply(0)]
    sends = broadcast(0, swaps[0])
    swaps.append(multiply(1))
    sends += broadcast(1, swaps[1])
    mixes = [finish(0), finish(1)]
    for _, came in mixes:
        came.wait_recv()

    mixed = mix[...].reshape(tokens, feats)
    column = jnp.sum(mixed * mixed, axis=1, keepdims=True)
    place = lax.broadcasted_iota(jnp.int32, (tokens, tokens), 0) + tile * (z + nz - HOP)
    diagonal = lax.rem(place, tokens) == lax.broadcasted_iota(jnp.int32, (tokens, tokens), 1)
    squares[z] = jnp.sum(jnp.where(diagonal, column, 0.0), axis=0, keepdims=True)
    sq_sends = []
    order = sorted(range(1, nz), key=lambda d: -min(d, nz - d))
    for d in order:
        copy = remote(
            squares.at[z], squares.at[z], sq_sems.at[0, d - 1], sq_sems.at[1, d - 1], to_z(d)
        )
        copy.start()
        sq_sends.append(copy)
    out_gain = og_ref[...]
    scaled_mixed = mixed * out_gain
    for d in reversed(order):
        came = squares.at[block(-d)]
        remote(came, came, sq_sems.at[0, d - 1], sq_sems.at[1, d - 1], to_z(d)).wait_recv()
    everything = squares[0]
    for j in range(1, nz):
        everything += squares[j]
    inv_row = lax.rsqrt(everything / width + 1e-06)
    inv_second = jnp.sum(jnp.where(diagonal, inv_row, 0.0), axis=1, keepdims=True)
    result = (scaled_mixed * inv_second).reshape(nz, tile, feats).astype(BF16)
    for r in range(nz):
        out_ref[block(r - HOP)] = result[r]

    for copy in list(far.values()) + list(near.values()) + relay + list(spread.values()):
        copy.wait_send()
    for copy in swaps + sends + [own for own, _ in mixes] + sq_sends:
        copy.wait_send()


def solution(mesh):
    nz, nc = mesh.shape["ra"], mesh.shape["cb"]
    nx = nc // 2

    def on_device(tokens, norm_gain, gw, gs, uw, us, dw, ds, og):
        count, feats = tokens.shape
        units = gw.shape[1]
        padded = -(-units // LANES) * LANES
        tile = count // nz
        cols = 2 * units + LANES
        share = nz // 4
        vmem = pl.BlockSpec(memory_space=pltpu.VMEM)
        hbm = pl.BlockSpec(memory_space=pl.ANY)
        dma = pltpu.SemaphoreType.DMA
        row = lambda v: v.reshape(1, -1)
        out = pl.pallas_call(
            functools.partial(kernel, nz, nc),
            out_shape=jax.ShapeDtypeStruct((nz, tile, feats), BF16),
            in_specs=[vmem, vmem, hbm, vmem, hbm, vmem, hbm, vmem, vmem],
            out_specs=vmem,
            scratch_shapes=[
                pltpu.VMEM((2 * units, feats), F32),
                pltpu.VMEM((padded, feats), F32),
                pltpu.VMEM((nz, tile, cols), BF16),
                pltpu.VMEM((2, HOP - 1, tile, cols), BF16),
                pltpu.VMEM((2, tile, cols // 2), BF16),
                pltpu.VMEM((2, HOP - 1, tile, cols), BF16),
                pltpu.VMEM((2, tile, cols), BF16),
                pltpu.VMEM((2, tile, cols), BF16),
                pltpu.VMEM((nz, tile, padded), BF16),
                pltpu.VMEM((2, nz // 2, tile, feats), BF16),
                pltpu.VMEM((2, share, tile, feats), BF16),
                pltpu.VMEM((2, nx, share, tile, feats), BF16),
                pltpu.VMEM((nz, tile, feats), F32),
                pltpu.VMEM((nz, 1, LANES), F32),
                dma((5,)),
                dma((2, 2, HOP)),
                dma((2, 2, HOP - 1)),
                dma((2, 2)),
                dma((2, nz - 1)),
                dma((2, 2)),
                dma((2, 2, nx - 1)),
                dma((2, 2)),
                dma((2, nz - 1)),
            ],
            compiler_params=pltpu.CompilerParams(collective_id=0, has_side_effects=True),
        )(
            tokens.reshape(nz, tile, feats),
            row(norm_gain),
            gw.T,
            gs,
            uw.T,
            us,
            dw,
            row(ds),
            row(og),
        )
        return out.reshape(count, feats)

    return jax.shard_map(
        on_device,
        mesh=mesh,
        in_specs=(
            P("grp", "ra"),
            P("ra"),
            P("ra", "cb"),
            P("cb"),
            P("ra", "cb"),
            P("cb"),
            P("cb", "ra"),
            P("ra"),
            P("ra"),
        ),
        out_specs=P("grp", "ra"),
        check_vma=False,
    )
```

```python
import functools

import jax
import jax.numpy as jnp
from jax import lax
from jax.experimental import pallas as pl
from jax.experimental.pallas import tpu as pltpu
from jax.sharding import PartitionSpec as P

MESH = pl.DeviceIdType.MESH
LANES = 128
F32 = jnp.float32
BF16 = jnp.bfloat16
HOP = 4


def remote(src, dst, send_sem, recv_sem, peer):
    return pltpu.make_async_remote_copy(
        src_ref=src,
        dst_ref=dst,
        send_sem=send_sem,
        recv_sem=recv_sem,
        device_id=peer,
        device_id_type=MESH,
    )


def split_tail(column, lane):
    high = column.astype(BF16).astype(F32)
    return jnp.where(lane == 0, high, jnp.where(lane == 1, column - high, 0.0))


def kernel(
    nz,
    nc,
    tok_hbm,
    gain_hbm,
    gw_ref,
    gs_hbm,
    uw_ref,
    us_hbm,
    dw_ref,
    ds_hbm,
    og_hbm,
    out_ref,
    tok_ref,
    gain_ref,
    gs_ref,
    us_ref,
    ds_ref,
    og_ref,
    gu_v,
    dw_v,
    part,
    far_in,
    far_in_half,
    near_in,
    relay_out,
    relay_in,
    hid,
    pair,
    pair_in,
    chips,
    mix,
    squares,
    load_sem,
    far_sems,
    near_sems,
    relay_sems,
    hid_sems,
    pair_sems,
    chip_sems,
    mix_sems,
    sq_sems,
):
    z = lax.axis_index("ra")
    cb = lax.axis_index("cb")
    chip = cb // 2
    core = cb % 2
    nx = nc // 2
    tile, feats = tok_ref.shape[1:]
    tokens = nz * tile
    units = gw_ref.shape[0]
    main = units // LANES * LANES
    rest = units - main
    width = feats * nz
    cols = part.shape[2]
    halves = (slice(0, cols // 2), slice(cols // 2, cols))

    def to_z(d):
        return {"ra": lax.rem(z + d + nz, nz)}

    def to_chip(d):
        return {"cb": lax.rem(chip + d, nx) * 2 + core}

    mate = {"cb": chip * 2 + 1 - core}

    def block(d):
        return lax.rem(z + d + 2 * nz, nz)

    barrier = pltpu.get_barrier_semaphore()
    peers = [to_z(s * d) for d in range(1, HOP + 1) for s in (1, -1)]
    peers += [to_chip(d) for d in range(1, nx)] + [mate]
    for peer in peers:
        pl.semaphore_signal(barrier, inc=1, device_id=peer, device_id_type=MESH)

    loads = [
        pltpu.make_async_copy(src, dst, load_sem.at[k])
        for k, (src, dst) in enumerate(
            [
                (tok_hbm, tok_ref),
                (gain_hbm, gain_ref),
                (gw_ref.at[:main], gu_v.at[:main]),
                (uw_ref.at[:main], gu_v.at[main : 2 * main]),
                (gw_ref.at[main:], gu_v.at[2 * main : 2 * main + rest]),
                (uw_ref.at[main:], gu_v.at[2 * main + rest :]),
                (gs_hbm, gs_ref),
                (us_hbm, us_ref),
                (dw_ref, dw_v.at[:units]),
                (ds_hbm, ds_ref),
                (og_hbm, og_ref),
            ]
        )
    ]
    for copy in loads:
        copy.start()

    for copy in loads[:2]:
        copy.wait()
    values = tok_ref[...].astype(F32).reshape(tokens, feats)
    scaled = (values * gain_ref[...]).astype(BF16)
    lane = lax.broadcasted_iota(jnp.int32, (tokens, LANES), 1)
    tail = split_tail(jnp.sum(values * values, axis=1, keepdims=True), lane)
    part[:, :, 2 * units :] = tail.reshape(nz, tile, LANES).astype(BF16)
    for copy in loads[2:6]:
        copy.wait()
    both = lax.dot_general(
        scaled, gu_v[...].astype(BF16), (((1,), (1,)), ((), ())), preferred_element_type=F32
    )
    part[:, :, : 2 * units] = both.reshape(nz, tile, 2 * units).astype(BF16)

    pl.semaphore_wait(barrier, len(peers))

    waiting = []
    far = {}
    for k in range(HOP, 0, -1):
        for i, s in enumerate((1, -1)):
            src = part.at[block(s * (k + HOP))]
            dst = far_in.at[i, k - 1] if k < HOP else far_in_half.at[i]
            if k == HOP:
                src = part.at[block(s * (k + HOP)), :, halves[i]]
            far[i, k] = remote(src, dst, far_sems.at[0, i, k - 1], far_sems.at[1, i, k - 1], to_z(s * k))
            far[i, k].start()
    near = {}
    for k in range(HOP - 1, 0, -1):
        for i, s in enumerate((1, -1)):
            near[i, k] = remote(
                part.at[block(s * k)],
                near_in.at[i, k - 1],
                near_sems.at[0, i, k - 1],
                near_sems.at[1, i, k - 1],
                to_z(s * k),
            )
            near[i, k].start()

    for copy in loads[6:]:
        copy.wait()
    row = lax.broadcasted_iota(jnp.int32, dw_v.shape, 0)
    down = jnp.where(row < units, dw_v[...], 0.0).astype(BF16)

    tile_lane = lax.broadcasted_iota(jnp.int32, (tile, LANES), 1)
    relay = []
    for i, s in enumerate((1, -1)):
        for k in range(1, HOP + 1):
            far[i, k].wait_recv()
        total = part[block(s * HOP)].astype(F32)
        for k in range(1, HOP):
            total += far_in[i, k - 1].astype(F32)
        half = far_in_half[i].astype(F32)
        pieces = [total[:, halves[0]], total[:, halves[1]]]
        pieces[i] += half
        last = pieces[1][:, -LANES:]
        relay_out[i, :, halves[0]] = pieces[0].astype(BF16)
        relay_out[i, :, cols // 2 : cols - LANES] = pieces[1][:, :-LANES].astype(BF16)
        relay_out[i, :, cols - LANES :] = split_tail(
            jnp.sum(last, axis=1, keepdims=True), tile_lane
        ).astype(BF16)
        copy = remote(
            relay_out.at[i], relay_in.at[i], relay_sems.at[0, i], relay_sems.at[1, i], to_z(s * HOP)
        )
        copy.start()
        relay.append(copy)

    total = part[z].astype(F32)
    for k in range(1, HOP):
        for i in range(2):
            near[i, k].wait_recv()
            total += near_in[i, k - 1].astype(F32)
    gate_scale = gs_ref[...].reshape(1, units)
    up_scale = us_ref[...].reshape(1, units)
    mixed_scale = jnp.concatenate([gate_scale[:, main:], up_scale[:, main:]], axis=1)
    for i in range(2):
        relay[i].wait_recv()
        total += relay_in[i].astype(F32)
    square = jnp.sum(total[:, 2 * units :], axis=1, keepdims=True)
    inv = lax.rsqrt(square / width + 1e-06)
    g = total[:, :main] * inv * gate_scale[:, :main]
    u = total[:, main : 2 * main] * inv * up_scale[:, :main]
    both = total[:, 2 * main : 2 * units] * inv * mixed_scale
    swapped = pltpu.roll(both, rest, 1)
    hid[HOP, :, :main] = (g * jax.nn.sigmoid(g) * u).astype(BF16)
    last = both * jax.nn.sigmoid(both) * swapped
    hid[HOP, :, main:] = jnp.where(tile_lane < rest, last, 0.0).astype(BF16)

    spread = {}
    order = [nz // 2] + [s * k for k in range(nz // 2 - 1, 0, -1) for s in (1, -1)]
    for d in order:
        e = d % nz
        spread[e] = remote(
            hid.at[HOP],
            hid.at[(HOP - d) % nz],
            hid_sems.at[0, e - 1],
            hid_sems.at[1, e - 1],
            to_z(d),
        )
        spread[e].start()

    groups = 2
    size = nz // groups
    share = size // 2

    def multiply(k):
        for r in range(k * size, (k + 1) * size):
            if r != HOP:
                spread[(HOP - r) % nz].wait_recv()
        rows = hid[k * size : (k + 1) * size].reshape(size * tile, hid.shape[2])
        partial = jnp.dot(rows, down, preferred_element_type=F32)
        pair[k] = partial.reshape(size, tile, feats).astype(BF16)
        copy = remote(
            pair.at[k, pl.ds((1 - core) * share, share)],
            pair_in.at[k],
            pair_sems.at[0, k],
            pair_sems.at[1, k],
            mate,
        )
        copy.start()
        return copy

    def broadcast(k, copy):
        copy.wait_recv()
        own = pair[k, pl.ds(core * share, share)].astype(F32) + pair_in[k].astype(F32)
        chips[k, chip] = own.astype(BF16)
        copies = []
        for d in sorted(range(1, nx), key=lambda d: -min(d, nx - d)):
            to = remote(
                chips.at[k, chip],
                chips.at[k, chip],
                chip_sems.at[0, k, d - 1],
                chip_sems.at[1, k, d - 1],
                to_chip(d),
            )
            to.start()
            copies.append(to)
        return copies

    def finish(k):
        for d in range(1, nx):
            came = chips.at[k, lax.rem(chip + nx - d, nx)]
            remote(came, came, chip_sems.at[0, k, d - 1], chip_sems.at[1, k, d - 1], to_chip(d)).wait_recv()
        branch = chips[k, 0].astype(F32)
        for j in range(1, nx):
            branch += chips[k, j].astype(F32)
        first = k * size + core * share
        for j in range(share):
            own = tok_ref[block(first + j - HOP)].astype(F32)
            mix[first + j] = 0.5 * own + branch[j] * ds_ref[...]
        rows = pl.ds(first, share)
        mine = mix[rows].reshape(share * tile, feats)
        column = jnp.sum(mine * mine, axis=1, keepdims=True)
        square = jnp.sum(jnp.where(diagonal(first, share), column, 0.0), axis=0, keepdims=True)
        copy = remote(mix.at[rows], mix.at[rows], mix_sems.at[0, k], mix_sems.at[1, k], mate)
        copy.start()
        other = pl.ds(k * size + (1 - core) * share, share)
        return square, copy, remote(mix.at[other], mix.at[other], mix_sems.at[0, k], mix_sems.at[1, k], mate)

    def diagonal(first, count):
        place = lax.broadcasted_iota(jnp.int32, (count * tile, tokens), 0)
        place = lax.rem(place + tile * (z + first + nz - HOP), tokens)
        return place == lax.broadcasted_iota(jnp.int32, (count * tile, tokens), 1)

    swaps = [multiply(0)]
    sends = broadcast(0, swaps[0])
    swaps.append(multiply(1))
    sends += broadcast(1, swaps[1])
    near_squares, near_mix, near_came = finish(0)
    far_squares, far_mix, far_came = finish(1)

    squares[core, z] = near_squares + far_squares
    own = squares.at[core, z]
    sq_sends = [remote(own, own, sq_sems.at[0, 0, 0], sq_sems.at[1, 0, 0], mate)]
    order = sorted(range(1, nz), key=lambda d: -min(d, nz - d))
    for d in order:
        for t in range(2):
            peer = {"ra": lax.rem(z + d, nz), "cb": chip * 2 + lax.rem(core + t, 2)}
            sq_sends.append(remote(own, own, sq_sems.at[0, t, d], sq_sems.at[1, t, d], peer))
    for copy in sq_sends:
        copy.start()
    near_came.wait_recv()
    far_came.wait_recv()
    scaled_mixed = mix[...].reshape(tokens, feats) * og_ref[...]
    came = squares.at[1 - core, z]
    remote(came, came, sq_sems.at[0, 0, 0], sq_sems.at[1, 0, 0], mate).wait_recv()
    for d in reversed(order):
        for t in range(2):
            came = squares.at[lax.rem(core + t, 2), block(-d)]
            remote(came, came, sq_sems.at[0, t, d], sq_sems.at[1, t, d], mate).wait_recv()
    everything = squares[0, 0]
    for j in range(1, 2 * nz):
        everything += squares[j // nz, j % nz]
    inv_row = lax.rsqrt(everything / width + 1e-06)
    inv_second = jnp.sum(jnp.where(diagonal(0, nz), inv_row, 0.0), axis=1, keepdims=True)
    result = (scaled_mixed * inv_second).reshape(nz, tile, feats).astype(BF16)
    for r in range(nz):
        out_ref[block(r - HOP)] = result[r]

    for copy in list(far.values()) + list(near.values()) + relay + list(spread.values()):
        copy.wait_send()
    for copy in swaps + sends + [near_mix, far_mix] + sq_sends:
        copy.wait_send()


def solution(mesh):
    nz, nc = mesh.shape["ra"], mesh.shape["cb"]
    nx = nc // 2

    def on_device(tokens, norm_gain, gw, gs, uw, us, dw, ds, og):
        count, feats = tokens.shape
        units = gw.shape[1]
        padded = -(-units // LANES) * LANES
        tile = count // nz
        cols = 2 * units + LANES
        share = nz // 4
        vmem = pl.BlockSpec(memory_space=pltpu.VMEM)
        hbm = pl.BlockSpec(memory_space=pltpu.HBM)
        dma = pltpu.SemaphoreType.DMA
        row = lambda v: v.reshape(1, -1)
        out = pl.pallas_call(
            functools.partial(kernel, nz, nc),
            out_shape=pltpu.VMEM((nz, tile, feats), BF16),
            in_specs=[hbm] * 9,
            out_specs=vmem,
            scratch_shapes=[
                pltpu.VMEM((nz, tile, feats), BF16),
                pltpu.VMEM((1, feats), F32),
                pltpu.VMEM((units,), F32),
                pltpu.VMEM((units,), F32),
                pltpu.VMEM((1, feats), F32),
                pltpu.VMEM((1, feats), F32),
                pltpu.VMEM((2 * units, feats), F32),
                pltpu.VMEM((padded, feats), F32),
                pltpu.VMEM((nz, tile, cols), BF16),
                pltpu.VMEM((2, HOP - 1, tile, cols), BF16),
                pltpu.VMEM((2, tile, cols // 2), BF16),
                pltpu.VMEM((2, HOP - 1, tile, cols), BF16),
                pltpu.VMEM((2, tile, cols), BF16),
                pltpu.VMEM((2, tile, cols), BF16),
                pltpu.VMEM((nz, tile, padded), BF16),
                pltpu.VMEM((2, nz // 2, tile, feats), BF16),
                pltpu.VMEM((2, share, tile, feats), BF16),
                pltpu.VMEM((2, nx, share, tile, feats), BF16),
                pltpu.VMEM((nz, tile, feats), F32),
                pltpu.VMEM((2, nz, 1, LANES), F32),
                dma((11,)),
                dma((2, 2, HOP)),
                dma((2, 2, HOP - 1)),
                dma((2, 2)),
                dma((2, nz - 1)),
                dma((2, 2)),
                dma((2, 2, nx - 1)),
                dma((2, 2)),
                dma((2, 2, nz)),
            ],
            compiler_params=pltpu.CompilerParams(
                collective_id=0, has_side_effects=True
            ),
        )(
            tokens.reshape(nz, tile, feats),
            row(norm_gain),
            gw.T,
            gs,
            uw.T,
            us,
            dw,
            row(ds),
            row(og),
        )
        return out.reshape(count, feats)

    return jax.shard_map(
        on_device,
        mesh=mesh,
        in_specs=(
            P("grp", "ra"),
            P("ra"),
            P("ra", "cb"),
            P("cb"),
            P("ra", "cb"),
            P("cb"),
            P("cb", "ra"),
            P("ra"),
            P("ra"),
        ),
        out_specs=P("grp", "ra"),
        check_vma=False,
    )
```

```python
import functools

import jax
import jax.numpy as jnp
from jax import lax
from jax.experimental import pallas as pl
from jax.experimental.pallas import tpu as pltpu
from jax.sharding import PartitionSpec as P

MESH = pl.DeviceIdType.MESH
LANES = 128
F32 = jnp.float32
BF16 = jnp.bfloat16
HOP = 4


def remote(src, dst, send_sem, recv_sem, peer):
    return pltpu.make_async_remote_copy(
        src_ref=src,
        dst_ref=dst,
        send_sem=send_sem,
        recv_sem=recv_sem,
        device_id=peer,
        device_id_type=MESH,
    )


def split_tail(column, lane):
    high = column.astype(BF16).astype(F32)
    return jnp.where(lane == 0, high, jnp.where(lane == 1, column - high, 0.0))


def kernel(
    nz,
    nc,
    tok_hbm,
    gain_hbm,
    gw_ref,
    gs_hbm,
    uw_ref,
    us_hbm,
    dw_ref,
    ds_hbm,
    og_hbm,
    out_ref,
    tok_ref,
    gain_ref,
    gs_ref,
    us_ref,
    ds_ref,
    og_ref,
    gu_v,
    dw_v,
    part,
    far_in,
    far_in_half,
    near_in,
    relay_out,
    relay_in,
    hid,
    pair,
    pair_in,
    chips,
    mix,
    squares,
    load_sem,
    ready,
    far_sems,
    near_sems,
    relay_sems,
    hid_sems,
    pair_sems,
    chip_sems,
    mix_sems,
    sq_sems,
):
    z = lax.axis_index("ra")
    cb = lax.axis_index("cb")
    chip = cb // 2
    core = cb % 2
    nx = nc // 2
    tile, feats = tok_ref.shape[1:]
    tokens = nz * tile
    units = gw_ref.shape[0]
    main = units // LANES * LANES
    rest = units - main
    width = feats * nz
    cols = part.shape[2]
    halves = (slice(0, cols // 2), slice(cols // 2, cols))

    def to_z(d):
        return {"ra": lax.rem(z + d + nz, nz)}

    def to_chip(d):
        return {"cb": lax.rem(chip + d, nx) * 2 + core}

    mate = {"cb": chip * 2 + 1 - core}

    def block(d):
        return lax.rem(z + d + 2 * nz, nz)

    near_peers = [(i, k) for k in range(HOP, 0, -1) for i in (0, 1)]
    rising = [(0, k) for k in range(1, HOP + 1)] + [(1, k) for k in range(HOP, 0, -1)]
    sign = (1, -1)

    def lower(i, k):
        return block(sign[i] * k) < z

    barrier = pltpu.get_barrier_semaphore()
    x_peers = [to_chip(d) for d in range(1, nx)] + [mate]
    for i, k in near_peers:

        @pl.when(jnp.logical_not(lower(i, k)))
        def _():
            pl.semaphore_signal(barrier, inc=1, device_id=to_z(sign[i] * k), device_id_type=MESH)

    for peer in x_peers:
        pl.semaphore_signal(barrier, inc=1, device_id=peer, device_id_type=MESH)

    loads = [
        pltpu.make_async_copy(src, dst, load_sem.at[k])
        for k, (src, dst) in enumerate(
            [
                (tok_hbm, tok_ref),
                (gain_hbm, gain_ref),
                (gw_ref.at[:main], gu_v.at[:main]),
                (uw_ref.at[:main], gu_v.at[main : 2 * main]),
                (gw_ref.at[main:], gu_v.at[2 * main : 2 * main + rest]),
                (uw_ref.at[main:], gu_v.at[2 * main + rest :]),
                (gs_hbm, gs_ref),
                (us_hbm, us_ref),
                (dw_ref, dw_v.at[:units]),
                (ds_hbm, ds_ref),
                (og_hbm, og_ref),
            ]
        )
    ]
    for copy in loads:
        copy.start()

    count = len(x_peers) + sum(jnp.where(lower(i, k), 1, 0) for i, k in near_peers)
    pl.semaphore_wait(barrier, count)
    for i, k in near_peers:

        @pl.when(lower(i, k))
        def _():
            pl.semaphore_signal(
                ready.at[1 - i, k - 1], inc=1, device_id=to_z(sign[i] * k), device_id_type=MESH
            )

    for copy in loads[:2]:
        copy.wait()
    values = tok_ref[...].astype(F32).reshape(tokens, feats)
    scaled = (values * gain_ref[...]).astype(BF16)
    lane = lax.broadcasted_iota(jnp.int32, (tokens, LANES), 1)
    tail = split_tail(jnp.sum(values * values, axis=1, keepdims=True), lane)
    part[:, :, 2 * units :] = tail.reshape(nz, tile, LANES).astype(BF16)
    for copy in loads[2:6]:
        copy.wait()
    both = lax.dot_general(
        scaled, gu_v[...].astype(BF16), (((1,), (1,)), ((), ())), preferred_element_type=F32
    )
    part[:, :, : 2 * units] = both.reshape(nz, tile, 2 * units).astype(BF16)

    far = {}
    near = {}
    for i, k in near_peers:
        src = part.at[block(sign[i] * (k + HOP))]
        dst = far_in.at[i, k - 1] if k < HOP else far_in_half.at[i]
        if k == HOP:
            src = part.at[block(sign[i] * (k + HOP)), :, halves[i]]
        sems = far_sems.at[0, i, k - 1], far_sems.at[1, i, k - 1]
        far[i, k] = remote(src, dst, *sems, to_z(sign[i] * k))
        if k < HOP:
            sems = near_sems.at[0, i, k - 1], near_sems.at[1, i, k - 1]
            near[i, k] = remote(
                part.at[block(sign[i] * k)], near_in.at[i, k - 1], *sems, to_z(sign[i] * k)
            )

    for table in (far, near):
        for i, k in near_peers:
            if (i, k) in table:

                @pl.when(lower(i, k))
                def _():
                    table[i, k].start()

    for i, k in rising:

        @pl.when(jnp.logical_not(lower(i, k)))
        def _():
            pl.semaphore_wait(ready.at[i, k - 1], 1)
            far[i, k].start()
            if k < HOP:
                near[i, k].start()

    for copy in loads[6:]:
        copy.wait()
    row = lax.broadcasted_iota(jnp.int32, dw_v.shape, 0)
    down = jnp.where(row < units, dw_v[...], 0.0).astype(BF16)

    tile_lane = lax.broadcasted_iota(jnp.int32, (tile, LANES), 1)
    relay = [
        remote(
            relay_out.at[i], relay_in.at[i], relay_sems.at[0, i], relay_sems.at[1, i], to_z(sign[i] * HOP)
        )
        for i in (0, 1)
    ]

    def pass_on(i):
        for k in range(1, HOP + 1):
            far[i, k].wait_recv()
        total = part[block(sign[i] * HOP)].astype(F32)
        for k in range(1, HOP):
            total += far_in[i, k - 1].astype(F32)
        pieces = [total[:, halves[0]], total[:, halves[1]]]
        pieces[i] += far_in_half[i].astype(F32)
        last = pieces[1][:, -LANES:]
        relay_out[i, :, halves[0]] = pieces[0].astype(BF16)
        relay_out[i, :, cols // 2 : cols - LANES] = pieces[1][:, :-LANES].astype(BF16)
        relay_out[i, :, cols - LANES :] = split_tail(
            jnp.sum(last, axis=1, keepdims=True), tile_lane
        ).astype(BF16)
        relay[i].start()

    @pl.when(z >= HOP)
    def _():
        pass_on(0)

    pass_on(1)

    @pl.when(z < HOP)
    def _():
        pass_on(0)

    total = part[z].astype(F32)
    for k in range(1, HOP):
        for i in range(2):
            near[i, k].wait_recv()
            total += near_in[i, k - 1].astype(F32)
    gate_scale = gs_ref[...].reshape(1, units)
    up_scale = us_ref[...].reshape(1, units)
    mixed_scale = jnp.concatenate([gate_scale[:, main:], up_scale[:, main:]], axis=1)
    for i in range(2):
        relay[i].wait_recv()
        total += relay_in[i].astype(F32)
    square = jnp.sum(total[:, 2 * units :], axis=1, keepdims=True)
    inv = lax.rsqrt(square / width + 1e-06)
    g = total[:, :main] * inv * gate_scale[:, :main]
    u = total[:, main : 2 * main] * inv * up_scale[:, :main]
    both = total[:, 2 * main : 2 * units] * inv * mixed_scale
    swapped = pltpu.roll(both, rest, 1)
    hid[HOP, :, :main] = (g * jax.nn.sigmoid(g) * u).astype(BF16)
    last = both * jax.nn.sigmoid(both) * swapped
    hid[HOP, :, main:] = jnp.where(tile_lane < rest, last, 0.0).astype(BF16)

    hid_cols = hid.shape[2]
    hid_halves = (slice(0, hid_cols // 2), slice(hid_cols // 2, hid_cols))
    spread = {}
    for i, k in near_peers:
        spread[i, k] = remote(
            hid.at[HOP],
            hid.at[(HOP - sign[i] * k) % nz],
            hid_sems.at[0, 0, i, k - 1],
            hid_sems.at[1, 0, i, k - 1],
            to_z(sign[i] * k),
        )
        spread[i, k].start()
    onward = {}
    for i in (0, 1):
        spread[i, HOP].wait_recv()
        for k in range(HOP, 0, -1):
            src = hid.at[(HOP - sign[i] * HOP) % nz]
            dst = hid.at[(HOP - sign[i] * (HOP + k)) % nz]
            if k == HOP:
                src = hid.at[(HOP - sign[i] * HOP) % nz, :, hid_halves[i]]
                dst = hid.at[(HOP - sign[i] * (HOP + k)) % nz, :, hid_halves[i]]
            onward[i, k] = remote(
                src, dst, hid_sems.at[0, 1, i, k - 1], hid_sems.at[1, 1, i, k - 1], to_z(sign[i] * k)
            )
            onward[i, k].start()

    groups = 2
    size = nz // groups
    share = size // 2

    def multiply(k):
        for i, j in near_peers:
            if k == 1:
                onward[i, j].wait_recv()
            elif j < HOP:
                spread[i, j].wait_recv()
        rows = hid[k * size : (k + 1) * size].reshape(size * tile, hid.shape[2])
        partial = jnp.dot(rows, down, preferred_element_type=F32)
        pair[k] = partial.reshape(size, tile, feats).astype(BF16)
        copy = remote(
            pair.at[k, pl.ds((1 - core) * share, share)],
            pair_in.at[k],
            pair_sems.at[0, k],
            pair_sems.at[1, k],
            mate,
        )
        copy.start()
        return copy

    def broadcast(k, copy):
        copy.wait_recv()
        own = pair[k, pl.ds(core * share, share)].astype(F32) + pair_in[k].astype(F32)
        chips[k, chip] = own.astype(BF16)
        copies = []
        for d in sorted(range(1, nx), key=lambda d: -min(d, nx - d)):
            to = remote(
                chips.at[k, chip],
                chips.at[k, chip],
                chip_sems.at[0, k, d - 1],
                chip_sems.at[1, k, d - 1],
                to_chip(d),
            )
            to.start()
            copies.append(to)
        return copies

    def finish(k):
        for d in range(1, nx):
            came = chips.at[k, lax.rem(chip + nx - d, nx)]
            remote(came, came, chip_sems.at[0, k, d - 1], chip_sems.at[1, k, d - 1], to_chip(d)).wait_recv()
        branch = chips[k, 0].astype(F32)
        for j in range(1, nx):
            branch += chips[k, j].astype(F32)
        first = k * size + core * share
        for j in range(share):
            own = tok_ref[block(first + j - HOP)].astype(F32)
            mix[first + j] = 0.5 * own + branch[j] * ds_ref[...]
        rows = pl.ds(first, share)
        mine = mix[rows].reshape(share * tile, feats)
        column = jnp.sum(mine * mine, axis=1, keepdims=True)
        square = jnp.sum(jnp.where(diagonal(first, share), column, 0.0), axis=0, keepdims=True)
        copy = remote(mix.at[rows], mix.at[rows], mix_sems.at[0, k], mix_sems.at[1, k], mate)
        copy.start()
        other = pl.ds(k * size + (1 - core) * share, share)
        return square, copy, remote(mix.at[other], mix.at[other], mix_sems.at[0, k], mix_sems.at[1, k], mate)

    def diagonal(first, count):
        place = lax.broadcasted_iota(jnp.int32, (count * tile, tokens), 0)
        place = lax.rem(place + tile * (z + first + nz - HOP), tokens)
        return place == lax.broadcasted_iota(jnp.int32, (count * tile, tokens), 1)

    swaps = [multiply(0)]
    sends = broadcast(0, swaps[0])
    swaps.append(multiply(1))
    sends += broadcast(1, swaps[1])
    near_squares, near_mix, near_came = finish(0)
    far_squares, far_mix, far_came = finish(1)

    squares[core, z] = near_squares + far_squares
    own = squares.at[core, z]
    sq_sends = [remote(own, own, sq_sems.at[0, 0, 0], sq_sems.at[1, 0, 0], mate)]
    order = sorted(range(1, nz), key=lambda d: -min(d, nz - d))
    for d in order:
        for t in range(2):
            peer = {"ra": lax.rem(z + d, nz), "cb": chip * 2 + lax.rem(core + t, 2)}
            sq_sends.append(remote(own, own, sq_sems.at[0, t, d], sq_sems.at[1, t, d], peer))
    for copy in sq_sends:
        copy.start()
    near_came.wait_recv()
    far_came.wait_recv()
    scaled_mixed = mix[...].reshape(tokens, feats) * og_ref[...]
    came = squares.at[1 - core, z]
    remote(came, came, sq_sems.at[0, 0, 0], sq_sems.at[1, 0, 0], mate).wait_recv()
    for d in reversed(order):
        for t in range(2):
            came = squares.at[lax.rem(core + t, 2), block(-d)]
            remote(came, came, sq_sems.at[0, t, d], sq_sems.at[1, t, d], mate).wait_recv()
    everything = squares[0, 0]
    for j in range(1, 2 * nz):
        everything += squares[j // nz, j % nz]
    inv_row = lax.rsqrt(everything / width + 1e-06)
    inv_second = jnp.sum(jnp.where(diagonal(0, nz), inv_row, 0.0), axis=1, keepdims=True)
    result = (scaled_mixed * inv_second).reshape(nz, tile, feats).astype(BF16)
    for r in range(nz):
        out_ref[block(r - HOP)] = result[r]

    tables = (far, near, spread, onward)
    for copy in relay + [copy for table in tables for copy in table.values()]:
        copy.wait_send()
    for copy in swaps + sends + [near_mix, far_mix] + sq_sends:
        copy.wait_send()


def solution(mesh):
    nz, nc = mesh.shape["ra"], mesh.shape["cb"]
    nx = nc // 2

    def on_device(tokens, norm_gain, gw, gs, uw, us, dw, ds, og):
        count, feats = tokens.shape
        units = gw.shape[1]
        padded = -(-units // LANES) * LANES
        tile = count // nz
        cols = 2 * units + LANES
        share = nz // 4
        vmem = pl.BlockSpec(memory_space=pltpu.VMEM)
        hbm = pl.BlockSpec(memory_space=pltpu.HBM)
        dma = pltpu.SemaphoreType.DMA
        row = lambda v: v.reshape(1, -1)
        out = pl.pallas_call(
            functools.partial(kernel, nz, nc),
            out_shape=pltpu.VMEM((nz, tile, feats), BF16),
            in_specs=[hbm] * 9,
            out_specs=vmem,
            scratch_shapes=[
                pltpu.VMEM((nz, tile, feats), BF16),
                pltpu.VMEM((1, feats), F32),
                pltpu.VMEM((units,), F32),
                pltpu.VMEM((units,), F32),
                pltpu.VMEM((1, feats), F32),
                pltpu.VMEM((1, feats), F32),
                pltpu.VMEM((2 * units, feats), F32),
                pltpu.VMEM((padded, feats), F32),
                pltpu.VMEM((nz, tile, cols), BF16),
                pltpu.VMEM((2, HOP - 1, tile, cols), BF16),
                pltpu.VMEM((2, tile, cols // 2), BF16),
                pltpu.VMEM((2, HOP - 1, tile, cols), BF16),
                pltpu.VMEM((2, tile, cols), BF16),
                pltpu.VMEM((2, tile, cols), BF16),
                pltpu.VMEM((nz, tile, padded), BF16),
                pltpu.VMEM((2, nz // 2, tile, feats), BF16),
                pltpu.VMEM((2, share, tile, feats), BF16),
                pltpu.VMEM((2, nx, share, tile, feats), BF16),
                pltpu.VMEM((nz, tile, feats), F32),
                pltpu.VMEM((2, nz, 1, LANES), F32),
                dma((11,)),
                pltpu.SemaphoreType.REGULAR((2, HOP)),
                dma((2, 2, HOP)),
                dma((2, 2, HOP - 1)),
                dma((2, 2)),
                dma((2, 2, 2, HOP)),
                dma((2, 2)),
                dma((2, 2, nx - 1)),
                dma((2, 2)),
                dma((2, 2, nz)),
            ],
            compiler_params=pltpu.CompilerParams(
                collective_id=0, has_side_effects=True
            ),
        )(
            tokens.reshape(nz, tile, feats),
            row(norm_gain),
            gw.T,
            gs,
            uw.T,
            us,
            dw,
            row(ds),
            row(og),
        )
        return out.reshape(count, feats)

    return jax.shard_map(
        on_device,
        mesh=mesh,
        in_specs=(
            P("grp", "ra"),
            P("ra"),
            P("ra", "cb"),
            P("cb"),
            P("ra", "cb"),
            P("cb"),
            P("cb", "ra"),
            P("ra"),
            P("ra"),
        ),
        out_specs=P("grp", "ra"),
        check_vma=False,
    )
```

```python
import functools

import jax
import jax.numpy as jnp
from jax import lax
from jax.experimental import pallas as pl
from jax.experimental.pallas import tpu as pltpu
from jax.sharding import PartitionSpec as P

MESH = pl.DeviceIdType.MESH
LANES = 128
F32 = jnp.float32
BF16 = jnp.bfloat16
HOP = 4


def remote(src, dst, send_sem, recv_sem, peer):
    return pltpu.make_async_remote_copy(
        src_ref=src,
        dst_ref=dst,
        send_sem=send_sem,
        recv_sem=recv_sem,
        device_id=peer,
        device_id_type=MESH,
    )


def arrived(ref, sem, peer):
    remote(ref, ref, sem, sem, peer).wait_recv()


def left(ref, sem, peer):
    remote(ref, ref, sem, sem, peer).wait_send()


def split_tail(column, lane):
    high = column.astype(BF16).astype(F32)
    return jnp.where(lane == 0, high, jnp.where(lane == 1, column - high, 0.0))


def kernel(
    nz,
    nc,
    tok_hbm,
    gain_hbm,
    gw_ref,
    gs_hbm,
    uw_ref,
    us_hbm,
    dw_ref,
    ds_hbm,
    og_hbm,
    out_ref,
    tok_ref,
    gain_ref,
    gs_ref,
    us_ref,
    ds_ref,
    og_ref,
    gu_v,
    dw_v,
    part,
    far_in,
    far_in_half,
    near_in,
    relay_out,
    relay_in,
    hid,
    pair,
    pair_in,
    chips,
    mix,
    squares,
    load_sem,
    ready,
    x_ready,
    rs_send,
    far_recv,
    near_recv,
    relay_recv,
    hid_send,
    hid_recv,
    pair_send,
    pair_recv,
    chip_send,
    chip_recv,
    mix_send,
    mix_recv,
    sq_send,
    sq_recv,
):
    z = lax.axis_index("ra")
    cb = lax.axis_index("cb")
    chip = cb // 2
    core = cb % 2
    nx = nc // 2
    tile, feats = tok_ref.shape[1:]
    tokens = nz * tile
    units = gw_ref.shape[0]
    main = units // LANES * LANES
    rest = units - main
    width = feats * nz
    cols = part.shape[2]
    halves = (slice(0, cols // 2), slice(cols // 2, cols))

    def to_z(d):
        return {"ra": lax.rem(z + d + nz, nz)}

    def to_chip(d):
        return {"cb": lax.rem(chip + d, nx) * 2 + core}

    mate = {"cb": chip * 2 + 1 - core}

    def block(d):
        return lax.rem(z + d + 2 * nz, nz)

    near_peers = [(i, k) for k in range(HOP, 0, -1) for i in (0, 1)]
    rising = [(0, k) for k in range(1, HOP + 1)] + [(1, k) for k in range(HOP, 0, -1)]
    sign = (1, -1)

    def lower(i, k):
        return block(sign[i] * k) < z

    def turn(c):
        return jnp.minimum(c, nx - c) * nx + c

    def x_lower(d):
        return core == 0 if d == 0 else turn(lax.rem(chip + d, nx)) < turn(chip)

    def to_x(d):
        return mate if d == 0 else to_chip(d)

    barrier = pltpu.get_barrier_semaphore()
    for i, k in near_peers:

        @pl.when(jnp.logical_not(lower(i, k)))
        def _():
            pl.semaphore_signal(barrier, inc=1, device_id=to_z(sign[i] * k), device_id_type=MESH)

    for d in range(nx):

        @pl.when(jnp.logical_not(x_lower(d)))
        def _():
            pl.semaphore_signal(barrier, inc=1, device_id=to_x(d), device_id_type=MESH)

    loads = [
        pltpu.make_async_copy(src, dst, load_sem.at[k])
        for k, (src, dst) in enumerate(
            [
                (tok_hbm, tok_ref),
                (gain_hbm, gain_ref),
                (gw_ref.at[:main], gu_v.at[:main]),
                (uw_ref.at[:main], gu_v.at[main : 2 * main]),
                (gw_ref.at[main:], gu_v.at[2 * main : 2 * main + rest]),
                (uw_ref.at[main:], gu_v.at[2 * main + rest :]),
                (gs_hbm, gs_ref),
                (us_hbm, us_ref),
                (dw_ref, dw_v.at[:units]),
                (ds_hbm, ds_ref),
                (og_hbm, og_ref),
            ]
        )
    ]
    for copy in loads:
        copy.start()

    count = sum(jnp.where(lower(i, k), 1, 0) for i, k in near_peers)
    count += sum(jnp.where(x_lower(d), 1, 0) for d in range(nx))

    @pl.when(count > 0)
    def _():
        pl.semaphore_wait(barrier, count)

    for i, k in near_peers:

        @pl.when(lower(i, k))
        def _():
            pl.semaphore_signal(
                ready.at[1 - i, k - 1], inc=1, device_id=to_z(sign[i] * k), device_id_type=MESH
            )

    for d in range(nx):

        @pl.when(x_lower(d))
        def _():
            pl.semaphore_signal(
                x_ready.at[(nx - d) % nx], inc=1, device_id=to_x(d), device_id_type=MESH
            )

    for copy in loads[:2]:
        copy.wait()
    values = tok_ref[...].astype(F32).reshape(tokens, feats)
    scaled = (values * gain_ref[...]).astype(BF16)
    lane = lax.broadcasted_iota(jnp.int32, (tokens, LANES), 1)
    tail = split_tail(jnp.sum(values * values, axis=1, keepdims=True), lane)
    part[:, :, 2 * units :] = tail.reshape(nz, tile, LANES).astype(BF16)
    for copy in loads[2:6]:
        copy.wait()
    both = lax.dot_general(
        scaled, gu_v[...].astype(BF16), (((1,), (1,)), ((), ())), preferred_element_type=F32
    )
    part[:, :, : 2 * units] = both.reshape(nz, tile, 2 * units).astype(BF16)

    far = {}
    near = {}
    for i, k in near_peers:
        src = part.at[block(sign[i] * (k + HOP))]
        dst = far_in.at[i, k - 1] if k < HOP else far_in_half.at[i]
        if k == HOP:
            src = part.at[block(sign[i] * (k + HOP)), :, halves[i]]
        far[i, k] = remote(src, dst, rs_send, far_recv.at[i], to_z(sign[i] * k))
        if k < HOP:
            near[i, k] = remote(
                part.at[block(sign[i] * k)],
                near_in.at[i, k - 1],
                rs_send,
                near_recv,
                to_z(sign[i] * k),
            )

    for table in (far, near):
        for i, k in near_peers:
            if (i, k) in table:

                @pl.when(lower(i, k))
                def _():
                    table[i, k].start()

    for i, k in rising:

        @pl.when(jnp.logical_not(lower(i, k)))
        def _():
            pl.semaphore_wait(ready.at[i, k - 1], 1)
            far[i, k].start()
            if k < HOP:
                near[i, k].start()

    for copy in loads[6:]:
        copy.wait()
    row = lax.broadcasted_iota(jnp.int32, dw_v.shape, 0)
    down = jnp.where(row < units, dw_v[...], 0.0).astype(BF16)

    tile_lane = lax.broadcasted_iota(jnp.int32, (tile, LANES), 1)
    relay = [
        remote(relay_out.at[i], relay_in.at[i], rs_send, relay_recv, to_z(sign[i] * HOP))
        for i in (0, 1)
    ]

    def pass_on(i):
        arrived(part.at[: 2 * HOP - 1, :, halves[0]], far_recv.at[i], mate)
        total = part[block(sign[i] * HOP)].astype(F32)
        for k in range(1, HOP):
            total += far_in[i, k - 1].astype(F32)
        pieces = [total[:, halves[0]], total[:, halves[1]]]
        pieces[i] += far_in_half[i].astype(F32)
        last = pieces[1][:, -LANES:]
        relay_out[i, :, halves[0]] = pieces[0].astype(BF16)
        relay_out[i, :, cols // 2 : cols - LANES] = pieces[1][:, :-LANES].astype(BF16)
        relay_out[i, :, cols - LANES :] = split_tail(
            jnp.sum(last, axis=1, keepdims=True), tile_lane
        ).astype(BF16)
        relay[i].start()

    @pl.when(z >= HOP)
    def _():
        pass_on(0)

    pass_on(1)

    @pl.when(z < HOP)
    def _():
        pass_on(0)

    total = part[z].astype(F32)
    arrived(near_in, near_recv, mate)
    for k in range(1, HOP):
        for i in range(2):
            total += near_in[i, k - 1].astype(F32)
    gate_scale = gs_ref[...].reshape(1, units)
    up_scale = us_ref[...].reshape(1, units)
    mixed_scale = jnp.concatenate([gate_scale[:, main:], up_scale[:, main:]], axis=1)
    arrived(relay_in, relay_recv, mate)
    for i in range(2):
        total += relay_in[i].astype(F32)
    square = jnp.sum(total[:, 2 * units :], axis=1, keepdims=True)
    inv = lax.rsqrt(square / width + 1e-06)
    g = total[:, :main] * inv * gate_scale[:, :main]
    u = total[:, main : 2 * main] * inv * up_scale[:, :main]
    both = total[:, 2 * main : 2 * units] * inv * mixed_scale
    swapped = pltpu.roll(both, rest, 1)
    hid[HOP, :, :main] = (g * jax.nn.sigmoid(g) * u).astype(BF16)
    last = both * jax.nn.sigmoid(both) * swapped
    hid[HOP, :, main:] = jnp.where(tile_lane < rest, last, 0.0).astype(BF16)

    hid_cols = hid.shape[2]
    hid_halves = (slice(0, hid_cols // 2), slice(hid_cols // 2, hid_cols))
    spread = {}
    for i, k in near_peers:
        spread[i, k] = remote(
            hid.at[HOP],
            hid.at[(HOP - sign[i] * k) % nz],
            hid_send,
            hid_recv.at[i if k == HOP else 2],
            to_z(sign[i] * k),
        )
        spread[i, k].start()
    onward = {}
    for i in (0, 1):
        arrived(hid.at[0], hid_recv.at[i], mate)
        for k in range(HOP, 0, -1):
            src = hid.at[(HOP - sign[i] * HOP) % nz]
            dst = hid.at[(HOP - sign[i] * (HOP + k)) % nz]
            if k == HOP:
                src = hid.at[(HOP - sign[i] * HOP) % nz, :, hid_halves[i]]
                dst = hid.at[(HOP - sign[i] * (HOP + k)) % nz, :, hid_halves[i]]
            onward[i, k] = remote(src, dst, hid_send, hid_recv.at[3], to_z(sign[i] * k))
            onward[i, k].start()

    groups = 2
    size = nz // groups
    share = size // 2

    def multiply(k):
        arrived(hid.at[: 2 * HOP - 2 + k], hid_recv.at[2 + k], mate)
        rows = hid[k * size : (k + 1) * size].reshape(size * tile, hid.shape[2])
        partial = jnp.dot(rows, down, preferred_element_type=F32)
        pair[k] = partial.reshape(size, tile, feats).astype(BF16)
        copy = remote(
            pair.at[k, pl.ds((1 - core) * share, share)],
            pair_in.at[k],
            pair_send,
            pair_recv.at[k],
            mate,
        )
        copy.start()

    def broadcast(k):
        arrived(pair_in.at[k], pair_recv.at[k], mate)
        own = pair[k, pl.ds(core * share, share)].astype(F32) + pair_in[k].astype(F32)
        chips[k, chip] = own.astype(BF16)
        for d in sorted(range(1, nx), key=lambda d: -min(d, nx - d)):
            to = remote(
                chips.at[k, chip],
                chips.at[k, chip],
                chip_send,
                chip_recv.at[k],
                to_chip(d),
            )
            to.start()

    def finish(k):
        arrived(chips.at[k, : nx - 1], chip_recv.at[k], mate)
        branch = chips[k, 0].astype(F32)
        for j in range(1, nx):
            branch += chips[k, j].astype(F32)
        first = k * size + core * share
        for j in range(share):
            own = tok_ref[block(first + j - HOP)].astype(F32)
            mix[first + j] = 0.5 * own + branch[j] * ds_ref[...]
        rows = pl.ds(first, share)
        mine = mix[rows].reshape(share * tile, feats)
        column = jnp.sum(mine * mine, axis=1, keepdims=True)
        square = jnp.sum(jnp.where(diagonal(first, share), column, 0.0), axis=0, keepdims=True)
        remote(mix.at[rows], mix.at[rows], mix_send, mix_recv, mate).start()
        return square

    def diagonal(first, count):
        place = lax.broadcasted_iota(jnp.int32, (count * tile, tokens), 0)
        place = lax.rem(place + tile * (z + first + nz - HOP), tokens)
        return place == lax.broadcasted_iota(jnp.int32, (count * tile, tokens), 1)

    @pl.when(jnp.logical_not(x_lower(0)))
    def _():
        pl.semaphore_wait(x_ready.at[0], 1)

    multiply(0)
    for d in range(1, nx):

        @pl.when(jnp.logical_not(x_lower(d)))
        def _():
            pl.semaphore_wait(x_ready.at[d], 1)

    broadcast(0)
    multiply(1)
    broadcast(1)
    near_squares = finish(0)
    far_squares = finish(1)

    squares[core * nz + z] = near_squares + far_squares
    own = squares.at[core * nz + z]
    order = sorted(range(1, nz), key=lambda d: -min(d, nz - d))
    for d in order:
        for t in range(2):
            peer = {"ra": lax.rem(z + d, nz), "cb": chip * 2 + lax.rem(core + t, 2)}
            remote(own, own, sq_send, sq_recv, peer).start()
    remote(own, own, sq_send, sq_recv, mate).start()
    arrived(mix.at[: 2 * share], mix_recv, mate)
    scaled_mixed = mix[...].reshape(tokens, feats) * og_ref[...]
    arrived(squares.at[: 2 * nz - 1], sq_recv, mate)
    everything = squares[0]
    for j in range(1, 2 * nz):
        everything += squares[j]
    inv_row = lax.rsqrt(everything / width + 1e-06)
    inv_second = jnp.sum(jnp.where(diagonal(0, nz), inv_row, 0.0), axis=1, keepdims=True)
    result = (scaled_mixed * inv_second).reshape(nz, tile, feats).astype(BF16)
    for r in range(nz):
        out_ref[block(r - HOP)] = result[r]

    left(part.at[: 4 * HOP - 1], rs_send, mate)
    left(hid.at[: 4 * HOP - 1], hid_send, mate)
    left(pair.at[0], pair_send, mate)
    left(chips.at[:, : nx - 1], chip_send, mate)
    left(mix.at[: 2 * share], mix_send, mate)
    left(squares.at[: 2 * nz - 1], sq_send, mate)


def solution(mesh):
    nz, nc = mesh.shape["ra"], mesh.shape["cb"]
    nx = nc // 2

    def on_device(tokens, norm_gain, gw, gs, uw, us, dw, ds, og):
        count, feats = tokens.shape
        units = gw.shape[1]
        padded = -(-units // LANES) * LANES
        tile = count // nz
        cols = 2 * units + LANES
        share = nz // 4
        vmem = pl.BlockSpec(memory_space=pltpu.VMEM)
        hbm = pl.BlockSpec(memory_space=pltpu.HBM)
        dma = pltpu.SemaphoreType.DMA
        row = lambda v: v.reshape(1, -1)
        out = pl.pallas_call(
            functools.partial(kernel, nz, nc),
            out_shape=pltpu.VMEM((nz, tile, feats), BF16),
            in_specs=[hbm] * 9,
            out_specs=vmem,
            scratch_shapes=[
                pltpu.VMEM((nz, tile, feats), BF16),
                pltpu.VMEM((1, feats), F32),
                pltpu.VMEM((units,), F32),
                pltpu.VMEM((units,), F32),
                pltpu.VMEM((1, feats), F32),
                pltpu.VMEM((1, feats), F32),
                pltpu.VMEM((2 * units, feats), F32),
                pltpu.VMEM((padded, feats), F32),
                pltpu.VMEM((nz, tile, cols), BF16),
                pltpu.VMEM((2, HOP - 1, tile, cols), BF16),
                pltpu.VMEM((2, tile, cols // 2), BF16),
                pltpu.VMEM((2, HOP - 1, tile, cols), BF16),
                pltpu.VMEM((2, tile, cols), BF16),
                pltpu.VMEM((2, tile, cols), BF16),
                pltpu.VMEM((nz, tile, padded), BF16),
                pltpu.VMEM((2, nz // 2, tile, feats), BF16),
                pltpu.VMEM((2, share, tile, feats), BF16),
                pltpu.VMEM((2, nx, share, tile, feats), BF16),
                pltpu.VMEM((nz, tile, feats), F32),
                pltpu.VMEM((2 * nz, 1, LANES), F32),
                dma((11,)),
                pltpu.SemaphoreType.REGULAR((2, HOP)),
                pltpu.SemaphoreType.REGULAR((nx,)),
                dma,
                dma((2,)),
                dma,
                dma,
                dma,
                dma((4,)),
                dma,
                dma((2,)),
                dma,
                dma((2,)),
                dma,
                dma,
                dma,
                dma,
            ],
            compiler_params=pltpu.CompilerParams(
                collective_id=0, has_side_effects=True
            ),
        )(
            tokens.reshape(nz, tile, feats),
            row(norm_gain),
            gw.T,
            gs,
            uw.T,
            us,
            dw,
            row(ds),
            row(og),
        )
        return out.reshape(count, feats)

    return jax.shard_map(
        on_device,
        mesh=mesh,
        in_specs=(
            P("grp", "ra"),
            P("ra"),
            P("ra", "cb"),
            P("cb"),
            P("ra", "cb"),
            P("cb"),
            P("cb", "ra"),
            P("ra"),
            P("ra"),
        ),
        out_specs=P("grp", "ra"),
        check_vma=False,
    )
```

```python
import functools

import jax
import jax.numpy as jnp
from jax import lax
from jax.experimental import pallas as pl
from jax.experimental.pallas import tpu as pltpu
from jax.sharding import PartitionSpec as P

MESH = pl.DeviceIdType.MESH
LANES = 128
F32 = jnp.float32
BF16 = jnp.bfloat16
HOP = 4


def remote(src, dst, send_sem, recv_sem, peer):
    return pltpu.make_async_remote_copy(
        src_ref=src,
        dst_ref=dst,
        send_sem=send_sem,
        recv_sem=recv_sem,
        device_id=peer,
        device_id_type=MESH,
    )


def arrived(ref, sem, peer):
    remote(ref, ref, sem, sem, peer).wait_recv()


def left(ref, sem, peer):
    remote(ref, ref, sem, sem, peer).wait_send()


def split_tail(column, lane):
    high = column.astype(BF16).astype(F32)
    return jnp.where(lane == 0, high, jnp.where(lane == 1, column - high, 0.0))


def kernel(
    nz,
    nc,
    tok_hbm,
    gain_hbm,
    gw_ref,
    gs_hbm,
    uw_ref,
    us_hbm,
    dw_ref,
    ds_hbm,
    og_hbm,
    out_ref,
    tok_ref,
    gain_ref,
    gs_ref,
    us_ref,
    ds_ref,
    og_ref,
    gu_v,
    dw_v,
    part,
    far_in,
    far_in_half,
    near_in,
    relay_out,
    relay_in,
    hid,
    pair,
    pair_in,
    chips,
    mix,
    squares,
    load_sem,
    ready,
    x_ready,
    word,
    rs_send,
    far_recv,
    near_recv,
    relay_recv,
    hid_send,
    hid_recv,
    pair_send,
    pair_recv,
    chip_send,
    chip_recv,
    mix_send,
    mix_recv,
    sq_send,
    sq_recv,
):
    z = lax.axis_index("ra")
    cb = lax.axis_index("cb")
    chip = cb // 2
    core = cb % 2
    nx = nc // 2
    tile, feats = tok_ref.shape[1:]
    tokens = nz * tile
    units = gw_ref.shape[0]
    main = units // LANES * LANES
    rest = units - main
    width = feats * nz
    cols = part.shape[2]
    halves = (slice(0, cols // 2), slice(cols // 2, cols))

    def to_z(d):
        return {"ra": lax.rem(z + d + nz, nz)}

    def to_chip(d):
        return {"cb": lax.rem(chip + d, nx) * 2 + core}

    mate = {"cb": chip * 2 + 1 - core}

    def block(d):
        return lax.rem(z + d + 2 * nz, nz)

    near_peers = [(i, k) for k in range(HOP, 0, -1) for i in (0, 1)]
    rising = [(0, k) for k in range(1, HOP + 1)] + [(1, k) for k in range(HOP, 0, -1)]
    sign = (1, -1)

    def lower(i, k):
        return block(sign[i] * k) < z

    def turn(c):
        return jnp.minimum(c, nx - c) * nx + c

    def x_lower(d):
        return core == 0 if d == 0 else turn(lax.rem(chip + d, nx)) < turn(chip)

    def to_x(d):
        return mate if d == 0 else to_chip(d)

    beside = (0, 1, nx - 1)
    barrier = pltpu.get_barrier_semaphore()
    for i, k in near_peers:

        @pl.when(jnp.logical_not(lower(i, k)))
        def _():
            pl.semaphore_signal(barrier, inc=1, device_id=to_z(sign[i] * k), device_id_type=MESH)

    for d in beside:

        @pl.when(jnp.logical_not(x_lower(d)))
        def _():
            pl.semaphore_signal(barrier, inc=1, device_id=to_x(d), device_id_type=MESH)

    loads = [
        pltpu.make_async_copy(src, dst, load_sem.at[k])
        for k, (src, dst) in enumerate(
            [
                (tok_hbm, tok_ref),
                (gain_hbm, gain_ref),
                (gw_ref.at[:main], gu_v.at[:main]),
                (uw_ref.at[:main], gu_v.at[main : 2 * main]),
                (gw_ref.at[main:], gu_v.at[2 * main : 2 * main + rest]),
                (uw_ref.at[main:], gu_v.at[2 * main + rest :]),
                (gs_hbm, gs_ref),
                (us_hbm, us_ref),
                (dw_ref, dw_v.at[:units]),
                (ds_hbm, ds_ref),
                (og_hbm, og_ref),
            ]
        )
    ]
    for copy in loads:
        copy.start()

    count = sum(jnp.where(lower(i, k), 1, 0) for i, k in near_peers)
    count += sum(jnp.where(x_lower(d), 1, 0) for d in beside)

    @pl.when(count > 0)
    def _():
        pl.semaphore_wait(barrier, count)

    for i, k in near_peers:

        @pl.when(lower(i, k))
        def _():
            pl.semaphore_signal(
                ready.at[1 - i, k - 1], inc=1, device_id=to_z(sign[i] * k), device_id_type=MESH
            )

    for n, d in enumerate(beside):

        @pl.when(x_lower(d))
        def _():
            pl.semaphore_signal(
                x_ready.at[(3 - n) % 3], inc=1, device_id=to_x(d), device_id_type=MESH
            )

    for copy in loads[:2]:
        copy.wait()
    values = tok_ref[...].astype(F32).reshape(tokens, feats)
    scaled = (values * gain_ref[...]).astype(BF16)
    lane = lax.broadcasted_iota(jnp.int32, (tokens, LANES), 1)
    tail = split_tail(jnp.sum(values * values, axis=1, keepdims=True), lane)
    part[:, :, 2 * units :] = tail.reshape(nz, tile, LANES).astype(BF16)
    for copy in loads[2:6]:
        copy.wait()
    both = lax.dot_general(
        scaled, gu_v[...].astype(BF16), (((1,), (1,)), ((), ())), preferred_element_type=F32
    )
    part[:, :, : 2 * units] = both.reshape(nz, tile, 2 * units).astype(BF16)

    far = {}
    near = {}
    for i, k in near_peers:
        src = part.at[block(sign[i] * (k + HOP))]
        dst = far_in.at[i, k - 1] if k < HOP else far_in_half.at[i]
        if k == HOP:
            src = part.at[block(sign[i] * (k + HOP)), :, halves[i]]
        far[i, k] = remote(src, dst, rs_send, far_recv.at[i], to_z(sign[i] * k))
        if k < HOP:
            near[i, k] = remote(
                part.at[block(sign[i] * k)],
                near_in.at[i, k - 1],
                rs_send,
                near_recv,
                to_z(sign[i] * k),
            )

    for table in (far, near):
        for i, k in near_peers:
            if (i, k) in table:

                @pl.when(lower(i, k))
                def _():
                    table[i, k].start()

    for i, k in rising:

        @pl.when(jnp.logical_not(lower(i, k)))
        def _():
            pl.semaphore_wait(ready.at[i, k - 1], 1)
            far[i, k].start()
            if k < HOP:
                near[i, k].start()

    def tell(m):
        for n, d in ((0, 1), (1, nx - 1)):
            pl.semaphore_signal(word.at[m, 1 - n], inc=1, device_id=to_x(d), device_id_type=MESH)

    def hear(m):
        for n in (0, 1):
            pl.semaphore_wait(word.at[m, n], 1)

    for n, d in ((1, 1), (2, nx - 1)):

        @pl.when(jnp.logical_not(x_lower(d)))
        def _():
            pl.semaphore_wait(x_ready.at[n], 1)

    tell(0)

    for copy in loads[6:]:
        copy.wait()
    row = lax.broadcasted_iota(jnp.int32, dw_v.shape, 0)
    down = jnp.where(row < units, dw_v[...], 0.0).astype(BF16)

    tile_lane = lax.broadcasted_iota(jnp.int32, (tile, LANES), 1)
    relay = [
        remote(relay_out.at[i], relay_in.at[i], rs_send, relay_recv, to_z(sign[i] * HOP))
        for i in (0, 1)
    ]

    def pass_on(i):
        arrived(part.at[: 2 * HOP - 1, :, halves[0]], far_recv.at[i], mate)
        total = part[block(sign[i] * HOP)].astype(F32)
        for k in range(1, HOP):
            total += far_in[i, k - 1].astype(F32)
        pieces = [total[:, halves[0]], total[:, halves[1]]]
        pieces[i] += far_in_half[i].astype(F32)
        last = pieces[1][:, -LANES:]
        relay_out[i, :, halves[0]] = pieces[0].astype(BF16)
        relay_out[i, :, cols // 2 : cols - LANES] = pieces[1][:, :-LANES].astype(BF16)
        relay_out[i, :, cols - LANES :] = split_tail(
            jnp.sum(last, axis=1, keepdims=True), tile_lane
        ).astype(BF16)
        relay[i].start()

    @pl.when(z >= HOP)
    def _():
        pass_on(0)

    pass_on(1)

    @pl.when(z < HOP)
    def _():
        pass_on(0)

    hear(0)
    tell(1)

    total = part[z].astype(F32)
    arrived(near_in, near_recv, mate)
    for k in range(1, HOP):
        for i in range(2):
            total += near_in[i, k - 1].astype(F32)
    gate_scale = gs_ref[...].reshape(1, units)
    up_scale = us_ref[...].reshape(1, units)
    mixed_scale = jnp.concatenate([gate_scale[:, main:], up_scale[:, main:]], axis=1)
    arrived(relay_in, relay_recv, mate)
    for i in range(2):
        total += relay_in[i].astype(F32)
    square = jnp.sum(total[:, 2 * units :], axis=1, keepdims=True)
    inv = lax.rsqrt(square / width + 1e-06)
    g = total[:, :main] * inv * gate_scale[:, :main]
    u = total[:, main : 2 * main] * inv * up_scale[:, :main]
    both = total[:, 2 * main : 2 * units] * inv * mixed_scale
    swapped = pltpu.roll(both, rest, 1)
    hid[HOP, :, :main] = (g * jax.nn.sigmoid(g) * u).astype(BF16)
    last = both * jax.nn.sigmoid(both) * swapped
    hid[HOP, :, main:] = jnp.where(tile_lane < rest, last, 0.0).astype(BF16)

    hid_cols = hid.shape[2]
    hid_halves = (slice(0, hid_cols // 2), slice(hid_cols // 2, hid_cols))
    spread = {}
    for i, k in near_peers:
        spread[i, k] = remote(
            hid.at[HOP],
            hid.at[(HOP - sign[i] * k) % nz],
            hid_send,
            hid_recv.at[i if k == HOP else 2],
            to_z(sign[i] * k),
        )
        spread[i, k].start()
    for m in range(1, nx // 2 - 2):
        hear(m)
        tell(m + 1)
    onward = {}
    for i in (0, 1):
        arrived(hid.at[0], hid_recv.at[i], mate)
        for k in range(HOP, 0, -1):
            src = hid.at[(HOP - sign[i] * HOP) % nz]
            dst = hid.at[(HOP - sign[i] * (HOP + k)) % nz]
            if k == HOP:
                src = hid.at[(HOP - sign[i] * HOP) % nz, :, hid_halves[i]]
                dst = hid.at[(HOP - sign[i] * (HOP + k)) % nz, :, hid_halves[i]]
            onward[i, k] = remote(src, dst, hid_send, hid_recv.at[3], to_z(sign[i] * k))
            onward[i, k].start()

    groups = 2
    size = nz // groups
    share = size // 2

    def multiply(k):
        arrived(hid.at[: 2 * HOP - 2 + k], hid_recv.at[2 + k], mate)
        rows = hid[k * size : (k + 1) * size].reshape(size * tile, hid.shape[2])
        partial = jnp.dot(rows, down, preferred_element_type=F32)
        pair[k] = partial.reshape(size, tile, feats).astype(BF16)
        copy = remote(
            pair.at[k, pl.ds((1 - core) * share, share)],
            pair_in.at[k],
            pair_send,
            pair_recv.at[k],
            mate,
        )
        copy.start()

    def broadcast(k):
        arrived(pair_in.at[k], pair_recv.at[k], mate)
        own = pair[k, pl.ds(core * share, share)].astype(F32) + pair_in[k].astype(F32)
        chips[k, chip] = own.astype(BF16)
        for d in sorted(range(1, nx), key=lambda d: -min(d, nx - d)):
            to = remote(
                chips.at[k, chip],
                chips.at[k, chip],
                chip_send,
                chip_recv.at[k],
                to_chip(d),
            )
            to.start()

    def finish(k):
        arrived(chips.at[k, : nx - 1], chip_recv.at[k], mate)
        branch = chips[k, 0].astype(F32)
        for j in range(1, nx):
            branch += chips[k, j].astype(F32)
        first = k * size + core * share
        for j in range(share):
            own = tok_ref[block(first + j - HOP)].astype(F32)
            mix[first + j] = 0.5 * own + branch[j] * ds_ref[...]
        rows = pl.ds(first, share)
        mine = mix[rows].reshape(share * tile, feats)
        column = jnp.sum(mine * mine, axis=1, keepdims=True)
        square = jnp.sum(jnp.where(diagonal(first, share), column, 0.0), axis=0, keepdims=True)
        remote(mix.at[rows], mix.at[rows], mix_send, mix_recv, mate).start()
        return square

    def diagonal(first, count):
        place = lax.broadcasted_iota(jnp.int32, (count * tile, tokens), 0)
        place = lax.rem(place + tile * (z + first + nz - HOP), tokens)
        return place == lax.broadcasted_iota(jnp.int32, (count * tile, tokens), 1)

    @pl.when(jnp.logical_not(x_lower(0)))
    def _():
        pl.semaphore_wait(x_ready.at[0], 1)

    multiply(0)
    hear(nx // 2 - 2)
    broadcast(0)
    multiply(1)
    broadcast(1)
    near_squares = finish(0)
    far_squares = finish(1)

    squares[core * nz + z] = near_squares + far_squares
    own = squares.at[core * nz + z]
    order = sorted(range(1, nz), key=lambda d: -min(d, nz - d))
    for d in order:
        for t in range(2):
            peer = {"ra": lax.rem(z + d, nz), "cb": chip * 2 + lax.rem(core + t, 2)}
            remote(own, own, sq_send, sq_recv, peer).start()
    remote(own, own, sq_send, sq_recv, mate).start()
    arrived(mix.at[: 2 * share], mix_recv, mate)
    scaled_mixed = mix[...].reshape(tokens, feats) * og_ref[...]
    arrived(squares.at[: 2 * nz - 1], sq_recv, mate)
    everything = squares[0]
    for j in range(1, 2 * nz):
        everything += squares[j]
    inv_row = lax.rsqrt(everything / width + 1e-06)
    inv_second = jnp.sum(jnp.where(diagonal(0, nz), inv_row, 0.0), axis=1, keepdims=True)
    result = (scaled_mixed * inv_second).reshape(nz, tile, feats).astype(BF16)
    for r in range(nz):
        out_ref[block(r - HOP)] = result[r]

    left(part.at[: 4 * HOP - 1], rs_send, mate)
    left(hid.at[: 4 * HOP - 1], hid_send, mate)
    left(pair.at[0], pair_send, mate)
    left(chips.at[:, : nx - 1], chip_send, mate)
    left(mix.at[: 2 * share], mix_send, mate)
    left(squares.at[: 2 * nz - 1], sq_send, mate)


def solution(mesh):
    nz, nc = mesh.shape["ra"], mesh.shape["cb"]
    nx = nc // 2

    def on_device(tokens, norm_gain, gw, gs, uw, us, dw, ds, og):
        count, feats = tokens.shape
        units = gw.shape[1]
        padded = -(-units // LANES) * LANES
        tile = count // nz
        cols = 2 * units + LANES
        share = nz // 4
        vmem = pl.BlockSpec(memory_space=pltpu.VMEM)
        hbm = pl.BlockSpec(memory_space=pltpu.HBM)
        dma = pltpu.SemaphoreType.DMA
        row = lambda v: v.reshape(1, -1)
        out = pl.pallas_call(
            functools.partial(kernel, nz, nc),
            out_shape=pltpu.VMEM((nz, tile, feats), BF16),
            in_specs=[hbm] * 9,
            out_specs=vmem,
            scratch_shapes=[
                pltpu.VMEM((nz, tile, feats), BF16),
                pltpu.VMEM((1, feats), F32),
                pltpu.VMEM((units,), F32),
                pltpu.VMEM((units,), F32),
                pltpu.VMEM((1, feats), F32),
                pltpu.VMEM((1, feats), F32),
                pltpu.VMEM((2 * units, feats), F32),
                pltpu.VMEM((padded, feats), F32),
                pltpu.VMEM((nz, tile, cols), BF16),
                pltpu.VMEM((2, HOP - 1, tile, cols), BF16),
                pltpu.VMEM((2, tile, cols // 2), BF16),
                pltpu.VMEM((2, HOP - 1, tile, cols), BF16),
                pltpu.VMEM((2, tile, cols), BF16),
                pltpu.VMEM((2, tile, cols), BF16),
                pltpu.VMEM((nz, tile, padded), BF16),
                pltpu.VMEM((2, nz // 2, tile, feats), BF16),
                pltpu.VMEM((2, share, tile, feats), BF16),
                pltpu.VMEM((2, nx, share, tile, feats), BF16),
                pltpu.VMEM((nz, tile, feats), F32),
                pltpu.VMEM((2 * nz, 1, LANES), F32),
                dma((11,)),
                pltpu.SemaphoreType.REGULAR((2, HOP)),
                pltpu.SemaphoreType.REGULAR((3,)),
                pltpu.SemaphoreType.REGULAR((nx // 2 - 1, 2)),
                dma,
                dma((2,)),
                dma,
                dma,
                dma,
                dma((4,)),
                dma,
                dma((2,)),
                dma,
                dma((2,)),
                dma,
                dma,
                dma,
                dma,
            ],
            compiler_params=pltpu.CompilerParams(
                collective_id=0, has_side_effects=True
            ),
        )(
            tokens.reshape(nz, tile, feats),
            row(norm_gain),
            gw.T,
            gs,
            uw.T,
            us,
            dw,
            row(ds),
            row(og),
        )
        return out.reshape(count, feats)

    return jax.shard_map(
        on_device,
        mesh=mesh,
        in_specs=(
            P("grp", "ra"),
            P("ra"),
            P("ra", "cb"),
            P("cb"),
            P("ra", "cb"),
            P("cb"),
            P("cb", "ra"),
            P("ra"),
            P("ra"),
        ),
        out_specs=P("grp", "ra"),
        check_vma=False,
    )
```

```python
import functools

import jax
import jax.numpy as jnp
from jax import lax
from jax.experimental import pallas as pl
from jax.experimental.pallas import tpu as pltpu
from jax.sharding import PartitionSpec as P

MESH = pl.DeviceIdType.MESH
LANES = 128
F32 = jnp.float32
BF16 = jnp.bfloat16
HOP = 4


def remote(src, dst, send_sem, recv_sem, peer):
    return pltpu.make_async_remote_copy(
        src_ref=src,
        dst_ref=dst,
        send_sem=send_sem,
        recv_sem=recv_sem,
        device_id=peer,
        device_id_type=MESH,
    )


def arrived(ref, sem, peer):
    remote(ref, ref, sem, sem, peer).wait_recv()


def left(ref, sem, peer):
    remote(ref, ref, sem, sem, peer).wait_send()


def split_tail(column, lane):
    high = column.astype(BF16).astype(F32)
    return jnp.where(lane == 0, high, jnp.where(lane == 1, column - high, 0.0))


def kernel(
    nz,
    nc,
    tok_hbm,
    gain_hbm,
    gw_ref,
    gs_hbm,
    uw_ref,
    us_hbm,
    dw_ref,
    ds_hbm,
    og_hbm,
    out_ref,
    tok_ref,
    gain_ref,
    gs_ref,
    us_ref,
    ds_ref,
    og_ref,
    gu_v,
    dw_v,
    part,
    far_in,
    far_in_half,
    near_in,
    relay_out,
    relay_in,
    hid,
    pair,
    pair_in,
    chips,
    mix,
    squares,
    load_sem,
    ready,
    x_ready,
    word,
    rs_send,
    far_recv,
    near_recv,
    relay_recv,
    hid_send,
    hid_recv,
    pair_send,
    pair_recv,
    chip_send,
    chip_recv,
    mix_send,
    mix_recv,
    sq_send,
    sq_recv,
):
    z = lax.axis_index("ra")
    cb = lax.axis_index("cb")
    chip = cb // 2
    core = cb % 2
    nx = nc // 2
    tile, feats = tok_ref.shape[1:]
    tokens = nz * tile
    units = gw_ref.shape[0]
    main = units // LANES * LANES
    rest = units - main
    width = feats * nz
    cols = part.shape[2]
    halves = (slice(0, cols // 2), slice(cols // 2, cols))

    def to_z(d):
        return {"ra": lax.rem(z + d + nz, nz)}

    def to_chip(d):
        return {"cb": lax.rem(chip + d, nx) * 2 + core}

    mate = {"cb": chip * 2 + 1 - core}

    def block(d):
        return lax.rem(z + d + 2 * nz, nz)

    near_peers = [(i, k) for k in range(HOP, 0, -1) for i in (0, 1)]
    rising = [(0, k) for k in range(1, HOP + 1)] + [(1, k) for k in range(HOP, 0, -1)]
    sign = (1, -1)

    def lower(i, k):
        return block(sign[i] * k) < z

    def turn(c):
        return jnp.minimum(c, nx - c) * nx + c

    def x_lower(d):
        return core == 0 if d == 0 else turn(lax.rem(chip + d, nx)) < turn(chip)

    def to_x(d):
        return mate if d == 0 else to_chip(d)

    beside = (0, 1, nx - 1)
    barrier = pltpu.get_barrier_semaphore()
    for i, k in near_peers:

        @pl.when(jnp.logical_not(lower(i, k)))
        def _():
            pl.semaphore_signal(barrier, inc=1, device_id=to_z(sign[i] * k), device_id_type=MESH)

    for d in beside:

        @pl.when(jnp.logical_not(x_lower(d)))
        def _():
            pl.semaphore_signal(barrier, inc=1, device_id=to_x(d), device_id_type=MESH)

    loads = [
        pltpu.make_async_copy(src, dst, load_sem.at[k])
        for k, (src, dst) in enumerate(
            [
                (tok_hbm, tok_ref),
                (gain_hbm, gain_ref),
                (gw_ref.at[:main], gu_v.at[:main]),
                (uw_ref.at[:main], gu_v.at[main : 2 * main]),
                (gw_ref.at[main:], gu_v.at[2 * main : 2 * main + rest]),
                (uw_ref.at[main:], gu_v.at[2 * main + rest :]),
                (gs_hbm, gs_ref),
                (us_hbm, us_ref),
                (dw_ref, dw_v.at[:units]),
                (ds_hbm, ds_ref),
                (og_hbm, og_ref),
            ]
        )
    ]
    for copy in loads:
        copy.start()

    count = sum(jnp.where(lower(i, k), 1, 0) for i, k in near_peers)
    count += sum(jnp.where(x_lower(d), 1, 0) for d in beside)

    @pl.when(count > 0)
    def _():
        pl.semaphore_wait(barrier, count)

    for i, k in near_peers:

        @pl.when(lower(i, k))
        def _():
            pl.semaphore_signal(
                ready.at[1 - i, k - 1], inc=1, device_id=to_z(sign[i] * k), device_id_type=MESH
            )

    for n, d in enumerate(beside):

        @pl.when(x_lower(d))
        def _():
            pl.semaphore_signal(
                x_ready.at[(3 - n) % 3], inc=1, device_id=to_x(d), device_id_type=MESH
            )

    for copy in loads[:2]:
        copy.wait()
    values = tok_ref[...].astype(F32).reshape(tokens, feats)
    scaled = (values * gain_ref[...]).astype(BF16)
    lane = lax.broadcasted_iota(jnp.int32, (tokens, LANES), 1)
    tail = split_tail(jnp.sum(values * values, axis=1, keepdims=True), lane)
    part[:, :, 2 * units :] = tail.reshape(nz, tile, LANES).astype(BF16)
    for copy in loads[2:6]:
        copy.wait()
    both = lax.dot_general(
        scaled, gu_v[...].astype(BF16), (((1,), (1,)), ((), ())), preferred_element_type=F32
    )
    part[:, :, : 2 * units] = both.reshape(nz, tile, 2 * units).astype(BF16)

    far = {}
    near = {}
    for i, k in near_peers:
        src = part.at[block(sign[i] * (k + HOP))]
        dst = far_in.at[i, k - 1] if k < HOP else far_in_half.at[i]
        if k == HOP:
            src = part.at[block(sign[i] * (k + HOP)), :, halves[i]]
        far[i, k] = remote(src, dst, rs_send, far_recv.at[i], to_z(sign[i] * k))
        if k < HOP:
            near[i, k] = remote(
                part.at[block(sign[i] * k)],
                near_in.at[i, k - 1],
                rs_send,
                near_recv,
                to_z(sign[i] * k),
            )

    for table in (far, near):
        for i, k in near_peers:
            if (i, k) in table:

                @pl.when(lower(i, k))
                def _():
                    table[i, k].start()

    for i, k in rising:

        @pl.when(jnp.logical_not(lower(i, k)))
        def _():
            pl.semaphore_wait(ready.at[i, k - 1], 1)
            far[i, k].start()

    def tell(m):
        for n, d in ((0, 1), (1, nx - 1)):
            pl.semaphore_signal(word.at[m, 1 - n], inc=1, device_id=to_x(d), device_id_type=MESH)

    def hear(m):
        for n in (0, 1):
            pl.semaphore_wait(word.at[m, n], 1)

    for n, d in ((1, 1), (2, nx - 1)):

        @pl.when(jnp.logical_not(x_lower(d)))
        def _():
            pl.semaphore_wait(x_ready.at[n], 1)

    tell(0)

    for copy in loads[6:]:
        copy.wait()
    row = lax.broadcasted_iota(jnp.int32, dw_v.shape, 0)
    down = jnp.where(row < units, dw_v[...], 0.0).astype(BF16)

    tile_lane = lax.broadcasted_iota(jnp.int32, (tile, LANES), 1)
    relay = [
        remote(relay_out.at[i], relay_in.at[i], rs_send, relay_recv, to_z(sign[i] * HOP))
        for i in (0, 1)
    ]

    def pass_on(i):
        arrived(part.at[: 2 * HOP - 1, :, halves[0]], far_recv.at[i], mate)
        total = part[block(sign[i] * HOP)].astype(F32)
        for k in range(1, HOP):
            total += far_in[i, k - 1].astype(F32)
        pieces = [total[:, halves[0]], total[:, halves[1]]]
        pieces[i] += far_in_half[i].astype(F32)
        last = pieces[1][:, -LANES:]
        relay_out[i, :, halves[0]] = pieces[0].astype(BF16)
        relay_out[i, :, cols // 2 : cols - LANES] = pieces[1][:, :-LANES].astype(BF16)
        relay_out[i, :, cols - LANES :] = split_tail(
            jnp.sum(last, axis=1, keepdims=True), tile_lane
        ).astype(BF16)
        relay[i].start()

    @pl.when(z >= HOP)
    def _():
        pass_on(0)

    pass_on(1)

    for i, k in rising:
        if k < HOP:

            @pl.when(jnp.logical_not(lower(i, k)))
            def _():
                near[i, k].start()

    @pl.when(z < HOP)
    def _():
        pass_on(0)

    hear(0)
    tell(1)

    total = part[z].astype(F32)
    arrived(near_in, near_recv, mate)
    for k in range(1, HOP):
        for i in range(2):
            total += near_in[i, k - 1].astype(F32)
    gate_scale = gs_ref[...].reshape(1, units)
    up_scale = us_ref[...].reshape(1, units)
    mixed_scale = jnp.concatenate([gate_scale[:, main:], up_scale[:, main:]], axis=1)
    arrived(relay_in, relay_recv, mate)
    for i in range(2):
        total += relay_in[i].astype(F32)
    square = jnp.sum(total[:, 2 * units :], axis=1, keepdims=True)
    inv = lax.rsqrt(square / width + 1e-06)
    g = total[:, :main] * inv * gate_scale[:, :main]
    u = total[:, main : 2 * main] * inv * up_scale[:, :main]
    both = total[:, 2 * main : 2 * units] * inv * mixed_scale
    swapped = pltpu.roll(both, rest, 1)
    hid[HOP, :, :main] = (g * jax.nn.sigmoid(g) * u).astype(BF16)
    last = both * jax.nn.sigmoid(both) * swapped
    hid[HOP, :, main:] = jnp.where(tile_lane < rest, last, 0.0).astype(BF16)

    direct = nz // 2 - 1

    def slot(d):
        return (HOP - d) % nz

    for d in (nz // 2, direct, -direct):
        remote(hid.at[HOP], hid.at[slot(d)], hid_send, hid_recv.at[3], to_z(d)).start()
    for i, k in near_peers:
        d = sign[i] * k
        sem = hid_recv.at[i if k == HOP else 2]
        remote(hid.at[HOP], hid.at[slot(d)], hid_send, sem, to_z(d)).start()
    for m in range(1, nx // 2 - 2):
        hear(m)
        tell(m + 1)

    def forward(i):
        arrived(hid.at[0], hid_recv.at[i], mate)
        src = hid.at[slot(sign[i] * HOP)]
        for k in range(direct - HOP - 1, 0, -1):
            dst = hid.at[slot(sign[i] * (HOP + k))]
            remote(src, dst, hid_send, hid_recv.at[3], to_z(sign[i] * k)).start()

    @pl.when(z >= nz // 2)
    def _():
        forward(0)

    forward(1)

    @pl.when(z < nz // 2)
    def _():
        forward(0)

    groups = 2
    size = nz // groups
    share = size // 2

    def multiply(k):
        arrived(hid.at[: 2 * HOP - 2 + k], hid_recv.at[2 + k], mate)
        rows = hid[k * size : (k + 1) * size].reshape(size * tile, hid.shape[2])
        partial = jnp.dot(rows, down, preferred_element_type=F32)
        pair[k] = partial.reshape(size, tile, feats).astype(BF16)
        copy = remote(
            pair.at[k, pl.ds((1 - core) * share, share)],
            pair_in.at[k],
            pair_send,
            pair_recv.at[k],
            mate,
        )
        copy.start()

    def broadcast(k):
        arrived(pair_in.at[k], pair_recv.at[k], mate)
        own = pair[k, pl.ds(core * share, share)].astype(F32) + pair_in[k].astype(F32)
        chips[k, chip] = own.astype(BF16)
        for d in sorted(range(1, nx), key=lambda d: -min(d, nx - d)):
            to = remote(
                chips.at[k, chip],
                chips.at[k, chip],
                chip_send,
                chip_recv.at[k],
                to_chip(d),
            )
            to.start()

    def finish(k):
        arrived(chips.at[k, : nx - 1], chip_recv.at[k], mate)
        branch = chips[k, 0].astype(F32)
        for j in range(1, nx):
            branch += chips[k, j].astype(F32)
        first = k * size + core * share
        for j in range(share):
            own = tok_ref[block(first + j - HOP)].astype(F32)
            mix[first + j] = 0.5 * own + branch[j] * ds_ref[...]
        rows = pl.ds(first, share)
        mine = mix[rows].reshape(share * tile, feats)
        column = jnp.sum(mine * mine, axis=1, keepdims=True)
        square = jnp.sum(jnp.where(diagonal(first, share), column, 0.0), axis=0, keepdims=True)
        remote(mix.at[rows], mix.at[rows], mix_send, mix_recv, mate).start()
        return square

    def diagonal(first, count):
        place = lax.broadcasted_iota(jnp.int32, (count * tile, tokens), 0)
        place = lax.rem(place + tile * (z + first + nz - HOP), tokens)
        return place == lax.broadcasted_iota(jnp.int32, (count * tile, tokens), 1)

    @pl.when(jnp.logical_not(x_lower(0)))
    def _():
        pl.semaphore_wait(x_ready.at[0], 1)

    multiply(0)
    hear(nx // 2 - 2)
    broadcast(0)
    multiply(1)
    broadcast(1)
    near_squares = finish(0)
    far_squares = finish(1)

    squares[core * nz + z] = near_squares + far_squares
    own = squares.at[core * nz + z]
    order = sorted(range(1, nz), key=lambda d: -min(d, nz - d))
    for d in order:
        for t in range(2):
            peer = {"ra": lax.rem(z + d, nz), "cb": chip * 2 + lax.rem(core + t, 2)}
            remote(own, own, sq_send, sq_recv, peer).start()
    remote(own, own, sq_send, sq_recv, mate).start()
    arrived(mix.at[: 2 * share], mix_recv, mate)
    scaled_mixed = mix[...].reshape(tokens, feats) * og_ref[...]
    arrived(squares.at[: 2 * nz - 1], sq_recv, mate)
    everything = squares[0]
    for j in range(1, 2 * nz):
        everything += squares[j]
    inv_row = lax.rsqrt(everything / width + 1e-06)
    inv_second = jnp.sum(jnp.where(diagonal(0, nz), inv_row, 0.0), axis=1, keepdims=True)
    result = (scaled_mixed * inv_second).reshape(nz, tile, feats).astype(BF16)
    for r in range(nz):
        out_ref[block(r - HOP)] = result[r]

    left(part.at[: 4 * HOP - 1], rs_send, mate)
    left(hid.at[: 4 * HOP - 1], hid_send, mate)
    left(pair.at[0], pair_send, mate)
    left(chips.at[:, : nx - 1], chip_send, mate)
    left(mix.at[: 2 * share], mix_send, mate)
    left(squares.at[: 2 * nz - 1], sq_send, mate)


def solution(mesh):
    nz, nc = mesh.shape["ra"], mesh.shape["cb"]
    nx = nc // 2

    def on_device(tokens, norm_gain, gw, gs, uw, us, dw, ds, og):
        count, feats = tokens.shape
        units = gw.shape[1]
        padded = -(-units // LANES) * LANES
        tile = count // nz
        cols = 2 * units + LANES
        share = nz // 4
        vmem = pl.BlockSpec(memory_space=pltpu.VMEM)
        hbm = pl.BlockSpec(memory_space=pltpu.HBM)
        dma = pltpu.SemaphoreType.DMA
        row = lambda v: v.reshape(1, -1)
        out = pl.pallas_call(
            functools.partial(kernel, nz, nc),
            out_shape=pltpu.VMEM((nz, tile, feats), BF16),
            in_specs=[hbm] * 9,
            out_specs=vmem,
            scratch_shapes=[
                pltpu.VMEM((nz, tile, feats), BF16),
                pltpu.VMEM((1, feats), F32),
                pltpu.VMEM((units,), F32),
                pltpu.VMEM((units,), F32),
                pltpu.VMEM((1, feats), F32),
                pltpu.VMEM((1, feats), F32),
                pltpu.VMEM((2 * units, feats), F32),
                pltpu.VMEM((padded, feats), F32),
                pltpu.VMEM((nz, tile, cols), BF16),
                pltpu.VMEM((2, HOP - 1, tile, cols), BF16),
                pltpu.VMEM((2, tile, cols // 2), BF16),
                pltpu.VMEM((2, HOP - 1, tile, cols), BF16),
                pltpu.VMEM((2, tile, cols), BF16),
                pltpu.VMEM((2, tile, cols), BF16),
                pltpu.VMEM((nz, tile, padded), BF16),
                pltpu.VMEM((2, nz // 2, tile, feats), BF16),
                pltpu.VMEM((2, share, tile, feats), BF16),
                pltpu.VMEM((2, nx, share, tile, feats), BF16),
                pltpu.VMEM((nz, tile, feats), F32),
                pltpu.VMEM((2 * nz, 1, LANES), F32),
                dma((11,)),
                pltpu.SemaphoreType.REGULAR((2, HOP)),
                pltpu.SemaphoreType.REGULAR((3,)),
                pltpu.SemaphoreType.REGULAR((nx // 2 - 1, 2)),
                dma,
                dma((2,)),
                dma,
                dma,
                dma,
                dma((4,)),
                dma,
                dma((2,)),
                dma,
                dma((2,)),
                dma,
                dma,
                dma,
                dma,
            ],
            compiler_params=pltpu.CompilerParams(
                collective_id=0, has_side_effects=True
            ),
        )(
            tokens.reshape(nz, tile, feats),
            row(norm_gain),
            gw.T,
            gs,
            uw.T,
            us,
            dw,
            row(ds),
            row(og),
        )
        return out.reshape(count, feats)

    return jax.shard_map(
        on_device,
        mesh=mesh,
        in_specs=(
            P("grp", "ra"),
            P("ra"),
            P("ra", "cb"),
            P("cb"),
            P("ra", "cb"),
            P("cb"),
            P("cb", "ra"),
            P("ra"),
            P("ra"),
        ),
        out_specs=P("grp", "ra"),
        check_vma=False,
    )
```

```python
import functools

import jax
import jax.numpy as jnp
from jax import lax
from jax.experimental import pallas as pl
from jax.experimental.pallas import tpu as pltpu
from jax.sharding import PartitionSpec as P

MESH = pl.DeviceIdType.MESH
LANES = 128
F32 = jnp.float32
BF16 = jnp.bfloat16
HOP = 4


def remote(src, dst, send_sem, recv_sem, peer):
    return pltpu.make_async_remote_copy(
        src_ref=src,
        dst_ref=dst,
        send_sem=send_sem,
        recv_sem=recv_sem,
        device_id=peer,
        device_id_type=MESH,
    )


def arrived(ref, sem, peer):
    remote(ref, ref, sem, sem, peer).wait_recv()


def left(ref, sem, peer):
    remote(ref, ref, sem, sem, peer).wait_send()


def split_tail(column, lane):
    high = column.astype(BF16).astype(F32)
    return jnp.where(lane == 0, high, jnp.where(lane == 1, column - high, 0.0))


def kernel(
    nz,
    nc,
    tok_hbm,
    gain_hbm,
    gw_ref,
    gs_hbm,
    uw_ref,
    us_hbm,
    dw_ref,
    ds_hbm,
    og_hbm,
    out_ref,
    tok_ref,
    gain_ref,
    gs_ref,
    us_ref,
    ds_ref,
    og_ref,
    gu_v,
    dw_v,
    part,
    far_in,
    far_in_half,
    near_in,
    relay_out,
    relay_in,
    straight_in,
    straight_half,
    extra,
    hid,
    pair,
    pair_in,
    chips,
    mix,
    squares,
    load_sem,
    ready,
    x_ready,
    word,
    late_ready,
    straight_recv,
    rs_send,
    far_recv,
    near_recv,
    relay_recv,
    hid_send,
    hid_recv,
    pair_send,
    pair_recv,
    chip_send,
    chip_recv,
    mix_send,
    mix_recv,
    sq_send,
    sq_recv,
):
    z = lax.axis_index("ra")
    cb = lax.axis_index("cb")
    chip = cb // 2
    core = cb % 2
    nx = nc // 2
    tile, feats = tok_ref.shape[1:]
    tokens = nz * tile
    units = gw_ref.shape[0]
    main = units // LANES * LANES
    rest = units - main
    width = feats * nz
    cols = part.shape[2]
    halves = (slice(0, cols // 2), slice(cols // 2, cols))

    def to_z(d):
        return {"ra": lax.rem(z + d + nz, nz)}

    def to_chip(d):
        return {"cb": lax.rem(chip + d, nx) * 2 + core}

    mate = {"cb": chip * 2 + 1 - core}

    def block(d):
        return lax.rem(z + d + 2 * nz, nz)

    near_peers = [(i, k) for k in range(HOP, 0, -1) for i in (0, 1)]
    rising = [(0, k) for k in range(1, HOP + 1)] + [(1, k) for k in range(HOP, 0, -1)]
    sign = (1, -1)

    def lower(i, k):
        return block(sign[i] * k) < z

    last = nz - 1
    first, late = HOP - 1, nz - 1 - HOP

    def at_z(index):
        return {"ra": jnp.int32(index)}

    def is_last(i, k):
        return block(sign[i] * k) == last

    def turn(c):
        return jnp.minimum(c, nx - c) * nx + c

    def x_lower(d):
        return core == 0 if d == 0 else turn(lax.rem(chip + d, nx)) < turn(chip)

    def to_x(d):
        return mate if d == 0 else to_chip(d)

    beside = (0, 1, nx - 1)
    barrier = pltpu.get_barrier_semaphore()
    for i, k in near_peers:

        @pl.when(jnp.logical_not(lower(i, k)))
        def _():
            pl.semaphore_signal(barrier, inc=1, device_id=to_z(sign[i] * k), device_id_type=MESH)

    @pl.when(z == first)
    def _():
        for k in range(1, HOP + 1):
            pl.semaphore_signal(barrier, inc=1, device_id=at_z(last - k), device_id_type=MESH)

    @pl.when(z < first)
    def _():
        pl.semaphore_signal(barrier, inc=1, device_id=at_z(late), device_id_type=MESH)

    for d in beside:

        @pl.when(jnp.logical_not(x_lower(d)))
        def _():
            pl.semaphore_signal(barrier, inc=1, device_id=to_x(d), device_id_type=MESH)

    loads = [
        pltpu.make_async_copy(src, dst, load_sem.at[k])
        for k, (src, dst) in enumerate(
            [
                (tok_hbm, tok_ref),
                (gain_hbm, gain_ref),
                (gw_ref.at[:main], gu_v.at[:main]),
                (uw_ref.at[:main], gu_v.at[main : 2 * main]),
                (gw_ref.at[main:], gu_v.at[2 * main : 2 * main + rest]),
                (uw_ref.at[main:], gu_v.at[2 * main + rest :]),
                (gs_hbm, gs_ref),
                (us_hbm, us_ref),
                (dw_ref, dw_v.at[:units]),
                (ds_hbm, ds_ref),
                (og_hbm, og_ref),
            ]
        )
    ]
    for copy in loads:
        copy.start()

    count = sum(jnp.where(lower(i, k), 1, 0) for i, k in near_peers)
    count += sum(jnp.where(x_lower(d), 1, 0) for d in beside)
    count += jnp.where(z >= late, jnp.where(z < last, 1, 0), 0) + jnp.where(z == late, first, 0)

    @pl.when(count > 0)
    def _():
        pl.semaphore_wait(barrier, count)

    for i, k in near_peers:

        @pl.when(lower(i, k))
        def _():
            pl.semaphore_signal(
                ready.at[1 - i, k - 1], inc=1, device_id=to_z(sign[i] * k), device_id_type=MESH
            )

    @pl.when(z == late)
    def _():
        for k in range(HOP):
            pl.semaphore_signal(late_ready, inc=1, device_id=at_z(k), device_id_type=MESH)

    for n, d in enumerate(beside):

        @pl.when(x_lower(d))
        def _():
            pl.semaphore_signal(
                x_ready.at[(3 - n) % 3], inc=1, device_id=to_x(d), device_id_type=MESH
            )

    for copy in loads[:2]:
        copy.wait()
    values = tok_ref[...].astype(F32).reshape(tokens, feats)
    scaled = (values * gain_ref[...]).astype(BF16)
    lane = lax.broadcasted_iota(jnp.int32, (tokens, LANES), 1)
    tail = split_tail(jnp.sum(values * values, axis=1, keepdims=True), lane)
    part[:, :, 2 * units :] = tail.reshape(nz, tile, LANES).astype(BF16)
    for copy in loads[2:6]:
        copy.wait()
    both = lax.dot_general(
        scaled, gu_v[...].astype(BF16), (((1,), (1,)), ((), ())), preferred_element_type=F32
    )
    part[:, :, : 2 * units] = both.reshape(nz, tile, 2 * units).astype(BF16)

    far = {}
    near = {}
    for i, k in near_peers:
        src = part.at[block(sign[i] * (k + HOP))]
        dst = far_in.at[i, k - 1] if k < HOP else far_in_half.at[i]
        if k == HOP:
            src = part.at[block(sign[i] * (k + HOP)), :, halves[i]]
        far[i, k] = remote(src, dst, rs_send, far_recv.at[i], to_z(sign[i] * k))
        if k < HOP:
            near[i, k] = remote(
                part.at[block(sign[i] * k)],
                near_in.at[i, k - 1],
                rs_send,
                near_recv,
                to_z(sign[i] * k),
            )

    straight = {}
    for i, k in near_peers:
        src = part.at[block(sign[i] * (k + HOP))]
        dst = straight_in.at[k - 1] if k < HOP else straight_half
        if k == HOP:
            src = part.at[block(sign[i] * (k + HOP)), :, halves[i]]
        straight[i, k] = remote(src, dst, rs_send, straight_recv, to_z(sign[i] * (k + HOP)))

    for k in range(HOP, 0, -1):

        @pl.when(z == last - k)
        def _():
            straight[0, k].start()

    for table in (far, near):
        for i, k in near_peers:
            if (i, k) in table:

                @pl.when(lower(i, k))
                def _():
                    table[i, k].start()

    for i, k in rising:
        if (i, k) == (1, HOP):
            for j in range(HOP, 0, -1):

                @pl.when(z == j - 1)
                def _():
                    pl.semaphore_wait(late_ready, 1)
                    straight[1, j].start()

        @pl.when(jnp.logical_not(lower(i, k)))
        def _():
            pl.semaphore_wait(ready.at[i, k - 1], 1)

            @pl.when(jnp.logical_not(is_last(i, k)))
            def _():
                far[i, k].start()
                if k < HOP:
                    near[i, k].start()

    def tell(m):
        for n, d in ((0, 1), (1, nx - 1)):
            pl.semaphore_signal(word.at[m, 1 - n], inc=1, device_id=to_x(d), device_id_type=MESH)

    def hear(m):
        for n in (0, 1):
            pl.semaphore_wait(word.at[m, n], 1)

    for n, d in ((1, 1), (2, nx - 1)):

        @pl.when(jnp.logical_not(x_lower(d)))
        def _():
            pl.semaphore_wait(x_ready.at[n], 1)

    tell(0)

    for copy in loads[6:]:
        copy.wait()
    row = lax.broadcasted_iota(jnp.int32, dw_v.shape, 0)
    down = jnp.where(row < units, dw_v[...], 0.0).astype(BF16)

    tile_lane = lax.broadcasted_iota(jnp.int32, (tile, LANES), 1)
    relay = [
        remote(relay_out.at[i], relay_in.at[i], rs_send, relay_recv, to_z(sign[i] * HOP))
        for i in (0, 1)
    ]

    def pass_on(i):
        @pl.when(z == last)
        def _():
            remote(
                part.at[block(sign[i] * HOP)], relay_in.at[i], rs_send, relay_recv, to_z(sign[i] * HOP)
            ).start()

        @pl.when(z < last)
        def _():
            arrived(part.at[: 2 * HOP - 1, :, halves[0]], far_recv.at[i], mate)
            total = part[block(sign[i] * HOP)].astype(F32)
            for k in range(1, HOP):
                total += far_in[i, k - 1].astype(F32)
            pieces = [total[:, halves[0]], total[:, halves[1]]]
            pieces[i] += far_in_half[i].astype(F32)
            last = pieces[1][:, -LANES:]
            relay_out[i, :, halves[0]] = pieces[0].astype(BF16)
            relay_out[i, :, cols // 2 : cols - LANES] = pieces[1][:, :-LANES].astype(BF16)
            relay_out[i, :, cols - LANES :] = split_tail(
                jnp.sum(last, axis=1, keepdims=True), tile_lane
            ).astype(BF16)
            relay[i].start()

    @pl.when(z >= HOP)
    def _():
        pass_on(0)

    pass_on(1)

    for i, k in rising:
        if k < HOP:

            @pl.when(is_last(i, k))
            def _():
                near[i, k].start()

    @pl.when(z < HOP)
    def _():
        pass_on(0)

    hear(0)
    tell(1)

    total = part[z].astype(F32)
    arrived(near_in, near_recv, mate)
    for k in range(1, HOP):
        for i in range(2):
            total += near_in[i, k - 1].astype(F32)
    gate_scale = gs_ref[...].reshape(1, units)
    up_scale = us_ref[...].reshape(1, units)
    mixed_scale = jnp.concatenate([gate_scale[:, main:], up_scale[:, main:]], axis=1)
    extra[...] = jnp.zeros_like(extra)
    for i, target in ((0, first), (1, late)):

        @pl.when(z == target)
        def _():
            arrived(part.at[: 2 * HOP - 1, :, halves[0]], straight_recv, mate)
            rest_of = straight_in[0].astype(F32)
            for k in range(1, HOP - 1):
                rest_of += straight_in[k].astype(F32)
            extra[...] = rest_of
            extra[:, halves[i]] += straight_half[...].astype(F32)

    arrived(relay_in, relay_recv, mate)
    total += extra[...]
    for i in range(2):
        total += relay_in[i].astype(F32)
    square = jnp.sum(total[:, 2 * units :], axis=1, keepdims=True)
    inv = lax.rsqrt(square / width + 1e-06)
    g = total[:, :main] * inv * gate_scale[:, :main]
    u = total[:, main : 2 * main] * inv * up_scale[:, :main]
    both = total[:, 2 * main : 2 * units] * inv * mixed_scale
    swapped = pltpu.roll(both, rest, 1)
    hid[HOP, :, :main] = (g * jax.nn.sigmoid(g) * u).astype(BF16)
    last = both * jax.nn.sigmoid(both) * swapped
    hid[HOP, :, main:] = jnp.where(tile_lane < rest, last, 0.0).astype(BF16)

    direct = nz // 2 - 1

    def slot(d):
        return (HOP - d) % nz

    for d in (nz // 2, direct, -direct):
        remote(hid.at[HOP], hid.at[slot(d)], hid_send, hid_recv.at[3], to_z(d)).start()
    for i, k in near_peers:
        d = sign[i] * k
        sem = hid_recv.at[i if k == HOP else 2]
        remote(hid.at[HOP], hid.at[slot(d)], hid_send, sem, to_z(d)).start()
    for m in range(1, nx // 2 - 2):
        hear(m)
        tell(m + 1)

    def forward(i):
        arrived(hid.at[0], hid_recv.at[i], mate)
        src = hid.at[slot(sign[i] * HOP)]
        for k in range(direct - HOP - 1, 0, -1):
            dst = hid.at[slot(sign[i] * (HOP + k))]
            remote(src, dst, hid_send, hid_recv.at[3], to_z(sign[i] * k)).start()

    @pl.when(z >= nz // 2)
    def _():
        forward(0)

    forward(1)

    @pl.when(z < nz // 2)
    def _():
        forward(0)

    groups = 2
    size = nz // groups
    share = size // 2

    def multiply(k):
        arrived(hid.at[: 2 * HOP - 2 + k], hid_recv.at[2 + k], mate)
        rows = hid[k * size : (k + 1) * size].reshape(size * tile, hid.shape[2])
        partial = jnp.dot(rows, down, preferred_element_type=F32)
        pair[k] = partial.reshape(size, tile, feats).astype(BF16)
        copy = remote(
            pair.at[k, pl.ds((1 - core) * share, share)],
            pair_in.at[k],
            pair_send,
            pair_recv.at[k],
            mate,
        )
        copy.start()

    def broadcast(k):
        arrived(pair_in.at[k], pair_recv.at[k], mate)
        own = pair[k, pl.ds(core * share, share)].astype(F32) + pair_in[k].astype(F32)
        chips[k, chip] = own.astype(BF16)
        for d in sorted(range(1, nx), key=lambda d: -min(d, nx - d)):
            to = remote(
                chips.at[k, chip],
                chips.at[k, chip],
                chip_send,
                chip_recv.at[k],
                to_chip(d),
            )
            to.start()

    def finish(k):
        arrived(chips.at[k, : nx - 1], chip_recv.at[k], mate)
        branch = chips[k, 0].astype(F32)
        for j in range(1, nx):
            branch += chips[k, j].astype(F32)
        first = k * size + core * share
        for j in range(share):
            own = tok_ref[block(first + j - HOP)].astype(F32)
            mix[first + j] = 0.5 * own + branch[j] * ds_ref[...]
        rows = pl.ds(first, share)
        mine = mix[rows].reshape(share * tile, feats)
        column = jnp.sum(mine * mine, axis=1, keepdims=True)
        square = jnp.sum(jnp.where(diagonal(first, share), column, 0.0), axis=0, keepdims=True)
        remote(mix.at[rows], mix.at[rows], mix_send, mix_recv, mate).start()
        return square

    def diagonal(first, count):
        place = lax.broadcasted_iota(jnp.int32, (count * tile, tokens), 0)
        place = lax.rem(place + tile * (z + first + nz - HOP), tokens)
        return place == lax.broadcasted_iota(jnp.int32, (count * tile, tokens), 1)

    @pl.when(jnp.logical_not(x_lower(0)))
    def _():
        pl.semaphore_wait(x_ready.at[0], 1)

    multiply(0)
    hear(nx // 2 - 2)
    broadcast(0)
    multiply(1)
    broadcast(1)
    near_squares = finish(0)
    far_squares = finish(1)

    squares[core * nz + z] = near_squares + far_squares
    own = squares.at[core * nz + z]
    order = sorted(range(1, nz), key=lambda d: -min(d, nz - d))
    for d in order:
        for t in range(2):
            peer = {"ra": lax.rem(z + d, nz), "cb": chip * 2 + lax.rem(core + t, 2)}
            remote(own, own, sq_send, sq_recv, peer).start()
    remote(own, own, sq_send, sq_recv, mate).start()
    arrived(mix.at[: 2 * share], mix_recv, mate)
    scaled_mixed = mix[...].reshape(tokens, feats) * og_ref[...]
    arrived(squares.at[: 2 * nz - 1], sq_recv, mate)
    everything = squares[0]
    for j in range(1, 2 * nz):
        everything += squares[j]
    inv_row = lax.rsqrt(everything / width + 1e-06)
    inv_second = jnp.sum(jnp.where(diagonal(0, nz), inv_row, 0.0), axis=1, keepdims=True)
    result = (scaled_mixed * inv_second).reshape(nz, tile, feats).astype(BF16)
    for r in range(nz):
        out_ref[block(r - HOP)] = result[r]

    left(part.at[: 4 * HOP - 1], rs_send, mate)
    left(hid.at[: 4 * HOP - 1], hid_send, mate)
    left(pair.at[0], pair_send, mate)
    left(chips.at[:, : nx - 1], chip_send, mate)
    left(mix.at[: 2 * share], mix_send, mate)
    left(squares.at[: 2 * nz - 1], sq_send, mate)


def solution(mesh):
    nz, nc = mesh.shape["ra"], mesh.shape["cb"]
    nx = nc // 2

    def on_device(tokens, norm_gain, gw, gs, uw, us, dw, ds, og):
        count, feats = tokens.shape
        units = gw.shape[1]
        padded = -(-units // LANES) * LANES
        tile = count // nz
        cols = 2 * units + LANES
        share = nz // 4
        vmem = pl.BlockSpec(memory_space=pltpu.VMEM)
        hbm = pl.BlockSpec(memory_space=pltpu.HBM)
        dma = pltpu.SemaphoreType.DMA
        row = lambda v: v.reshape(1, -1)
        out = pl.pallas_call(
            functools.partial(kernel, nz, nc),
            out_shape=pltpu.VMEM((nz, tile, feats), BF16),
            in_specs=[hbm] * 9,
            out_specs=vmem,
            scratch_shapes=[
                pltpu.VMEM((nz, tile, feats), BF16),
                pltpu.VMEM((1, feats), F32),
                pltpu.VMEM((units,), F32),
                pltpu.VMEM((units,), F32),
                pltpu.VMEM((1, feats), F32),
                pltpu.VMEM((1, feats), F32),
                pltpu.VMEM((2 * units, feats), F32),
                pltpu.VMEM((padded, feats), F32),
                pltpu.VMEM((nz, tile, cols), BF16),
                pltpu.VMEM((2, HOP - 1, tile, cols), BF16),
                pltpu.VMEM((2, tile, cols // 2), BF16),
                pltpu.VMEM((2, HOP - 1, tile, cols), BF16),
                pltpu.VMEM((2, tile, cols), BF16),
                pltpu.VMEM((2, tile, cols), BF16),
                pltpu.VMEM((HOP - 1, tile, cols), BF16),
                pltpu.VMEM((tile, cols // 2), BF16),
                pltpu.VMEM((tile, cols), F32),
                pltpu.VMEM((nz, tile, padded), BF16),
                pltpu.VMEM((2, nz // 2, tile, feats), BF16),
                pltpu.VMEM((2, share, tile, feats), BF16),
                pltpu.VMEM((2, nx, share, tile, feats), BF16),
                pltpu.VMEM((nz, tile, feats), F32),
                pltpu.VMEM((2 * nz, 1, LANES), F32),
                dma((11,)),
                pltpu.SemaphoreType.REGULAR((2, HOP)),
                pltpu.SemaphoreType.REGULAR((3,)),
                pltpu.SemaphoreType.REGULAR((nx // 2 - 1, 2)),
                pltpu.SemaphoreType.REGULAR,
                dma,
                dma,
                dma((2,)),
                dma,
                dma,
                dma,
                dma((4,)),
                dma,
                dma((2,)),
                dma,
                dma((2,)),
                dma,
                dma,
                dma,
                dma,
            ],
            compiler_params=pltpu.CompilerParams(
                collective_id=0, has_side_effects=True
            ),
        )(
            tokens.reshape(nz, tile, feats),
            row(norm_gain),
            gw.T,
            gs,
            uw.T,
            us,
            dw,
            row(ds),
            row(og),
        )
        return out.reshape(count, feats)

    return jax.shard_map(
        on_device,
        mesh=mesh,
        in_specs=(
            P("grp", "ra"),
            P("ra"),
            P("ra", "cb"),
            P("cb"),
            P("ra", "cb"),
            P("cb"),
            P("cb", "ra"),
            P("ra"),
            P("ra"),
        ),
        out_specs=P("grp", "ra"),
        check_vma=False,
    )
```

```python
import functools

import jax
import jax.numpy as jnp
from jax import lax
from jax.experimental import pallas as pl
from jax.experimental.pallas import tpu as pltpu
from jax.sharding import PartitionSpec as P

MESH = pl.DeviceIdType.MESH
LANES = 128
F32 = jnp.float32
BF16 = jnp.bfloat16
HOP = 4


def remote(src, dst, send_sem, recv_sem, peer):
    return pltpu.make_async_remote_copy(
        src_ref=src,
        dst_ref=dst,
        send_sem=send_sem,
        recv_sem=recv_sem,
        device_id=peer,
        device_id_type=MESH,
    )


def arrived(ref, sem, peer):
    remote(ref, ref, sem, sem, peer).wait_recv()


def left(ref, sem, peer):
    remote(ref, ref, sem, sem, peer).wait_send()


def split_tail(column, lane):
    high = column.astype(BF16).astype(F32)
    return jnp.where(lane == 0, high, jnp.where(lane == 1, column - high, 0.0))


def kernel(
    nz,
    nc,
    tok_hbm,
    gain_hbm,
    gw_ref,
    gs_hbm,
    uw_ref,
    us_hbm,
    dw_ref,
    ds_hbm,
    og_hbm,
    out_ref,
    tok_ref,
    gain_ref,
    gs_ref,
    us_ref,
    ds_ref,
    og_ref,
    gu_v,
    dw_v,
    part,
    far_in,
    far_in_half,
    near_in,
    relay_out,
    relay_in,
    hid,
    pair,
    pair_in,
    chips,
    mix,
    squares,
    load_sem,
    ready,
    x_ready,
    word,
    rs_send,
    far_recv,
    near_recv,
    relay_recv,
    hid_send,
    late_send,
    onward_send,
    hid_recv,
    pair_send,
    pair_recv,
    chip_send,
    chip_recv,
    mix_send,
    mix_recv,
    sq_send,
    sq_recv,
):
    z = lax.axis_index("ra")
    cb = lax.axis_index("cb")
    chip = cb // 2
    core = cb % 2
    nx = nc // 2
    tile, feats = tok_ref.shape[1:]
    tokens = nz * tile
    units = gw_ref.shape[0]
    main = units // LANES * LANES
    rest = units - main
    width = feats * nz
    cols = part.shape[2]
    halves = (slice(0, cols // 2), slice(cols // 2, cols))

    def to_z(d):
        return {"ra": lax.rem(z + d + nz, nz)}

    def to_chip(d):
        return {"cb": lax.rem(chip + d, nx) * 2 + core}

    mate = {"cb": chip * 2 + 1 - core}

    def block(d):
        return lax.rem(z + d + 2 * nz, nz)

    near_peers = [(i, k) for k in range(HOP, 0, -1) for i in (0, 1)]
    rising = [(0, k) for k in range(1, HOP + 1)] + [(1, k) for k in range(HOP, 0, -1)]
    sign = (1, -1)

    def lower(i, k):
        return block(sign[i] * k) < z

    def is_last(i, k):
        return block(sign[i] * k) == nz - 1

    def turn(c):
        return jnp.minimum(c, nx - c) * nx + c

    def x_lower(d):
        return core == 0 if d == 0 else turn(lax.rem(chip + d, nx)) < turn(chip)

    def to_x(d):
        return mate if d == 0 else to_chip(d)

    beside = (0, 1, nx - 1)
    barrier = pltpu.get_barrier_semaphore()
    for i, k in near_peers:

        @pl.when(jnp.logical_not(lower(i, k)))
        def _():
            pl.semaphore_signal(barrier, inc=1, device_id=to_z(sign[i] * k), device_id_type=MESH)

    for d in beside:

        @pl.when(jnp.logical_not(x_lower(d)))
        def _():
            pl.semaphore_signal(barrier, inc=1, device_id=to_x(d), device_id_type=MESH)

    loads = [
        pltpu.make_async_copy(src, dst, load_sem.at[k])
        for k, (src, dst) in enumerate(
            [
                (tok_hbm, tok_ref),
                (gain_hbm, gain_ref),
                (gw_ref.at[:main], gu_v.at[:main]),
                (uw_ref.at[:main], gu_v.at[main : 2 * main]),
                (gw_ref.at[main:], gu_v.at[2 * main : 2 * main + rest]),
                (uw_ref.at[main:], gu_v.at[2 * main + rest :]),
                (gs_hbm, gs_ref),
                (us_hbm, us_ref),
                (dw_ref, dw_v.at[:units]),
                (ds_hbm, ds_ref),
                (og_hbm, og_ref),
            ]
        )
    ]
    for copy in loads:
        copy.start()

    count = sum(jnp.where(lower(i, k), 1, 0) for i, k in near_peers)
    count += sum(jnp.where(x_lower(d), 1, 0) for d in beside)

    @pl.when(count > 0)
    def _():
        pl.semaphore_wait(barrier, count)

    for i, k in near_peers:

        @pl.when(lower(i, k))
        def _():
            pl.semaphore_signal(
                ready.at[1 - i, k - 1], inc=1, device_id=to_z(sign[i] * k), device_id_type=MESH
            )

    for n, d in enumerate(beside):

        @pl.when(x_lower(d))
        def _():
            pl.semaphore_signal(
                x_ready.at[(3 - n) % 3], inc=1, device_id=to_x(d), device_id_type=MESH
            )

    for copy in loads[:2]:
        copy.wait()
    values = tok_ref[...].astype(F32).reshape(tokens, feats)
    scaled = (values * gain_ref[...]).astype(BF16)
    lane = lax.broadcasted_iota(jnp.int32, (tokens, LANES), 1)
    tail = split_tail(jnp.sum(values * values, axis=1, keepdims=True), lane)
    part[:, :, 2 * units :] = tail.reshape(nz, tile, LANES).astype(BF16)
    for copy in loads[2:6]:
        copy.wait()
    both = lax.dot_general(
        scaled, gu_v[...].astype(BF16), (((1,), (1,)), ((), ())), preferred_element_type=F32
    )
    part[:, :, : 2 * units] = both.reshape(nz, tile, 2 * units).astype(BF16)

    far = {}
    near = {}
    for i, k in near_peers:
        src = part.at[block(sign[i] * (k + HOP))]
        dst = far_in.at[i, k - 1] if k < HOP else far_in_half.at[i]
        if k == HOP:
            src = part.at[block(sign[i] * (k + HOP)), :, halves[i]]
        far[i, k] = remote(src, dst, rs_send, far_recv.at[i], to_z(sign[i] * k))
        if k < HOP:
            near[i, k] = remote(
                part.at[block(sign[i] * k)],
                near_in.at[i, k - 1],
                rs_send,
                near_recv,
                to_z(sign[i] * k),
            )

    for table in (far, near):
        for i, k in near_peers:
            if (i, k) in table:

                @pl.when(lower(i, k))
                def _():
                    table[i, k].start()

    for i, k in rising:

        @pl.when(jnp.logical_not(lower(i, k)))
        def _():
            pl.semaphore_wait(ready.at[i, k - 1], 1)
            far[i, k].start()
            if k < HOP:

                @pl.when(jnp.logical_not(is_last(i, k)))
                def _():
                    near[i, k].start()

    def tell(m):
        for n, d in ((0, 1), (1, nx - 1)):
            pl.semaphore_signal(word.at[m, 1 - n], inc=1, device_id=to_x(d), device_id_type=MESH)

    def hear(m):
        for n in (0, 1):
            pl.semaphore_wait(word.at[m, n], 1)

    for n, d in ((1, 1), (2, nx - 1)):

        @pl.when(jnp.logical_not(x_lower(d)))
        def _():
            pl.semaphore_wait(x_ready.at[n], 1)

    tell(0)

    for copy in loads[6:]:
        copy.wait()
    row = lax.broadcasted_iota(jnp.int32, dw_v.shape, 0)
    down = jnp.where(row < units, dw_v[...], 0.0).astype(BF16)

    tile_lane = lax.broadcasted_iota(jnp.int32, (tile, LANES), 1)
    relay = [
        remote(relay_out.at[i], relay_in.at[i], rs_send, relay_recv, to_z(sign[i] * HOP))
        for i in (0, 1)
    ]

    def pass_on(i):
        arrived(part.at[: 2 * HOP - 1, :, halves[0]], far_recv.at[i], mate)
        total = part[block(sign[i] * HOP)].astype(F32)
        for k in range(1, HOP):
            total += far_in[i, k - 1].astype(F32)
        pieces = [total[:, halves[0]], total[:, halves[1]]]
        pieces[i] += far_in_half[i].astype(F32)
        last = pieces[1][:, -LANES:]
        relay_out[i, :, halves[0]] = pieces[0].astype(BF16)
        relay_out[i, :, cols // 2 : cols - LANES] = pieces[1][:, :-LANES].astype(BF16)
        relay_out[i, :, cols - LANES :] = split_tail(
            jnp.sum(last, axis=1, keepdims=True), tile_lane
        ).astype(BF16)
        relay[i].start()

    @pl.when(z >= HOP)
    def _():
        pass_on(0)

    pass_on(1)

    for i, k in rising:
        if k < HOP:

            @pl.when(is_last(i, k))
            def _():
                near[i, k].start()

    @pl.when(z < HOP)
    def _():
        pass_on(0)

    hear(0)
    tell(1)

    total = part[z].astype(F32)
    arrived(near_in, near_recv, mate)
    for k in range(1, HOP):
        for i in range(2):
            total += near_in[i, k - 1].astype(F32)
    gate_scale = gs_ref[...].reshape(1, units)
    up_scale = us_ref[...].reshape(1, units)
    mixed_scale = jnp.concatenate([gate_scale[:, main:], up_scale[:, main:]], axis=1)
    arrived(relay_in, relay_recv, mate)
    for i in range(2):
        total += relay_in[i].astype(F32)
    square = jnp.sum(total[:, 2 * units :], axis=1, keepdims=True)
    inv = lax.rsqrt(square / width + 1e-06)
    g = total[:, :main] * inv * gate_scale[:, :main]
    u = total[:, main : 2 * main] * inv * up_scale[:, :main]
    both = total[:, 2 * main : 2 * units] * inv * mixed_scale
    swapped = pltpu.roll(both, rest, 1)
    hid[HOP, :, :main] = (g * jax.nn.sigmoid(g) * u).astype(BF16)
    last = both * jax.nn.sigmoid(both) * swapped
    hid[HOP, :, main:] = jnp.where(tile_lane < rest, last, 0.0).astype(BF16)

    direct = nz // 2 - 1

    def slot(d):
        return (HOP - d) % nz

    for d in (nz // 2, direct, -direct):
        remote(hid.at[HOP], hid.at[slot(d)], hid_send, hid_recv.at[3], to_z(d)).start()
    for i, k in near_peers:
        d = sign[i] * k
        sem = hid_recv.at[i if k == HOP else 2]
        remote(hid.at[HOP], hid.at[slot(d)], hid_send, sem, to_z(d)).start()
    late = lax.rem(z, 2 * HOP) == HOP - 1
    no_relay = lax.rem(z, 2 * HOP) == 2 * HOP - 1
    between = [s * k for k in range(direct - 1, HOP, -1) for s in sign]

    @pl.when(late)
    def _():
        for d in between:
            remote(hid.at[HOP], hid.at[slot(d)], late_send, hid_recv.at[3], to_z(d)).start()

    for m in range(1, nx // 2 - 2):
        hear(m)
        tell(m + 1)

    def forward(i):
        @pl.when(jnp.logical_not(no_relay))
        def _():
            arrived(hid.at[0], hid_recv.at[i], mate)
            src = hid.at[slot(sign[i] * HOP)]
            for k in range(direct - HOP - 1, 0, -1):
                dst = hid.at[slot(sign[i] * (HOP + k))]
                remote(src, dst, onward_send, hid_recv.at[3], to_z(sign[i] * k)).start()

    @pl.when(z >= nz // 2)
    def _():
        forward(0)

    forward(1)

    @pl.when(z < nz // 2)
    def _():
        forward(0)

    groups = 2
    size = nz // groups
    share = size // 2

    def multiply(k):
        arrived(hid.at[: 2 * HOP - 2 + k], hid_recv.at[2 + k], mate)

        @pl.when(no_relay)
        def _():
            arrived(hid.at[0], hid_recv.at[k], mate)

        rows = hid[k * size : (k + 1) * size].reshape(size * tile, hid.shape[2])
        partial = jnp.dot(rows, down, preferred_element_type=F32)
        pair[k] = partial.reshape(size, tile, feats).astype(BF16)
        copy = remote(
            pair.at[k, pl.ds((1 - core) * share, share)],
            pair_in.at[k],
            pair_send,
            pair_recv.at[k],
            mate,
        )
        copy.start()

    def broadcast(k):
        arrived(pair_in.at[k], pair_recv.at[k], mate)
        own = pair[k, pl.ds(core * share, share)].astype(F32) + pair_in[k].astype(F32)
        chips[k, chip] = own.astype(BF16)
        for d in sorted(range(1, nx), key=lambda d: -min(d, nx - d)):
            to = remote(
                chips.at[k, chip],
                chips.at[k, chip],
                chip_send,
                chip_recv.at[k],
                to_chip(d),
            )
            to.start()

    def finish(k):
        arrived(chips.at[k, : nx - 1], chip_recv.at[k], mate)
        branch = chips[k, 0].astype(F32)
        for j in range(1, nx):
            branch += chips[k, j].astype(F32)
        first = k * size + core * share
        for j in range(share):
            own = tok_ref[block(first + j - HOP)].astype(F32)
            mix[first + j] = 0.5 * own + branch[j] * ds_ref[...]
        rows = pl.ds(first, share)
        mine = mix[rows].reshape(share * tile, feats)
        column = jnp.sum(mine * mine, axis=1, keepdims=True)
        square = jnp.sum(jnp.where(diagonal(first, share), column, 0.0), axis=0, keepdims=True)
        remote(mix.at[rows], mix.at[rows], mix_send, mix_recv, mate).start()
        return square

    def diagonal(first, count):
        place = lax.broadcasted_iota(jnp.int32, (count * tile, tokens), 0)
        place = lax.rem(place + tile * (z + first + nz - HOP), tokens)
        return place == lax.broadcasted_iota(jnp.int32, (count * tile, tokens), 1)

    @pl.when(jnp.logical_not(x_lower(0)))
    def _():
        pl.semaphore_wait(x_ready.at[0], 1)

    multiply(0)
    hear(nx // 2 - 2)
    broadcast(0)
    multiply(1)
    broadcast(1)
    near_squares = finish(0)
    far_squares = finish(1)

    squares[core * nz + z] = near_squares + far_squares
    own = squares.at[core * nz + z]
    order = sorted(range(1, nz), key=lambda d: -min(d, nz - d))
    for d in order:
        for t in range(2):
            peer = {"ra": lax.rem(z + d, nz), "cb": chip * 2 + lax.rem(core + t, 2)}
            remote(own, own, sq_send, sq_recv, peer).start()
    remote(own, own, sq_send, sq_recv, mate).start()
    arrived(mix.at[: 2 * share], mix_recv, mate)
    scaled_mixed = mix[...].reshape(tokens, feats) * og_ref[...]
    arrived(squares.at[: 2 * nz - 1], sq_recv, mate)
    everything = squares[0]
    for j in range(1, 2 * nz):
        everything += squares[j]
    inv_row = lax.rsqrt(everything / width + 1e-06)
    inv_second = jnp.sum(jnp.where(diagonal(0, nz), inv_row, 0.0), axis=1, keepdims=True)
    result = (scaled_mixed * inv_second).reshape(nz, tile, feats).astype(BF16)
    for r in range(nz):
        out_ref[block(r - HOP)] = result[r]

    left(part.at[: 4 * HOP - 1], rs_send, mate)
    left(hid.at[: 2 * HOP + 3], hid_send, mate)

    @pl.when(late)
    def _():
        left(hid.at[: len(between)], late_send, mate)

    @pl.when(jnp.logical_not(no_relay))
    def _():
        left(hid.at[: len(between)], onward_send, mate)

    left(pair.at[0], pair_send, mate)
    left(chips.at[:, : nx - 1], chip_send, mate)
    left(mix.at[: 2 * share], mix_send, mate)
    left(squares.at[: 2 * nz - 1], sq_send, mate)


def solution(mesh):
    nz, nc = mesh.shape["ra"], mesh.shape["cb"]
    nx = nc // 2

    def on_device(tokens, norm_gain, gw, gs, uw, us, dw, ds, og):
        count, feats = tokens.shape
        units = gw.shape[1]
        padded = -(-units // LANES) * LANES
        tile = count // nz
        cols = 2 * units + LANES
        share = nz // 4
        vmem = pl.BlockSpec(memory_space=pltpu.VMEM)
        hbm = pl.BlockSpec(memory_space=pltpu.HBM)
        dma = pltpu.SemaphoreType.DMA
        row = lambda v: v.reshape(1, -1)
        out = pl.pallas_call(
            functools.partial(kernel, nz, nc),
            out_shape=pltpu.VMEM((nz, tile, feats), BF16),
            in_specs=[hbm] * 9,
            out_specs=vmem,
            scratch_shapes=[
                pltpu.VMEM((nz, tile, feats), BF16),
                pltpu.VMEM((1, feats), F32),
                pltpu.VMEM((units,), F32),
                pltpu.VMEM((units,), F32),
                pltpu.VMEM((1, feats), F32),
                pltpu.VMEM((1, feats), F32),
                pltpu.VMEM((2 * units, feats), F32),
                pltpu.VMEM((padded, feats), F32),
                pltpu.VMEM((nz, tile, cols), BF16),
                pltpu.VMEM((2, HOP - 1, tile, cols), BF16),
                pltpu.VMEM((2, tile, cols // 2), BF16),
                pltpu.VMEM((2, HOP - 1, tile, cols), BF16),
                pltpu.VMEM((2, tile, cols), BF16),
                pltpu.VMEM((2, tile, cols), BF16),
                pltpu.VMEM((nz, tile, padded), BF16),
                pltpu.VMEM((2, nz // 2, tile, feats), BF16),
                pltpu.VMEM((2, share, tile, feats), BF16),
                pltpu.VMEM((2, nx, share, tile, feats), BF16),
                pltpu.VMEM((nz, tile, feats), F32),
                pltpu.VMEM((2 * nz, 1, LANES), F32),
                dma((11,)),
                pltpu.SemaphoreType.REGULAR((2, HOP)),
                pltpu.SemaphoreType.REGULAR((3,)),
                pltpu.SemaphoreType.REGULAR((nx // 2 - 1, 2)),
                dma,
                dma((2,)),
                dma,
                dma,
                dma,
                dma,
                dma,
                dma((4,)),
                dma,
                dma((2,)),
                dma,
                dma((2,)),
                dma,
                dma,
                dma,
                dma,
            ],
            compiler_params=pltpu.CompilerParams(
                collective_id=0, has_side_effects=True
            ),
        )(
            tokens.reshape(nz, tile, feats),
            row(norm_gain),
            gw.T,
            gs,
            uw.T,
            us,
            dw,
            row(ds),
            row(og),
        )
        return out.reshape(count, feats)

    return jax.shard_map(
        on_device,
        mesh=mesh,
        in_specs=(
            P("grp", "ra"),
            P("ra"),
            P("ra", "cb"),
            P("cb"),
            P("ra", "cb"),
            P("cb"),
            P("cb", "ra"),
            P("ra"),
            P("ra"),
        ),
        out_specs=P("grp", "ra"),
        check_vma=False,
    )
```

```python
import functools

import jax
import jax.numpy as jnp
from jax import lax
from jax.experimental import pallas as pl
from jax.experimental.pallas import tpu as pltpu
from jax.sharding import PartitionSpec as P

MESH = pl.DeviceIdType.MESH
LANES = 128
F32 = jnp.float32
BF16 = jnp.bfloat16
HOP = 4


def remote(src, dst, send_sem, recv_sem, peer):
    return pltpu.make_async_remote_copy(
        src_ref=src,
        dst_ref=dst,
        send_sem=send_sem,
        recv_sem=recv_sem,
        device_id=peer,
        device_id_type=MESH,
    )


def arrived(ref, sem, peer):
    remote(ref, ref, sem, sem, peer).wait_recv()


def left(ref, sem, peer):
    remote(ref, ref, sem, sem, peer).wait_send()


def split_tail(column, lane):
    high = column.astype(BF16).astype(F32)
    return jnp.where(lane == 0, high, jnp.where(lane == 1, column - high, 0.0))


def kernel(
    nz,
    nc,
    tok_hbm,
    gain_hbm,
    gw_ref,
    gs_hbm,
    uw_ref,
    us_hbm,
    dw_ref,
    ds_hbm,
    og_hbm,
    out_ref,
    tok_ref,
    gain_ref,
    gs_ref,
    us_ref,
    ds_ref,
    og_ref,
    gu_v,
    dw_v,
    part,
    far_in,
    far_in_half,
    near_in,
    relay_out,
    relay_in,
    hid,
    pair,
    pair_in,
    chips,
    mix,
    squares,
    load_sem,
    ready,
    x_ready,
    word,
    rs_send,
    far_recv,
    near_recv,
    relay_recv,
    hid_send,
    hid_recv,
    pair_send,
    pair_recv,
    chip_send,
    chip_recv,
    mix_send,
    mix_recv,
    sq_send,
    sq_recv,
):
    z = lax.axis_index("ra")
    cb = lax.axis_index("cb")
    chip = cb // 2
    core = cb % 2
    nx = nc // 2
    tile, feats = tok_ref.shape[1:]
    tokens = nz * tile
    units = gw_ref.shape[0]
    main = units // LANES * LANES
    rest = units - main
    width = feats * nz
    cols = part.shape[2]
    halves = (slice(0, cols // 2), slice(cols // 2, cols))

    def to_z(d):
        return {"ra": lax.rem(z + d + nz, nz)}

    def to_chip(d):
        return {"cb": lax.rem(chip + d, nx) * 2 + core}

    mate = {"cb": chip * 2 + 1 - core}

    def block(d):
        return lax.rem(z + d + 2 * nz, nz)

    near_peers = [(i, k) for k in range(HOP, 0, -1) for i in (0, 1)]
    rising = [(0, k) for k in range(1, HOP + 1)] + [(1, k) for k in range(HOP, 0, -1)]
    sign = (1, -1)

    def lower(i, k):
        return block(sign[i] * k) < z

    def is_last(i, k):
        return block(sign[i] * k) == nz - 1

    def turn(c):
        return jnp.minimum(c, nx - c) * nx + c

    def x_lower(d):
        return core == 0 if d == 0 else turn(lax.rem(chip + d, nx)) < turn(chip)

    def to_x(d):
        return mate if d == 0 else to_chip(d)

    beside = (0, 1, nx - 1)
    barrier = pltpu.get_barrier_semaphore()
    for i, k in near_peers:

        @pl.when(jnp.logical_not(lower(i, k)))
        def _():
            pl.semaphore_signal(barrier, inc=1, device_id=to_z(sign[i] * k), device_id_type=MESH)

    for d in beside:

        @pl.when(jnp.logical_not(x_lower(d)))
        def _():
            pl.semaphore_signal(barrier, inc=1, device_id=to_x(d), device_id_type=MESH)

    loads = [
        pltpu.make_async_copy(src, dst, load_sem.at[k])
        for k, (src, dst) in enumerate(
            [
                (tok_hbm, tok_ref),
                (gain_hbm, gain_ref),
                (gw_ref.at[:main], gu_v.at[:main]),
                (uw_ref.at[:main], gu_v.at[main : 2 * main]),
                (gw_ref.at[main:], gu_v.at[2 * main : 2 * main + rest]),
                (uw_ref.at[main:], gu_v.at[2 * main + rest :]),
                (gs_hbm, gs_ref),
                (us_hbm, us_ref),
                (dw_ref, dw_v.at[:units]),
                (ds_hbm, ds_ref),
                (og_hbm, og_ref),
            ]
        )
    ]
    for copy in loads:
        copy.start()

    count = sum(jnp.where(lower(i, k), 1, 0) for i, k in near_peers)
    count += sum(jnp.where(x_lower(d), 1, 0) for d in beside)

    @pl.when(count > 0)
    def _():
        pl.semaphore_wait(barrier, count)

    for i, k in near_peers:

        @pl.when(lower(i, k))
        def _():
            pl.semaphore_signal(
                ready.at[1 - i, k - 1], inc=1, device_id=to_z(sign[i] * k), device_id_type=MESH
            )

    for n, d in enumerate(beside):

        @pl.when(x_lower(d))
        def _():
            pl.semaphore_signal(
                x_ready.at[(3 - n) % 3], inc=1, device_id=to_x(d), device_id_type=MESH
            )

    for copy in loads[:2]:
        copy.wait()
    values = tok_ref[...].astype(F32).reshape(tokens, feats)
    scaled = (values * gain_ref[...]).astype(BF16)
    lane = lax.broadcasted_iota(jnp.int32, (tokens, LANES), 1)
    tail = split_tail(jnp.sum(values * values, axis=1, keepdims=True), lane)
    part[:, :, 2 * units :] = tail.reshape(nz, tile, LANES).astype(BF16)
    for copy in loads[2:6]:
        copy.wait()
    both = lax.dot_general(
        scaled, gu_v[...].astype(BF16), (((1,), (1,)), ((), ())), preferred_element_type=F32
    )
    part[:, :, : 2 * units] = both.reshape(nz, tile, 2 * units).astype(BF16)

    far = {}
    near = {}
    for i, k in near_peers:
        src = part.at[block(sign[i] * (k + HOP))]
        dst = far_in.at[i, k - 1] if k < HOP else far_in_half.at[i]
        if k == HOP:
            src = part.at[block(sign[i] * (k + HOP)), :, halves[i]]
        far[i, k] = remote(src, dst, rs_send, far_recv.at[i], to_z(sign[i] * k))
        if k < HOP:
            near[i, k] = remote(
                part.at[block(sign[i] * k)],
                near_in.at[i, k - 1],
                rs_send,
                near_recv,
                to_z(sign[i] * k),
            )

    for table in (far, near):
        for i, k in near_peers:
            if (i, k) in table:

                @pl.when(lower(i, k))
                def _():
                    table[i, k].start()

    for i, k in rising:

        @pl.when(jnp.logical_not(lower(i, k)))
        def _():
            pl.semaphore_wait(ready.at[i, k - 1], 1)
            far[i, k].start()
            if k < HOP:

                @pl.when(jnp.logical_not(is_last(i, k)))
                def _():
                    near[i, k].start()

    def tell(m):
        for n, d in ((0, 1), (1, nx - 1)):
            pl.semaphore_signal(word.at[m, 1 - n], inc=1, device_id=to_x(d), device_id_type=MESH)

    def hear(m):
        for n in (0, 1):
            pl.semaphore_wait(word.at[m, n], 1)

    for n, d in ((1, 1), (2, nx - 1)):

        @pl.when(jnp.logical_not(x_lower(d)))
        def _():
            pl.semaphore_wait(x_ready.at[n], 1)

    tell(0)

    for copy in loads[6:]:
        copy.wait()
    row = lax.broadcasted_iota(jnp.int32, dw_v.shape, 0)
    down = jnp.where(row < units, dw_v[...], 0.0).astype(BF16)

    tile_lane = lax.broadcasted_iota(jnp.int32, (tile, LANES), 1)
    relay = [
        remote(relay_out.at[i], relay_in.at[i], rs_send, relay_recv, to_z(sign[i] * HOP))
        for i in (0, 1)
    ]

    def pass_on(i):
        arrived(part.at[: 2 * HOP - 1, :, halves[0]], far_recv.at[i], mate)
        total = part[block(sign[i] * HOP)].astype(F32)
        for k in range(1, HOP):
            total += far_in[i, k - 1].astype(F32)
        pieces = [total[:, halves[0]], total[:, halves[1]]]
        pieces[i] += far_in_half[i].astype(F32)
        last = pieces[1][:, -LANES:]
        relay_out[i, :, halves[0]] = pieces[0].astype(BF16)
        relay_out[i, :, cols // 2 : cols - LANES] = pieces[1][:, :-LANES].astype(BF16)
        relay_out[i, :, cols - LANES :] = split_tail(
            jnp.sum(last, axis=1, keepdims=True), tile_lane
        ).astype(BF16)
        relay[i].start()

    @pl.when(z >= HOP)
    def _():
        pass_on(0)

    pass_on(1)

    for i, k in rising:
        if k < HOP:

            @pl.when(is_last(i, k))
            def _():
                near[i, k].start()

    @pl.when(z < HOP)
    def _():
        pass_on(0)

    hear(0)
    tell(1)

    total = part[z].astype(F32)
    arrived(near_in, near_recv, mate)
    for k in range(1, HOP):
        for i in range(2):
            total += near_in[i, k - 1].astype(F32)
    gate_scale = gs_ref[...].reshape(1, units)
    up_scale = us_ref[...].reshape(1, units)
    mixed_scale = jnp.concatenate([gate_scale[:, main:], up_scale[:, main:]], axis=1)
    arrived(relay_in, relay_recv, mate)
    for i in range(2):
        total += relay_in[i].astype(F32)
    square = jnp.sum(total[:, 2 * units :], axis=1, keepdims=True)
    inv = lax.rsqrt(square / width + 1e-06)
    g = total[:, :main] * inv * gate_scale[:, :main]
    u = total[:, main : 2 * main] * inv * up_scale[:, :main]
    both = total[:, 2 * main : 2 * units] * inv * mixed_scale
    swapped = pltpu.roll(both, rest, 1)
    hid[HOP, :, :main] = (g * jax.nn.sigmoid(g) * u).astype(BF16)
    last = both * jax.nn.sigmoid(both) * swapped
    hid[HOP, :, main:] = jnp.where(tile_lane < rest, last, 0.0).astype(BF16)

    def slot(d):
        return (HOP - d) % nz

    order = [nz // 2] + [s * k for k in range(nz // 2 - 1, 0, -1) for s in sign]
    for d in order:
        sem = hid_recv.at[0 if slot(d) < nz // 2 else 1]
        remote(hid.at[HOP], hid.at[slot(d)], hid_send, sem, to_z(d)).start()
    for m in range(1, nx // 2 - 2):
        hear(m)
        tell(m + 1)

    groups = 2
    size = nz // groups
    share = size // 2

    def multiply(k):
        arrived(hid.at[: size - 1 + k], hid_recv.at[k], mate)
        rows = hid[k * size : (k + 1) * size].reshape(size * tile, hid.shape[2])
        partial = jnp.dot(rows, down, preferred_element_type=F32)
        pair[k] = partial.reshape(size, tile, feats).astype(BF16)
        copy = remote(
            pair.at[k, pl.ds((1 - core) * share, share)],
            pair_in.at[k],
            pair_send,
            pair_recv.at[k],
            mate,
        )
        copy.start()

    def broadcast(k):
        arrived(pair_in.at[k], pair_recv.at[k], mate)
        own = pair[k, pl.ds(core * share, share)].astype(F32) + pair_in[k].astype(F32)
        chips[k, chip] = own.astype(BF16)
        for d in sorted(range(1, nx), key=lambda d: -min(d, nx - d)):
            to = remote(
                chips.at[k, chip],
                chips.at[k, chip],
                chip_send,
                chip_recv.at[k],
                to_chip(d),
            )
            to.start()

    def finish(k):
        arrived(chips.at[k, : nx - 1], chip_recv.at[k], mate)
        branch = chips[k, 0].astype(F32)
        for j in range(1, nx):
            branch += chips[k, j].astype(F32)
        first = k * size + core * share
        for j in range(share):
            own = tok_ref[block(first + j - HOP)].astype(F32)
            mix[first + j] = 0.5 * own + branch[j] * ds_ref[...]
        rows = pl.ds(first, share)
        mine = mix[rows].reshape(share * tile, feats)
        column = jnp.sum(mine * mine, axis=1, keepdims=True)
        square = jnp.sum(jnp.where(diagonal(first, share), column, 0.0), axis=0, keepdims=True)
        remote(mix.at[rows], mix.at[rows], mix_send, mix_recv, mate).start()
        return square

    def diagonal(first, count):
        place = lax.broadcasted_iota(jnp.int32, (count * tile, tokens), 0)
        place = lax.rem(place + tile * (z + first + nz - HOP), tokens)
        return place == lax.broadcasted_iota(jnp.int32, (count * tile, tokens), 1)

    @pl.when(jnp.logical_not(x_lower(0)))
    def _():
        pl.semaphore_wait(x_ready.at[0], 1)

    multiply(0)
    hear(nx // 2 - 2)
    broadcast(0)
    multiply(1)
    broadcast(1)
    near_squares = finish(0)
    far_squares = finish(1)

    squares[core * nz + z] = near_squares + far_squares
    own = squares.at[core * nz + z]
    order = sorted(range(1, nz), key=lambda d: -min(d, nz - d))
    for d in order:
        for t in range(2):
            peer = {"ra": lax.rem(z + d, nz), "cb": chip * 2 + lax.rem(core + t, 2)}
            remote(own, own, sq_send, sq_recv, peer).start()
    remote(own, own, sq_send, sq_recv, mate).start()
    arrived(mix.at[: 2 * share], mix_recv, mate)
    scaled_mixed = mix[...].reshape(tokens, feats) * og_ref[...]
    arrived(squares.at[: 2 * nz - 1], sq_recv, mate)
    everything = squares[0]
    for j in range(1, 2 * nz):
        everything += squares[j]
    inv_row = lax.rsqrt(everything / width + 1e-06)
    inv_second = jnp.sum(jnp.where(diagonal(0, nz), inv_row, 0.0), axis=1, keepdims=True)
    result = (scaled_mixed * inv_second).reshape(nz, tile, feats).astype(BF16)
    for r in range(nz):
        out_ref[block(r - HOP)] = result[r]

    left(part.at[: 4 * HOP - 1], rs_send, mate)
    left(hid.at[: nz - 1], hid_send, mate)
    left(pair.at[0], pair_send, mate)
    left(chips.at[:, : nx - 1], chip_send, mate)
    left(mix.at[: 2 * share], mix_send, mate)
    left(squares.at[: 2 * nz - 1], sq_send, mate)


def solution(mesh):
    nz, nc = mesh.shape["ra"], mesh.shape["cb"]
    nx = nc // 2

    def on_device(tokens, norm_gain, gw, gs, uw, us, dw, ds, og):
        count, feats = tokens.shape
        units = gw.shape[1]
        padded = -(-units // LANES) * LANES
        tile = count // nz
        cols = 2 * units + LANES
        share = nz // 4
        vmem = pl.BlockSpec(memory_space=pltpu.VMEM)
        hbm = pl.BlockSpec(memory_space=pltpu.HBM)
        dma = pltpu.SemaphoreType.DMA
        row = lambda v: v.reshape(1, -1)
        out = pl.pallas_call(
            functools.partial(kernel, nz, nc),
            out_shape=pltpu.VMEM((nz, tile, feats), BF16),
            in_specs=[hbm] * 9,
            out_specs=vmem,
            scratch_shapes=[
                pltpu.VMEM((nz, tile, feats), BF16),
                pltpu.VMEM((1, feats), F32),
                pltpu.VMEM((units,), F32),
                pltpu.VMEM((units,), F32),
                pltpu.VMEM((1, feats), F32),
                pltpu.VMEM((1, feats), F32),
                pltpu.VMEM((2 * units, feats), F32),
                pltpu.VMEM((padded, feats), F32),
                pltpu.VMEM((nz, tile, cols), BF16),
                pltpu.VMEM((2, HOP - 1, tile, cols), BF16),
                pltpu.VMEM((2, tile, cols // 2), BF16),
                pltpu.VMEM((2, HOP - 1, tile, cols), BF16),
                pltpu.VMEM((2, tile, cols), BF16),
                pltpu.VMEM((2, tile, cols), BF16),
                pltpu.VMEM((nz, tile, padded), BF16),
                pltpu.VMEM((2, nz // 2, tile, feats), BF16),
                pltpu.VMEM((2, share, tile, feats), BF16),
                pltpu.VMEM((2, nx, share, tile, feats), BF16),
                pltpu.VMEM((nz, tile, feats), F32),
                pltpu.VMEM((2 * nz, 1, LANES), F32),
                dma((11,)),
                pltpu.SemaphoreType.REGULAR((2, HOP)),
                pltpu.SemaphoreType.REGULAR((3,)),
                pltpu.SemaphoreType.REGULAR((nx // 2 - 1, 2)),
                dma,
                dma((2,)),
                dma,
                dma,
                dma,
                dma((2,)),
                dma,
                dma((2,)),
                dma,
                dma((2,)),
                dma,
                dma,
                dma,
                dma,
            ],
            compiler_params=pltpu.CompilerParams(
                collective_id=0, has_side_effects=True
            ),
        )(
            tokens.reshape(nz, tile, feats),
            row(norm_gain),
            gw.T,
            gs,
            uw.T,
            us,
            dw,
            row(ds),
            row(og),
        )
        return out.reshape(count, feats)

    return jax.shard_map(
        on_device,
        mesh=mesh,
        in_specs=(
            P("grp", "ra"),
            P("ra"),
            P("ra", "cb"),
            P("cb"),
            P("ra", "cb"),
            P("cb"),
            P("cb", "ra"),
            P("ra"),
            P("ra"),
        ),
        out_specs=P("grp", "ra"),
        check_vma=False,
    )
```

```python
import functools

import jax
import jax.numpy as jnp
from jax import lax
from jax.experimental import pallas as pl
from jax.experimental.pallas import tpu as pltpu
from jax.sharding import PartitionSpec as P

MESH = pl.DeviceIdType.MESH
LANES = 128
F32 = jnp.float32
BF16 = jnp.bfloat16
HOP = 4


def remote(src, dst, send_sem, recv_sem, peer):
    return pltpu.make_async_remote_copy(
        src_ref=src,
        dst_ref=dst,
        send_sem=send_sem,
        recv_sem=recv_sem,
        device_id=peer,
        device_id_type=MESH,
    )


def arrived(ref, sem, peer):
    remote(ref, ref, sem, sem, peer).wait_recv()


def left(ref, sem, peer):
    remote(ref, ref, sem, sem, peer).wait_send()


def split_tail(column, lane):
    high = column.astype(BF16).astype(F32)
    return jnp.where(lane == 0, high, jnp.where(lane == 1, column - high, 0.0))


def kernel(
    nz,
    nc,
    tok_hbm,
    gain_hbm,
    gw_ref,
    gs_hbm,
    uw_ref,
    us_hbm,
    dw_ref,
    ds_hbm,
    og_hbm,
    out_ref,
    tok_ref,
    gain_ref,
    gs_ref,
    us_ref,
    ds_ref,
    og_ref,
    gu_v,
    dw_v,
    part,
    far_in,
    far_in_half,
    near_in,
    relay_out,
    relay_in,
    hid,
    pair,
    pair_in,
    chips,
    mix,
    squares,
    load_sem,
    ready,
    x_ready,
    word,
    rs_send,
    far_recv,
    near_recv,
    relay_recv,
    hid_send,
    hid_recv,
    pair_send,
    pair_recv,
    chip_send,
    chip_recv,
    mix_send,
    mix_recv,
    sq_send,
    sq_recv,
):
    z = lax.axis_index("ra")
    cb = lax.axis_index("cb")
    chip = cb // 2
    core = cb % 2
    nx = nc // 2
    tile, feats = tok_ref.shape[1:]
    tokens = nz * tile
    units = gw_ref.shape[0]
    main = units // LANES * LANES
    rest = units - main
    width = feats * nz
    cols = part.shape[2]
    halves = (slice(0, cols // 2), slice(cols // 2, cols))

    def to_z(d):
        return {"ra": lax.rem(z + d + nz, nz)}

    def to_chip(d):
        return {"cb": lax.rem(chip + d, nx) * 2 + core}

    mate = {"cb": chip * 2 + 1 - core}

    def block(d):
        return lax.rem(z + d + 2 * nz, nz)

    near_peers = [(i, k) for k in range(HOP, 0, -1) for i in (0, 1)]
    rising = [(0, k) for k in range(1, HOP + 1)] + [(1, k) for k in range(HOP, 0, -1)]
    sign = (1, -1)

    def lower(i, k):
        return block(sign[i] * k) < z

    def is_last(i, k):
        return block(sign[i] * k) == nz - 1

    def turn(c):
        return jnp.minimum(c, nx - c) * nx + c

    def x_lower(d):
        return core == 0 if d == 0 else turn(lax.rem(chip + d, nx)) < turn(chip)

    def to_x(d):
        return mate if d == 0 else to_chip(d)

    beside = (0, 1, nx - 1)
    barrier = pltpu.get_barrier_semaphore()
    for i, k in near_peers:

        @pl.when(jnp.logical_not(lower(i, k)))
        def _():
            pl.semaphore_signal(barrier, inc=1, device_id=to_z(sign[i] * k), device_id_type=MESH)

    for d in beside:

        @pl.when(jnp.logical_not(x_lower(d)))
        def _():
            pl.semaphore_signal(barrier, inc=1, device_id=to_x(d), device_id_type=MESH)

    loads = [
        pltpu.make_async_copy(src, dst, load_sem.at[k])
        for k, (src, dst) in enumerate(
            [
                (tok_hbm, tok_ref),
                (gain_hbm, gain_ref),
                (gw_ref.at[:main], gu_v.at[:main]),
                (uw_ref.at[:main], gu_v.at[main : 2 * main]),
                (gw_ref.at[main:], gu_v.at[2 * main : 2 * main + rest]),
                (uw_ref.at[main:], gu_v.at[2 * main + rest :]),
                (gs_hbm, gs_ref),
                (us_hbm, us_ref),
                (dw_ref, dw_v.at[:units]),
                (ds_hbm, ds_ref),
                (og_hbm, og_ref),
            ]
        )
    ]
    for copy in loads:
        copy.start()

    count = sum(jnp.where(lower(i, k), 1, 0) for i, k in near_peers)
    count += sum(jnp.where(x_lower(d), 1, 0) for d in beside)

    @pl.when(count > 0)
    def _():
        pl.semaphore_wait(barrier, count)

    for i, k in near_peers:

        @pl.when(lower(i, k))
        def _():
            pl.semaphore_signal(
                ready.at[1 - i, k - 1], inc=1, device_id=to_z(sign[i] * k), device_id_type=MESH
            )

    for n, d in enumerate(beside):

        @pl.when(x_lower(d))
        def _():
            pl.semaphore_signal(
                x_ready.at[(3 - n) % 3], inc=1, device_id=to_x(d), device_id_type=MESH
            )

    for copy in loads[:2]:
        copy.wait()
    values = tok_ref[...].astype(F32).reshape(tokens, feats)
    scaled = (values * gain_ref[...]).astype(BF16)
    lane = lax.broadcasted_iota(jnp.int32, (tokens, LANES), 1)
    tail = split_tail(jnp.sum(values * values, axis=1, keepdims=True), lane)
    part[:, :, 2 * units :] = tail.reshape(nz, tile, LANES).astype(BF16)
    for copy in loads[2:6]:
        copy.wait()
    both = lax.dot_general(
        scaled, gu_v[...].astype(BF16), (((1,), (1,)), ((), ())), preferred_element_type=F32
    )
    part[:, :, : 2 * units] = both.reshape(nz, tile, 2 * units).astype(BF16)

    far = {}
    near = {}
    for i, k in near_peers:
        src = part.at[block(sign[i] * (k + HOP))]
        dst = far_in.at[i, k - 1] if k < HOP else far_in_half.at[i]
        if k == HOP:
            src = part.at[block(sign[i] * (k + HOP)), :, halves[i]]
        far[i, k] = remote(src, dst, rs_send, far_recv.at[i], to_z(sign[i] * k))
        if k < HOP:
            near[i, k] = remote(
                part.at[block(sign[i] * k)],
                near_in.at[i, k - 1],
                rs_send,
                near_recv,
                to_z(sign[i] * k),
            )

    for table in (far, near):
        for i, k in near_peers:
            if (i, k) in table:

                @pl.when(lower(i, k))
                def _():
                    table[i, k].start()

    for i, k in rising:

        @pl.when(jnp.logical_not(lower(i, k)))
        def _():
            pl.semaphore_wait(ready.at[i, k - 1], 1)
            far[i, k].start()
            if k < HOP:

                @pl.when(jnp.logical_not(is_last(i, k)))
                def _():
                    near[i, k].start()

    def tell(m):
        for n, d in ((0, 1), (1, nx - 1)):
            pl.semaphore_signal(word.at[m, 1 - n], inc=1, device_id=to_x(d), device_id_type=MESH)

    def hear(m):
        for n in (0, 1):
            pl.semaphore_wait(word.at[m, n], 1)

    for n, d in ((1, 1), (2, nx - 1)):

        @pl.when(jnp.logical_not(x_lower(d)))
        def _():
            pl.semaphore_wait(x_ready.at[n], 1)

    tell(0)

    for copy in loads[6:]:
        copy.wait()
    row = lax.broadcasted_iota(jnp.int32, dw_v.shape, 0)
    down = jnp.where(row < units, dw_v[...], 0.0).astype(BF16)

    tile_lane = lax.broadcasted_iota(jnp.int32, (tile, LANES), 1)
    relay = [
        remote(relay_out.at[i], relay_in.at[i], rs_send, relay_recv, to_z(sign[i] * HOP))
        for i in (0, 1)
    ]

    def pass_on(i):
        arrived(part.at[: 2 * HOP - 1, :, halves[0]], far_recv.at[i], mate)
        total = part[block(sign[i] * HOP)].astype(F32)
        for k in range(1, HOP):
            total += far_in[i, k - 1].astype(F32)
        pieces = [total[:, halves[0]], total[:, halves[1]]]
        pieces[i] += far_in_half[i].astype(F32)
        last = pieces[1][:, -LANES:]
        relay_out[i, :, halves[0]] = pieces[0].astype(BF16)
        relay_out[i, :, cols // 2 : cols - LANES] = pieces[1][:, :-LANES].astype(BF16)
        relay_out[i, :, cols - LANES :] = split_tail(
            jnp.sum(last, axis=1, keepdims=True), tile_lane
        ).astype(BF16)
        relay[i].start()

    @pl.when(z >= HOP)
    def _():
        pass_on(0)

    pass_on(1)

    for i, k in rising:
        if k < HOP:

            @pl.when(is_last(i, k))
            def _():
                near[i, k].start()

    @pl.when(z < HOP)
    def _():
        pass_on(0)

    hear(0)
    tell(1)

    total = part[z].astype(F32)
    arrived(near_in, near_recv, mate)
    for k in range(1, HOP):
        for i in range(2):
            total += near_in[i, k - 1].astype(F32)
    gate_scale = gs_ref[...].reshape(1, units)
    up_scale = us_ref[...].reshape(1, units)
    mixed_scale = jnp.concatenate([gate_scale[:, main:], up_scale[:, main:]], axis=1)
    arrived(relay_in, relay_recv, mate)
    for i in range(2):
        total += relay_in[i].astype(F32)
    square = jnp.sum(total[:, 2 * units :], axis=1, keepdims=True)
    inv = lax.rsqrt(square / width + 1e-06)
    g = total[:, :main] * inv * gate_scale[:, :main]
    u = total[:, main : 2 * main] * inv * up_scale[:, :main]
    both = total[:, 2 * main : 2 * units] * inv * mixed_scale
    swapped = pltpu.roll(both, rest, 1)
    hid[HOP, :, :main] = (g * jax.nn.sigmoid(g) * u).astype(BF16)
    last = both * jax.nn.sigmoid(both) * swapped
    hid[HOP, :, main:] = jnp.where(tile_lane < rest, last, 0.0).astype(BF16)

    def slot(d):
        return (HOP - d) % nz

    most = nz // 2 - 1
    steps = [most] + list(range(HOP, 0, -1)) + list(range(most - 1, HOP, -1))
    order = [nz // 2] + [s * k for k in steps for s in sign]
    for d in order:
        sem = hid_recv.at[0 if slot(d) < nz // 2 else 1]
        remote(hid.at[HOP], hid.at[slot(d)], hid_send, sem, to_z(d)).start()
    for m in range(1, nx // 2 - 2):
        hear(m)
        tell(m + 1)

    groups = 2
    size = nz // groups
    share = size // 2

    def multiply(k):
        arrived(hid.at[: size - 1 + k], hid_recv.at[k], mate)
        rows = hid[k * size : (k + 1) * size].reshape(size * tile, hid.shape[2])
        partial = jnp.dot(rows, down, preferred_element_type=F32)
        pair[k] = partial.reshape(size, tile, feats).astype(BF16)
        copy = remote(
            pair.at[k, pl.ds((1 - core) * share, share)],
            pair_in.at[k],
            pair_send,
            pair_recv.at[k],
            mate,
        )
        copy.start()

    def broadcast(k):
        arrived(pair_in.at[k], pair_recv.at[k], mate)
        own = pair[k, pl.ds(core * share, share)].astype(F32) + pair_in[k].astype(F32)
        chips[k, chip] = own.astype(BF16)
        for d in sorted(range(1, nx), key=lambda d: -min(d, nx - d)):
            to = remote(
                chips.at[k, chip],
                chips.at[k, chip],
                chip_send,
                chip_recv.at[k],
                to_chip(d),
            )
            to.start()

    def finish(k):
        arrived(chips.at[k, : nx - 1], chip_recv.at[k], mate)
        branch = chips[k, 0].astype(F32)
        for j in range(1, nx):
            branch += chips[k, j].astype(F32)
        first = k * size + core * share
        for j in range(share):
            own = tok_ref[block(first + j - HOP)].astype(F32)
            mix[first + j] = 0.5 * own + branch[j] * ds_ref[...]
        rows = pl.ds(first, share)
        mine = mix[rows].reshape(share * tile, feats)
        column = jnp.sum(mine * mine, axis=1, keepdims=True)
        square = jnp.sum(jnp.where(diagonal(first, share), column, 0.0), axis=0, keepdims=True)
        remote(mix.at[rows], mix.at[rows], mix_send, mix_recv, mate).start()
        return square

    def diagonal(first, count):
        place = lax.broadcasted_iota(jnp.int32, (count * tile, tokens), 0)
        place = lax.rem(place + tile * (z + first + nz - HOP), tokens)
        return place == lax.broadcasted_iota(jnp.int32, (count * tile, tokens), 1)

    @pl.when(jnp.logical_not(x_lower(0)))
    def _():
        pl.semaphore_wait(x_ready.at[0], 1)

    multiply(0)
    hear(nx // 2 - 2)
    broadcast(0)
    multiply(1)
    broadcast(1)
    near_squares = finish(0)
    far_squares = finish(1)

    squares[core * nz + z] = near_squares + far_squares
    own = squares.at[core * nz + z]
    order = sorted(range(1, nz), key=lambda d: -min(d, nz - d))
    for d in order:
        for t in range(2):
            peer = {"ra": lax.rem(z + d, nz), "cb": chip * 2 + lax.rem(core + t, 2)}
            remote(own, own, sq_send, sq_recv, peer).start()
    remote(own, own, sq_send, sq_recv, mate).start()
    arrived(mix.at[: 2 * share], mix_recv, mate)
    scaled_mixed = mix[...].reshape(tokens, feats) * og_ref[...]
    arrived(squares.at[: 2 * nz - 1], sq_recv, mate)
    everything = squares[0]
    for j in range(1, 2 * nz):
        everything += squares[j]
    inv_row = lax.rsqrt(everything / width + 1e-06)
    inv_second = jnp.sum(jnp.where(diagonal(0, nz), inv_row, 0.0), axis=1, keepdims=True)
    result = (scaled_mixed * inv_second).reshape(nz, tile, feats).astype(BF16)
    for r in range(nz):
        out_ref[block(r - HOP)] = result[r]

    left(part.at[: 4 * HOP - 1], rs_send, mate)
    left(hid.at[: nz - 1], hid_send, mate)
    left(pair.at[0], pair_send, mate)
    left(chips.at[:, : nx - 1], chip_send, mate)
    left(mix.at[: 2 * share], mix_send, mate)
    left(squares.at[: 2 * nz - 1], sq_send, mate)


def solution(mesh):
    nz, nc = mesh.shape["ra"], mesh.shape["cb"]
    nx = nc // 2

    def on_device(tokens, norm_gain, gw, gs, uw, us, dw, ds, og):
        count, feats = tokens.shape
        units = gw.shape[1]
        padded = -(-units // LANES) * LANES
        tile = count // nz
        cols = 2 * units + LANES
        share = nz // 4
        vmem = pl.BlockSpec(memory_space=pltpu.VMEM)
        hbm = pl.BlockSpec(memory_space=pltpu.HBM)
        dma = pltpu.SemaphoreType.DMA
        row = lambda v: v.reshape(1, -1)
        out = pl.pallas_call(
            functools.partial(kernel, nz, nc),
            out_shape=pltpu.VMEM((nz, tile, feats), BF16),
            in_specs=[hbm] * 9,
            out_specs=vmem,
            scratch_shapes=[
                pltpu.VMEM((nz, tile, feats), BF16),
                pltpu.VMEM((1, feats), F32),
                pltpu.VMEM((units,), F32),
                pltpu.VMEM((units,), F32),
                pltpu.VMEM((1, feats), F32),
                pltpu.VMEM((1, feats), F32),
                pltpu.VMEM((2 * units, feats), F32),
                pltpu.VMEM((padded, feats), F32),
                pltpu.VMEM((nz, tile, cols), BF16),
                pltpu.VMEM((2, HOP - 1, tile, cols), BF16),
                pltpu.VMEM((2, tile, cols // 2), BF16),
                pltpu.VMEM((2, HOP - 1, tile, cols), BF16),
                pltpu.VMEM((2, tile, cols), BF16),
                pltpu.VMEM((2, tile, cols), BF16),
                pltpu.VMEM((nz, tile, padded), BF16),
                pltpu.VMEM((2, nz // 2, tile, feats), BF16),
                pltpu.VMEM((2, share, tile, feats), BF16),
                pltpu.VMEM((2, nx, share, tile, feats), BF16),
                pltpu.VMEM((nz, tile, feats), F32),
                pltpu.VMEM((2 * nz, 1, LANES), F32),
                dma((11,)),
                pltpu.SemaphoreType.REGULAR((2, HOP)),
                pltpu.SemaphoreType.REGULAR((3,)),
                pltpu.SemaphoreType.REGULAR((nx // 2 - 1, 2)),
                dma,
                dma((2,)),
                dma,
                dma,
                dma,
                dma((2,)),
                dma,
                dma((2,)),
                dma,
                dma((2,)),
                dma,
                dma,
                dma,
                dma,
            ],
            compiler_params=pltpu.CompilerParams(
                collective_id=0, has_side_effects=True
            ),
        )(
            tokens.reshape(nz, tile, feats),
            row(norm_gain),
            gw.T,
            gs,
            uw.T,
            us,
            dw,
            row(ds),
            row(og),
        )
        return out.reshape(count, feats)

    return jax.shard_map(
        on_device,
        mesh=mesh,
        in_specs=(
            P("grp", "ra"),
            P("ra"),
            P("ra", "cb"),
            P("cb"),
            P("ra", "cb"),
            P("cb"),
            P("cb", "ra"),
            P("ra"),
            P("ra"),
        ),
        out_specs=P("grp", "ra"),
        check_vma=False,
    )
```

```python
import functools

import jax
import jax.numpy as jnp
from jax import lax
from jax.experimental import pallas as pl
from jax.experimental.pallas import tpu as pltpu
from jax.sharding import PartitionSpec as P

MESH = pl.DeviceIdType.MESH
LANES = 128
F32 = jnp.float32
BF16 = jnp.bfloat16
HOP = 4


def remote(src, dst, send_sem, recv_sem, peer):
    return pltpu.make_async_remote_copy(
        src_ref=src,
        dst_ref=dst,
        send_sem=send_sem,
        recv_sem=recv_sem,
        device_id=peer,
        device_id_type=MESH,
    )


def arrived(ref, sem, peer):
    remote(ref, ref, sem, sem, peer).wait_recv()


def left(ref, sem, peer):
    remote(ref, ref, sem, sem, peer).wait_send()


def split_tail(column, lane):
    high = column.astype(BF16).astype(F32)
    return jnp.where(lane == 0, high, jnp.where(lane == 1, column - high, 0.0))


def kernel(
    nz,
    nc,
    tok_hbm,
    gain_hbm,
    gw_ref,
    gs_hbm,
    uw_ref,
    us_hbm,
    dw_ref,
    ds_hbm,
    og_hbm,
    out_ref,
    tok_ref,
    gain_ref,
    gs_ref,
    us_ref,
    ds_ref,
    og_ref,
    gu_v,
    dw_v,
    part,
    far_in,
    far_in_half,
    near_in,
    relay_out,
    relay_in,
    hid,
    pair,
    pair_in,
    chips,
    mix,
    squares,
    load_sem,
    ready,
    x_ready,
    word,
    rs_send,
    far_recv,
    near_recv,
    relay_recv,
    hid_send,
    hid_recv,
    pair_send,
    pair_recv,
    chip_send,
    chip_recv,
    mix_send,
    mix_recv,
    sq_send,
    sq_recv,
):
    z = lax.axis_index("ra")
    cb = lax.axis_index("cb")
    chip = cb // 2
    core = cb % 2
    nx = nc // 2
    tile, feats = tok_ref.shape[1:]
    tokens = nz * tile
    units = gw_ref.shape[0]
    main = units // LANES * LANES
    rest = units - main
    width = feats * nz
    cols = part.shape[2]
    halves = (slice(0, cols // 2), slice(cols // 2, cols))

    def to_z(d):
        return {"ra": lax.rem(z + d + nz, nz)}

    def to_chip(d):
        return {"cb": lax.rem(chip + d, nx) * 2 + core}

    mate = {"cb": chip * 2 + 1 - core}

    def block(d):
        return lax.rem(z + d + 2 * nz, nz)

    near_peers = [(i, k) for k in range(HOP, 0, -1) for i in (0, 1)]
    rising = [(0, k) for k in range(1, HOP + 1)] + [(1, k) for k in range(HOP, 0, -1)]
    sign = (1, -1)

    def lower(i, k):
        return block(sign[i] * k) < z

    def is_last(i, k):
        return block(sign[i] * k) == nz - 1

    def turn(c):
        return jnp.minimum(c, nx - c) * nx + c

    def x_lower(d):
        return core == 0 if d == 0 else turn(lax.rem(chip + d, nx)) < turn(chip)

    def to_x(d):
        return mate if d == 0 else to_chip(d)

    beside = (0, 1, nx - 1)
    barrier = pltpu.get_barrier_semaphore()
    for i, k in near_peers:

        @pl.when(jnp.logical_not(lower(i, k)))
        def _():
            pl.semaphore_signal(barrier, inc=1, device_id=to_z(sign[i] * k), device_id_type=MESH)

    for d in beside:

        @pl.when(jnp.logical_not(x_lower(d)))
        def _():
            pl.semaphore_signal(barrier, inc=1, device_id=to_x(d), device_id_type=MESH)

    loads = [
        pltpu.make_async_copy(src, dst, load_sem.at[k])
        for k, (src, dst) in enumerate(
            [
                (tok_hbm, tok_ref),
                (gain_hbm, gain_ref),
                (gw_ref.at[:main], gu_v.at[:main]),
                (uw_ref.at[:main], gu_v.at[main : 2 * main]),
                (gw_ref.at[main:], gu_v.at[2 * main : 2 * main + rest]),
                (uw_ref.at[main:], gu_v.at[2 * main + rest :]),
                (gs_hbm, gs_ref),
                (us_hbm, us_ref),
                (dw_ref, dw_v.at[:units]),
                (ds_hbm, ds_ref),
                (og_hbm, og_ref),
            ]
        )
    ]
    for copy in loads:
        copy.start()

    count = sum(jnp.where(lower(i, k), 1, 0) for i, k in near_peers)
    count += sum(jnp.where(x_lower(d), 1, 0) for d in beside)

    @pl.when(count > 0)
    def _():
        pl.semaphore_wait(barrier, count)

    for i, k in near_peers:

        @pl.when(lower(i, k))
        def _():
            pl.semaphore_signal(
                ready.at[1 - i, k - 1], inc=1, device_id=to_z(sign[i] * k), device_id_type=MESH
            )

    for n, d in enumerate(beside):

        @pl.when(x_lower(d))
        def _():
            pl.semaphore_signal(
                x_ready.at[(3 - n) % 3], inc=1, device_id=to_x(d), device_id_type=MESH
            )

    for copy in loads[:2]:
        copy.wait()
    values = tok_ref[...].astype(F32).reshape(tokens, feats)
    scaled = (values * gain_ref[...]).astype(BF16)
    lane = lax.broadcasted_iota(jnp.int32, (tokens, LANES), 1)
    tail = split_tail(jnp.sum(values * values, axis=1, keepdims=True), lane)
    part[:, :, 2 * units :] = tail.reshape(nz, tile, LANES).astype(BF16)
    for copy in loads[2:6]:
        copy.wait()
    both = lax.dot_general(
        scaled, gu_v[...].astype(BF16), (((1,), (1,)), ((), ())), preferred_element_type=F32
    )
    part[:, :, : 2 * units] = both.reshape(nz, tile, 2 * units).astype(BF16)

    far = {}
    near = {}
    for i, k in near_peers:
        src = part.at[block(sign[i] * (k + HOP))]
        dst = far_in.at[i, k - 1] if k < HOP else far_in_half.at[i]
        if k == HOP:
            src = part.at[block(sign[i] * (k + HOP)), :, halves[i]]
        far[i, k] = remote(src, dst, rs_send, far_recv.at[i], to_z(sign[i] * k))
        if k < HOP:
            near[i, k] = remote(
                part.at[block(sign[i] * k)],
                near_in.at[i, k - 1],
                rs_send,
                near_recv,
                to_z(sign[i] * k),
            )

    for table in (far, near):
        for i, k in near_peers:
            if (i, k) in table:

                @pl.when(lower(i, k))
                def _():
                    table[i, k].start()

    for i, k in rising:

        @pl.when(jnp.logical_not(lower(i, k)))
        def _():
            pl.semaphore_wait(ready.at[i, k - 1], 1)
            far[i, k].start()
            if k < HOP:

                @pl.when(jnp.logical_not(is_last(i, k)))
                def _():
                    near[i, k].start()

    def tell(m):
        for n, d in ((0, 1), (1, nx - 1)):
            pl.semaphore_signal(word.at[m, 1 - n], inc=1, device_id=to_x(d), device_id_type=MESH)

    def hear(m):
        for n in (0, 1):
            pl.semaphore_wait(word.at[m, n], 1)

    for n, d in ((1, 1), (2, nx - 1)):

        @pl.when(jnp.logical_not(x_lower(d)))
        def _():
            pl.semaphore_wait(x_ready.at[n], 1)

    tell(0)

    for copy in loads[6:]:
        copy.wait()
    row = lax.broadcasted_iota(jnp.int32, dw_v.shape, 0)
    down = jnp.where(row < units, dw_v[...], 0.0).astype(BF16)

    tile_lane = lax.broadcasted_iota(jnp.int32, (tile, LANES), 1)
    relay = [
        remote(relay_out.at[i], relay_in.at[i], rs_send, relay_recv, to_z(sign[i] * HOP))
        for i in (0, 1)
    ]

    def pass_on(i):
        arrived(part.at[: 2 * HOP - 1, :, halves[0]], far_recv.at[i], mate)
        total = part[block(sign[i] * HOP)].astype(F32)
        for k in range(1, HOP):
            total += far_in[i, k - 1].astype(F32)
        pieces = [total[:, halves[0]], total[:, halves[1]]]
        pieces[i] += far_in_half[i].astype(F32)
        last = pieces[1][:, -LANES:]
        relay_out[i, :, halves[0]] = pieces[0].astype(BF16)
        relay_out[i, :, cols // 2 : cols - LANES] = pieces[1][:, :-LANES].astype(BF16)
        relay_out[i, :, cols - LANES :] = split_tail(
            jnp.sum(last, axis=1, keepdims=True), tile_lane
        ).astype(BF16)
        relay[i].start()

    @pl.when(z >= HOP)
    def _():
        pass_on(0)

    pass_on(1)

    for i, k in rising:
        if k < HOP:

            @pl.when(is_last(i, k))
            def _():
                near[i, k].start()

    @pl.when(z < HOP)
    def _():
        pass_on(0)

    hear(0)
    tell(1)

    total = part[z].astype(F32)
    arrived(near_in, near_recv, mate)
    for k in range(1, HOP):
        for i in range(2):
            total += near_in[i, k - 1].astype(F32)
    gate_scale = gs_ref[...].reshape(1, units)
    up_scale = us_ref[...].reshape(1, units)
    mixed_scale = jnp.concatenate([gate_scale[:, main:], up_scale[:, main:]], axis=1)
    arrived(relay_in, relay_recv, mate)
    for i in range(2):
        total += relay_in[i].astype(F32)
    square = jnp.sum(total[:, 2 * units :], axis=1, keepdims=True)
    inv = lax.rsqrt(square / width + 1e-06)
    g = total[:, :main] * inv * gate_scale[:, :main]
    u = total[:, main : 2 * main] * inv * up_scale[:, :main]
    both = total[:, 2 * main : 2 * units] * inv * mixed_scale
    swapped = pltpu.roll(both, rest, 1)
    hid[HOP, :, :main] = (g * jax.nn.sigmoid(g) * u).astype(BF16)
    last = both * jax.nn.sigmoid(both) * swapped
    hid[HOP, :, main:] = jnp.where(tile_lane < rest, last, 0.0).astype(BF16)

    direct = nz // 2 - 1

    def slot(d):
        return (HOP - d) % nz

    for d in (nz // 2, direct, -direct):
        remote(hid.at[HOP], hid.at[slot(d)], hid_send, hid_recv.at[3], to_z(d)).start()
    for i, k in near_peers:
        d = sign[i] * k
        sem = hid_recv.at[i if k == HOP else 2]
        remote(hid.at[HOP], hid.at[slot(d)], hid_send, sem, to_z(d)).start()
    for m in range(1, nx // 2 - 2):
        hear(m)
        tell(m + 1)

    def forward(i):
        arrived(hid.at[0], hid_recv.at[i], mate)
        src = hid.at[slot(sign[i] * HOP)]
        for k in range(direct - HOP - 1, 0, -1):
            dst = hid.at[slot(sign[i] * (HOP + k))]
            remote(src, dst, hid_send, hid_recv.at[3], to_z(sign[i] * k)).start()

    @pl.when(z >= nz // 2)
    def _():
        forward(0)

    forward(1)

    @pl.when(z < nz // 2)
    def _():
        forward(0)

    groups = 2
    size = nz // groups
    share = size // 2

    def multiply(k):
        arrived(hid.at[: 2 * HOP - 2 + k], hid_recv.at[2 + k], mate)
        rows = hid[k * size : (k + 1) * size].reshape(size * tile, hid.shape[2])
        partial = jnp.dot(rows, down, preferred_element_type=F32)
        pair[k] = partial.reshape(size, tile, feats).astype(BF16)
        copy = remote(
            pair.at[k, pl.ds((1 - core) * share, share)],
            pair_in.at[k],
            pair_send,
            pair_recv.at[k],
            mate,
        )
        copy.start()

    def broadcast(k):
        arrived(pair_in.at[k], pair_recv.at[k], mate)
        own = pair[k, pl.ds(core * share, share)].astype(F32) + pair_in[k].astype(F32)
        chips[k, chip] = own.astype(BF16)
        for d in sorted(range(1, nx), key=lambda d: -min(d, nx - d)):
            to = remote(
                chips.at[k, chip],
                chips.at[k, chip],
                chip_send,
                chip_recv.at[k],
                to_chip(d),
            )
            to.start()

    def finish(k):
        arrived(chips.at[k, : nx - 1], chip_recv.at[k], mate)
        branch = chips[k, 0].astype(F32)
        for j in range(1, nx):
            branch += chips[k, j].astype(F32)
        first = k * size + core * share
        for j in range(share):
            own = tok_ref[block(first + j - HOP)].astype(F32)
            mix[first + j] = 0.5 * own + branch[j] * ds_ref[...]
        rows = pl.ds(first, share)
        mine = mix[rows].reshape(share * tile, feats)
        column = jnp.sum(mine * mine, axis=1, keepdims=True)
        square = jnp.sum(jnp.where(diagonal(first, share), column, 0.0), axis=0, keepdims=True)
        remote(mix.at[rows], mix.at[rows], mix_send, mix_recv, mate).start()
        return square

    def diagonal(first, count):
        place = lax.broadcasted_iota(jnp.int32, (count * tile, tokens), 0)
        place = lax.rem(place + tile * (z + first + nz - HOP), tokens)
        return place == lax.broadcasted_iota(jnp.int32, (count * tile, tokens), 1)

    @pl.when(jnp.logical_not(x_lower(0)))
    def _():
        pl.semaphore_wait(x_ready.at[0], 1)

    multiply(0)
    hear(nx // 2 - 2)
    broadcast(0)
    multiply(1)
    broadcast(1)
    near_squares = finish(0)
    far_squares = finish(1)

    squares[core * nz + z] = near_squares + far_squares
    own = squares.at[core * nz + z]
    order = sorted(range(1, nz), key=lambda d: -min(d, nz - d))
    for d in order:
        for t in range(2):
            peer = {"ra": lax.rem(z + d, nz), "cb": chip * 2 + lax.rem(core + t, 2)}
            remote(own, own, sq_send, sq_recv, peer).start()
    remote(own, own, sq_send, sq_recv, mate).start()
    arrived(mix.at[: 2 * share], mix_recv, mate)
    scaled_mixed = mix[...].reshape(tokens, feats) * og_ref[...]
    arrived(squares.at[: 2 * nz - 1], sq_recv, mate)
    everything = squares[0]
    for j in range(1, 2 * nz):
        everything += squares[j]
    inv_row = lax.rsqrt(everything / width + 1e-06)
    inv_second = jnp.sum(jnp.where(diagonal(0, nz), inv_row, 0.0), axis=1, keepdims=True)
    result = (scaled_mixed * inv_second).reshape(nz, tile, feats).astype(BF16)
    for r in range(nz):
        out_ref[block(r - HOP)] = result[r]

    left(part.at[: 4 * HOP - 1], rs_send, mate)
    left(hid.at[: 4 * HOP - 1], hid_send, mate)
    left(pair.at[0], pair_send, mate)
    left(chips.at[:, : nx - 1], chip_send, mate)
    left(mix.at[: 2 * share], mix_send, mate)
    left(squares.at[: 2 * nz - 1], sq_send, mate)


def solution(mesh):
    nz, nc = mesh.shape["ra"], mesh.shape["cb"]
    nx = nc // 2

    def on_device(tokens, norm_gain, gw, gs, uw, us, dw, ds, og):
        count, feats = tokens.shape
        units = gw.shape[1]
        padded = -(-units // LANES) * LANES
        tile = count // nz
        cols = 2 * units + LANES
        share = nz // 4
        vmem = pl.BlockSpec(memory_space=pltpu.VMEM)
        hbm = pl.BlockSpec(memory_space=pltpu.HBM)
        dma = pltpu.SemaphoreType.DMA
        row = lambda v: v.reshape(1, -1)
        out = pl.pallas_call(
            functools.partial(kernel, nz, nc),
            out_shape=pltpu.VMEM((nz, tile, feats), BF16),
            in_specs=[hbm] * 9,
            out_specs=vmem,
            scratch_shapes=[
                pltpu.VMEM((nz, tile, feats), BF16),
                pltpu.VMEM((1, feats), F32),
                pltpu.VMEM((units,), F32),
                pltpu.VMEM((units,), F32),
                pltpu.VMEM((1, feats), F32),
                pltpu.VMEM((1, feats), F32),
                pltpu.VMEM((2 * units, feats), F32),
                pltpu.VMEM((padded, feats), F32),
                pltpu.VMEM((nz, tile, cols), BF16),
                pltpu.VMEM((2, HOP - 1, tile, cols), BF16),
                pltpu.VMEM((2, tile, cols // 2), BF16),
                pltpu.VMEM((2, HOP - 1, tile, cols), BF16),
                pltpu.VMEM((2, tile, cols), BF16),
                pltpu.VMEM((2, tile, cols), BF16),
                pltpu.VMEM((nz, tile, padded), BF16),
                pltpu.VMEM((2, nz // 2, tile, feats), BF16),
                pltpu.VMEM((2, share, tile, feats), BF16),
                pltpu.VMEM((2, nx, share, tile, feats), BF16),
                pltpu.VMEM((nz, tile, feats), F32),
                pltpu.VMEM((2 * nz, 1, LANES), F32),
                dma((11,)),
                pltpu.SemaphoreType.REGULAR((2, HOP)),
                pltpu.SemaphoreType.REGULAR((3,)),
                pltpu.SemaphoreType.REGULAR((nx // 2 - 1, 2)),
                dma,
                dma((2,)),
                dma,
                dma,
                dma,
                dma((4,)),
                dma,
                dma((2,)),
                dma,
                dma((2,)),
                dma,
                dma,
                dma,
                dma,
            ],
            compiler_params=pltpu.CompilerParams(
                collective_id=0, has_side_effects=True
            ),
        )(
            tokens.reshape(nz, tile, feats),
            row(norm_gain),
            gw.T,
            gs,
            uw.T,
            us,
            dw,
            row(ds),
            row(og),
        )
        return out.reshape(count, feats)

    return jax.shard_map(
        on_device,
        mesh=mesh,
        in_specs=(
            P("grp", "ra"),
            P("ra"),
            P("ra", "cb"),
            P("cb"),
            P("ra", "cb"),
            P("cb"),
            P("cb", "ra"),
            P("ra"),
            P("ra"),
        ),
        out_specs=P("grp", "ra"),
        check_vma=False,
    )
```

```python
import functools

import jax
import jax.numpy as jnp
from jax import lax
from jax.experimental import pallas as pl
from jax.experimental.pallas import tpu as pltpu
from jax.sharding import PartitionSpec as P

MESH = pl.DeviceIdType.MESH
LANES = 128
F32 = jnp.float32
BF16 = jnp.bfloat16
HOP = 4


def remote(src, dst, send_sem, recv_sem, peer):
    return pltpu.make_async_remote_copy(
        src_ref=src,
        dst_ref=dst,
        send_sem=send_sem,
        recv_sem=recv_sem,
        device_id=peer,
        device_id_type=MESH,
    )


def arrived(ref, sem, peer):
    remote(ref, ref, sem, sem, peer).wait_recv()


def left(ref, sem, peer):
    remote(ref, ref, sem, sem, peer).wait_send()


def split_tail(column, lane):
    high = column.astype(BF16).astype(F32)
    return jnp.where(lane == 0, high, jnp.where(lane == 1, column - high, 0.0))


def kernel(
    nz,
    nc,
    tok_hbm,
    gain_hbm,
    gw_ref,
    gs_hbm,
    uw_ref,
    us_hbm,
    dw_ref,
    ds_hbm,
    og_hbm,
    out_ref,
    tok_ref,
    gain_ref,
    gs_ref,
    us_ref,
    ds_ref,
    og_ref,
    gu_v,
    dw_v,
    part,
    far_in,
    far_in_half,
    near_in,
    relay_out,
    relay_in,
    hid,
    pair,
    pair_in,
    chips,
    mix,
    squares,
    load_sem,
    ready,
    x_ready,
    word,
    rs_send,
    far_recv,
    near_recv,
    relay_recv,
    hid_send,
    hid_recv,
    pair_send,
    pair_recv,
    chip_send,
    chip_recv,
    mix_send,
    mix_recv,
    sq_send,
    sq_recv,
):
    z = lax.axis_index("ra")
    cb = lax.axis_index("cb")
    chip = cb // 2
    core = cb % 2
    nx = nc // 2
    tile, feats = tok_ref.shape[1:]
    tokens = nz * tile
    units = gw_ref.shape[0]
    main = units // LANES * LANES
    rest = units - main
    width = feats * nz
    cols = part.shape[2]
    halves = (slice(0, cols // 2), slice(cols // 2, cols))

    def to_z(d):
        return {"ra": lax.rem(z + d + nz, nz)}

    def to_chip(d):
        return {"cb": lax.rem(chip + d, nx) * 2 + core}

    mate = {"cb": chip * 2 + 1 - core}

    def block(d):
        return lax.rem(z + d + 2 * nz, nz)

    near_peers = [(i, k) for k in range(HOP, 0, -1) for i in (0, 1)]
    rising = [(0, k) for k in range(1, HOP + 1)] + [(1, k) for k in range(HOP, 0, -1)]
    sign = (1, -1)

    def lower(i, k):
        return block(sign[i] * k) < z

    def turn(c):
        return jnp.minimum(c, nx - c) * nx + c

    def x_lower(d):
        return core == 0 if d == 0 else turn(lax.rem(chip + d, nx)) < turn(chip)

    def to_x(d):
        return mate if d == 0 else to_chip(d)

    beside = (0, 1, nx - 1)
    barrier = pltpu.get_barrier_semaphore()
    for i, k in near_peers:

        @pl.when(jnp.logical_not(lower(i, k)))
        def _():
            pl.semaphore_signal(barrier, inc=1, device_id=to_z(sign[i] * k), device_id_type=MESH)

    for d in beside:

        @pl.when(jnp.logical_not(x_lower(d)))
        def _():
            pl.semaphore_signal(barrier, inc=1, device_id=to_x(d), device_id_type=MESH)

    loads = [
        pltpu.make_async_copy(src, dst, load_sem.at[k])
        for k, (src, dst) in enumerate(
            [
                (tok_hbm, tok_ref),
                (gain_hbm, gain_ref),
                (gw_ref.at[:main], gu_v.at[:main]),
                (uw_ref.at[:main], gu_v.at[main : 2 * main]),
                (gw_ref.at[main:], gu_v.at[2 * main : 2 * main + rest]),
                (uw_ref.at[main:], gu_v.at[2 * main + rest :]),
                (gs_hbm, gs_ref),
                (us_hbm, us_ref),
                (dw_ref, dw_v.at[:units]),
                (ds_hbm, ds_ref),
                (og_hbm, og_ref),
            ]
        )
    ]
    for copy in loads:
        copy.start()

    count = sum(jnp.where(lower(i, k), 1, 0) for i, k in near_peers)
    count += sum(jnp.where(x_lower(d), 1, 0) for d in beside)

    @pl.when(count > 0)
    def _():
        pl.semaphore_wait(barrier, count)

    for i, k in near_peers:

        @pl.when(lower(i, k))
        def _():
            pl.semaphore_signal(
                ready.at[1 - i, k - 1], inc=1, device_id=to_z(sign[i] * k), device_id_type=MESH
            )

    for n, d in enumerate(beside):

        @pl.when(x_lower(d))
        def _():
            pl.semaphore_signal(
                x_ready.at[(3 - n) % 3], inc=1, device_id=to_x(d), device_id_type=MESH
            )

    for copy in loads[:2]:
        copy.wait()
    values = tok_ref[...].astype(F32).reshape(tokens, feats)
    scaled = (values * gain_ref[...]).astype(BF16)
    lane = lax.broadcasted_iota(jnp.int32, (tokens, LANES), 1)
    tail = split_tail(jnp.sum(values * values, axis=1, keepdims=True), lane)
    part[:, :, 2 * units :] = tail.reshape(nz, tile, LANES).astype(BF16)
    for copy in loads[2:6]:
        copy.wait()
    both = lax.dot_general(
        scaled, gu_v[...].astype(BF16), (((1,), (1,)), ((), ())), preferred_element_type=F32
    )
    part[:, :, : 2 * units] = both.reshape(nz, tile, 2 * units).astype(BF16)

    far = {}
    near = {}
    for i, k in near_peers:
        src = part.at[block(sign[i] * (k + HOP))]
        dst = far_in.at[i, k - 1] if k < HOP else far_in_half.at[i]
        if k == HOP:
            src = part.at[block(sign[i] * (k + HOP)), :, halves[i]]
        far[i, k] = remote(src, dst, rs_send, far_recv.at[i], to_z(sign[i] * k))
        if k < HOP:
            near[i, k] = remote(
                part.at[block(sign[i] * k)],
                near_in.at[i, k - 1],
                rs_send,
                near_recv,
                to_z(sign[i] * k),
            )

    for table in (far, near):
        for i, k in near_peers:
            if (i, k) in table:

                @pl.when(lower(i, k))
                def _():
                    table[i, k].start()

    for i, k in rising:

        @pl.when(jnp.logical_not(lower(i, k)))
        def _():
            pl.semaphore_wait(ready.at[i, k - 1], 1)
            far[i, k].start()
            if k < HOP:
                near[i, k].start()

    def tell(m):
        for n, d in ((0, 1), (1, nx - 1)):
            pl.semaphore_signal(word.at[m, 1 - n], inc=1, device_id=to_x(d), device_id_type=MESH)

    def hear(m):
        for n in (0, 1):
            pl.semaphore_wait(word.at[m, n], 1)

    for n, d in ((1, 1), (2, nx - 1)):

        @pl.when(jnp.logical_not(x_lower(d)))
        def _():
            pl.semaphore_wait(x_ready.at[n], 1)

    tell(0)

    for copy in loads[6:]:
        copy.wait()
    row = lax.broadcasted_iota(jnp.int32, dw_v.shape, 0)
    down = jnp.where(row < units, dw_v[...], 0.0).astype(BF16)

    tile_lane = lax.broadcasted_iota(jnp.int32, (tile, LANES), 1)
    relay = [
        remote(relay_out.at[i], relay_in.at[i], rs_send, relay_recv, to_z(sign[i] * HOP))
        for i in (0, 1)
    ]

    def pass_on(i):
        arrived(part.at[: 2 * HOP - 1, :, halves[0]], far_recv.at[i], mate)
        total = part[block(sign[i] * HOP)].astype(F32)
        for k in range(1, HOP):
            total += far_in[i, k - 1].astype(F32)
        pieces = [total[:, halves[0]], total[:, halves[1]]]
        pieces[i] += far_in_half[i].astype(F32)
        last = pieces[1][:, -LANES:]
        relay_out[i, :, halves[0]] = pieces[0].astype(BF16)
        relay_out[i, :, cols // 2 : cols - LANES] = pieces[1][:, :-LANES].astype(BF16)
        relay_out[i, :, cols - LANES :] = split_tail(
            jnp.sum(last, axis=1, keepdims=True), tile_lane
        ).astype(BF16)
        relay[i].start()

    @pl.when(z >= HOP)
    def _():
        pass_on(0)

    pass_on(1)

    @pl.when(z < HOP)
    def _():
        pass_on(0)

    hear(0)
    tell(1)

    total = part[z].astype(F32)
    arrived(near_in, near_recv, mate)
    for k in range(1, HOP):
        for i in range(2):
            total += near_in[i, k - 1].astype(F32)
    gate_scale = gs_ref[...].reshape(1, units)
    up_scale = us_ref[...].reshape(1, units)
    mixed_scale = jnp.concatenate([gate_scale[:, main:], up_scale[:, main:]], axis=1)
    arrived(relay_in, relay_recv, mate)
    for i in range(2):
        total += relay_in[i].astype(F32)
    square = jnp.sum(total[:, 2 * units :], axis=1, keepdims=True)
    inv = lax.rsqrt(square / width + 1e-06)
    g = total[:, :main] * inv * gate_scale[:, :main]
    u = total[:, main : 2 * main] * inv * up_scale[:, :main]
    both = total[:, 2 * main : 2 * units] * inv * mixed_scale
    swapped = pltpu.roll(both, rest, 1)
    hid[HOP, :, :main] = (g * jax.nn.sigmoid(g) * u).astype(BF16)
    last = both * jax.nn.sigmoid(both) * swapped
    hid[HOP, :, main:] = jnp.where(tile_lane < rest, last, 0.0).astype(BF16)

    direct = nz // 2 - 1

    def slot(d):
        return (HOP - d) % nz

    for d in (nz // 2, direct, -direct):
        remote(hid.at[HOP], hid.at[slot(d)], hid_send, hid_recv.at[3], to_z(d)).start()
    for i, k in near_peers:
        d = sign[i] * k
        sem = hid_recv.at[i if k == HOP else 2]
        remote(hid.at[HOP], hid.at[slot(d)], hid_send, sem, to_z(d)).start()
    for m in range(1, nx // 2 - 2):
        hear(m)
        tell(m + 1)

    def forward(i):
        arrived(hid.at[0], hid_recv.at[i], mate)
        src = hid.at[slot(sign[i] * HOP)]
        for k in range(direct - HOP - 1, 0, -1):
            dst = hid.at[slot(sign[i] * (HOP + k))]
            remote(src, dst, hid_send, hid_recv.at[3], to_z(sign[i] * k)).start()

    @pl.when(z >= nz // 2)
    def _():
        forward(0)

    forward(1)

    @pl.when(z < nz // 2)
    def _():
        forward(0)

    groups = 2
    size = nz // groups
    share = size // 2

    def multiply(k):
        arrived(hid.at[: 2 * HOP - 2 + k], hid_recv.at[2 + k], mate)
        rows = hid[k * size : (k + 1) * size].reshape(size * tile, hid.shape[2])
        partial = jnp.dot(rows, down, preferred_element_type=F32)
        pair[k] = partial.reshape(size, tile, feats).astype(BF16)
        copy = remote(
            pair.at[k, pl.ds((1 - core) * share, share)],
            pair_in.at[k],
            pair_send,
            pair_recv.at[k],
            mate,
        )
        copy.start()

    def broadcast(k):
        arrived(pair_in.at[k], pair_recv.at[k], mate)
        own = pair[k, pl.ds(core * share, share)].astype(F32) + pair_in[k].astype(F32)
        chips[k, chip] = own.astype(BF16)
        for d in sorted(range(1, nx), key=lambda d: -min(d, nx - d)):
            to = remote(
                chips.at[k, chip],
                chips.at[k, chip],
                chip_send,
                chip_recv.at[k],
                to_chip(d),
            )
            to.start()

    def finish(k):
        arrived(chips.at[k, : nx - 1], chip_recv.at[k], mate)
        branch = chips[k, 0].astype(F32)
        for j in range(1, nx):
            branch += chips[k, j].astype(F32)
        first = k * size + core * share
        for j in range(share):
            own = tok_ref[block(first + j - HOP)].astype(F32)
            mix[first + j] = 0.5 * own + branch[j] * ds_ref[...]
        rows = pl.ds(first, share)
        mine = mix[rows].reshape(share * tile, feats)
        column = jnp.sum(mine * mine, axis=1, keepdims=True)
        square = jnp.sum(jnp.where(diagonal(first, share), column, 0.0), axis=0, keepdims=True)
        remote(mix.at[rows], mix.at[rows], mix_send, mix_recv, mate).start()
        return square

    def diagonal(first, count):
        place = lax.broadcasted_iota(jnp.int32, (count * tile, tokens), 0)
        place = lax.rem(place + tile * (z + first + nz - HOP), tokens)
        return place == lax.broadcasted_iota(jnp.int32, (count * tile, tokens), 1)

    @pl.when(jnp.logical_not(x_lower(0)))
    def _():
        pl.semaphore_wait(x_ready.at[0], 1)

    multiply(0)
    hear(nx // 2 - 2)
    broadcast(0)
    multiply(1)
    broadcast(1)
    near_squares = finish(0)
    far_squares = finish(1)

    squares[core * nz + z] = near_squares + far_squares
    own = squares.at[core * nz + z]
    order = sorted(range(1, nz), key=lambda d: -min(d, nz - d))
    for d in order:
        for t in range(2):
            peer = {"ra": lax.rem(z + d, nz), "cb": chip * 2 + lax.rem(core + t, 2)}
            remote(own, own, sq_send, sq_recv, peer).start()
    remote(own, own, sq_send, sq_recv, mate).start()
    arrived(mix.at[: 2 * share], mix_recv, mate)
    scaled_mixed = mix[...].reshape(tokens, feats) * og_ref[...]
    arrived(squares.at[: 2 * nz - 1], sq_recv, mate)
    everything = squares[0]
    for j in range(1, 2 * nz):
        everything += squares[j]
    inv_row = lax.rsqrt(everything / width + 1e-06)
    inv_second = jnp.sum(jnp.where(diagonal(0, nz), inv_row, 0.0), axis=1, keepdims=True)
    result = (scaled_mixed * inv_second).reshape(nz, tile, feats).astype(BF16)
    for r in range(nz):
        out_ref[block(r - HOP)] = result[r]

    left(part.at[: 4 * HOP - 1], rs_send, mate)
    left(hid.at[: 4 * HOP - 1], hid_send, mate)
    left(pair.at[0], pair_send, mate)
    left(chips.at[:, : nx - 1], chip_send, mate)
    left(mix.at[: 2 * share], mix_send, mate)
    left(squares.at[: 2 * nz - 1], sq_send, mate)


def solution(mesh):
    nz, nc = mesh.shape["ra"], mesh.shape["cb"]
    nx = nc // 2

    def on_device(tokens, norm_gain, gw, gs, uw, us, dw, ds, og):
        count, feats = tokens.shape
        units = gw.shape[1]
        padded = -(-units // LANES) * LANES
        tile = count // nz
        cols = 2 * units + LANES
        share = nz // 4
        vmem = pl.BlockSpec(memory_space=pltpu.VMEM)
        hbm = pl.BlockSpec(memory_space=pltpu.HBM)
        dma = pltpu.SemaphoreType.DMA
        row = lambda v: v.reshape(1, -1)
        out = pl.pallas_call(
            functools.partial(kernel, nz, nc),
            out_shape=pltpu.VMEM((nz, tile, feats), BF16),
            in_specs=[hbm] * 9,
            out_specs=vmem,
            scratch_shapes=[
                pltpu.VMEM((nz, tile, feats), BF16),
                pltpu.VMEM((1, feats), F32),
                pltpu.VMEM((units,), F32),
                pltpu.VMEM((units,), F32),
                pltpu.VMEM((1, feats), F32),
                pltpu.VMEM((1, feats), F32),
                pltpu.VMEM((2 * units, feats), F32),
                pltpu.VMEM((padded, feats), F32),
                pltpu.VMEM((nz, tile, cols), BF16),
                pltpu.VMEM((2, HOP - 1, tile, cols), BF16),
                pltpu.VMEM((2, tile, cols // 2), BF16),
                pltpu.VMEM((2, HOP - 1, tile, cols), BF16),
                pltpu.VMEM((2, tile, cols), BF16),
                pltpu.VMEM((2, tile, cols), BF16),
                pltpu.VMEM((nz, tile, padded), BF16),
                pltpu.VMEM((2, nz // 2, tile, feats), BF16),
                pltpu.VMEM((2, share, tile, feats), BF16),
                pltpu.VMEM((2, nx, share, tile, feats), BF16),
                pltpu.VMEM((nz, tile, feats), F32),
                pltpu.VMEM((2 * nz, 1, LANES), F32),
                dma((11,)),
                pltpu.SemaphoreType.REGULAR((2, HOP)),
                pltpu.SemaphoreType.REGULAR((3,)),
                pltpu.SemaphoreType.REGULAR((nx // 2 - 1, 2)),
                dma,
                dma((2,)),
                dma,
                dma,
                dma,
                dma((4,)),
                dma,
                dma((2,)),
                dma,
                dma((2,)),
                dma,
                dma,
                dma,
                dma,
            ],
            compiler_params=pltpu.CompilerParams(
                collective_id=0, has_side_effects=True
            ),
        )(
            tokens.reshape(nz, tile, feats),
            row(norm_gain),
            gw.T,
            gs,
            uw.T,
            us,
            dw,
            row(ds),
            row(og),
        )
        return out.reshape(count, feats)

    return jax.shard_map(
        on_device,
        mesh=mesh,
        in_specs=(
            P("grp", "ra"),
            P("ra"),
            P("ra", "cb"),
            P("cb"),
            P("ra", "cb"),
            P("cb"),
            P("cb", "ra"),
            P("ra"),
            P("ra"),
        ),
        out_specs=P("grp", "ra"),
        check_vma=False,
    )
```
